512 devices in a mesh: sp: 64 (over z, y), tp: 8 (over x, core).
Axes of the slice: x: 4, y: 4, z: 16, core: 2. Of those that a mesh axis runs over, the one named last changes fastest.
Arguments:
- receptance: bfloat16 [12288, 1024], P('sp', 'tp'), may hold values from -6 to 6
- head_keys: bfloat16 [12288, 1024], P('sp', 'tp'), may hold values from -6 to 6
- head_values: bfloat16 [12288, 1024], P('sp', 'tp'), may hold values from -6 to 6
- decay_preact: float32 [12288, 1024], P('sp', 'tp'), may hold values from -13.5 to -0.5
- learning_rate_preact: float32 [12288, 1024], P('sp', 'tp'), may hold values from -10.5 to 2.5
- output_gate_preact: bfloat16 [12288, 1024], P('sp', 'tp'), may hold values from -8 to 8
- self_token_weight: float32 [16, 64], P('tp'), may hold values from -0.6 to 0.6
- head_norm_gain: float32 [1024], P('tp'), may hold values from 0.1 to 1.9
- output_weight: bfloat16 [1024, 2048], P('tp'), may hold values from -0.1875 to 0.1875
- residual: bfloat16 [12288, 2048], P('sp'), may hold values from -6 to 6
- premixer_norm_gain: float32 [2048], replicated, may hold values from 0.1 to 1.9
- mixer_gate_weight: bfloat16 [2048, 5120], P('sp', 'tp'), may hold values from -0.125 to 0.125
- mixer_up_weight: bfloat16 [2048, 5120], P('sp', 'tp'), may hold values from -0.125 to 0.125
- mixer_down_weight: bfloat16 [5120, 2048], P('tp', 'sp'), may hold values from -0.078125 to 0.078125
Outputs:
- layer_out: bfloat16 [12288, 2048], P(('sp', 'tp'))
The draws below stay inside these ranges and needn't reach their ends.
All inputs are finite; a program needn't handle non-finite values.
Results may differ from the reference program's by a relative error of at most 0.015.
Values may be sent and summed in bfloat16 or wider, within the bound.
A program may use at most 64 MiB of HBM per device.

```python
import jax
import jax.numpy as jnp
from jax import lax

D = 2048
WIDTH = 1024
HEAD_SIZE = 64
RECURRENT_HEADS = 16
FF = 5120
TOK_DEV = 192
TOKENS = 12288
N_TP = 8


def head_speed(key):
    chosen = jax.random.permutation(jax.random.fold_in(key, 4711), WIDTH // HEAD_SIZE)
    fast_count = WIDTH // HEAD_SIZE // 2
    return chosen < fast_count


def draw_decay_preact(key, part):
    fast_heads = head_speed(key)
    head_total = WIDTH // HEAD_SIZE
    keys_all = jax.random.split(jax.random.fold_in(key, 17), 5)
    fast_base = jax.random.uniform(keys_all[0], (head_total,), jnp.float32, -3.5, -2.5)
    slow_base = jax.random.uniform(keys_all[1], (head_total,), jnp.float32, -11.5, -10.5)
    head_base = jnp.where(fast_heads, fast_base, slow_base)
    shards = TOKENS // TOK_DEV
    block_shift = jax.random.uniform(keys_all[2], (shards, head_total), jnp.float32, -1.0, 1.0)
    block_shift = jnp.repeat(block_shift, TOK_DEV, axis=0)
    jitter = jax.random.uniform(keys_all[3], (TOKENS, head_total, HEAD_SIZE), jnp.float32, -1.0, 1.0)
    return (head_base[None, :, None] + block_shift[:, :, None] + jitter).reshape(TOKENS, WIDTH)


def draw_learning_rate_preact(key, part):
    fast_heads = head_speed(key)
    head_total = WIDTH // HEAD_SIZE
    keys_all = jax.random.split(jax.random.fold_in(key, 29), 2)
    fast_part = jax.random.uniform(keys_all[0], (TOKENS, head_total, HEAD_SIZE), jnp.float32, -2.5, 2.5)
    slow_part = jax.random.uniform(keys_all[1], (TOKENS, head_total, HEAD_SIZE), jnp.float32, -10.5, -7.5)
    return jnp.where(fast_heads[None, :, None], fast_part, slow_part).reshape(TOKENS, WIDTH)


def block_scale(own_key, dims, cuts, smallest, high):
    factor_of, own = 1.0, jax.random.fold_in(own_key, 6)
    for axis_at, shards_of in cuts:
        draws = jnp.exp(jax.random.uniform(jax.random.fold_in(own, axis_at), (shards_of,), jnp.float32, smallest / len(cuts), high / len(cuts)))
        factor_of = factor_of * jnp.repeat(draws, dims[axis_at] // shards_of).reshape([-1 if axis == axis_at else 1 for axis in range(len(dims))])
    return factor_of


def centred(key, shape, scale, most, cuts=(), held_as=jnp.bfloat16):
    drawn = jax.random.normal(key, shape, jnp.float32) * scale
    if len(cuts) > 0:
        drawn = block_scale(key, shape, cuts, -0.22, 0.18) * drawn
    return jnp.clip(drawn, min=-most, max=most).astype(held_as)


def setup_inputs(seed: int = 0) -> dict:
    keys = jax.random.split(jax.random.key(seed), 15)
    return {
        "receptance": centred(keys[0], (TOKENS, WIDTH), 1.0, 6.0, ((0, 64), (1, 8))),
        "head_keys": centred(keys[1], (TOKENS, WIDTH), 1.0, 6.0, ((0, 64), (1, 8))),
        "head_values": centred(keys[2], (TOKENS, WIDTH), 1.0, 6.0, ((0, 64), (1, 8))),
        "decay_preact": draw_decay_preact(jax.random.fold_in(keys[14], 71), 0),
        "learning_rate_preact": draw_learning_rate_preact(jax.random.fold_in(keys[14], 71), 0),
        "output_gate_preact": centred(keys[5], (TOKENS, WIDTH), 1.5, 8.0, ((0, 64), (1, 8))),
        "self_token_weight": centred(keys[6], (RECURRENT_HEADS, HEAD_SIZE), 0.1, 0.6, ((0, 8),), jnp.float32),
        "head_norm_gain": jnp.clip(1.0 + 0.18 * jax.random.normal(keys[7], (WIDTH,), jnp.float32), 0.1, 1.9),
        "output_weight": centred(keys[8], (WIDTH, D), WIDTH ** -0.5, 0.1875, ((0, 8),)),
        "residual": centred(keys[9], (TOKENS, D), 1.0, 6.0, ((0, 64),)),
        "premixer_norm_gain": jnp.clip(1.0 + 0.18 * jax.random.normal(keys[10], (D,), jnp.float32), 0.1, 1.9),
        "mixer_gate_weight": centred(keys[11], (D, FF), D ** -0.5, 0.125, ((0, 64), (1, 8))),
        "mixer_up_weight": centred(keys[12], (D, FF), D ** -0.5, 0.125, ((0, 64), (1, 8))),
        "mixer_down_weight": centred(keys[13], (FF, D), FF ** -0.5, 0.078125, ((0, 8), (1, 64))),
    }


GROUP_EPS = 0.00064
NORM_EPS = 1e-06
EXACT = lax.Precision.HIGHEST

def final_output(layer_result, receptance_rows, keys_single, values_single, self_token_weight, head_norm_gain, output_gate_preact):
    centre = lax.optimization_barrier(jnp.mean(layer_result, axis=-1, keepdims=True))
    spread = lax.optimization_barrier(jnp.mean(jnp.square(layer_result - centre), axis=-1, keepdims=True))
    scaled_rows = (layer_result - centre) * lax.rsqrt(spread + GROUP_EPS)
    self_token_term = lax.optimization_barrier(jnp.sum(receptance_rows * keys_single * self_token_weight[None], axis=-1, keepdims=True)) * values_single
    sequence_length = layer_result.shape[0]
    heads_merged = scaled_rows.reshape(sequence_length, -1) * head_norm_gain[None] + self_token_term.reshape(sequence_length, -1)
    return (heads_merged * jax.nn.sigmoid(output_gate_preact.astype(jnp.float32))).astype(jnp.bfloat16)

def reference(receptance, head_keys, head_values, decay_preact, learning_rate_preact, output_gate_preact, self_token_weight, head_norm_gain, output_weight, residual, premixer_norm_gain, mixer_gate_weight, mixer_up_weight, mixer_down_weight):
    sequence_length = receptance.shape[0]
    head_count = WIDTH // HEAD_SIZE
    layout = (sequence_length, head_count, HEAD_SIZE)
    receptance_rows = receptance.astype(jnp.float32).reshape(layout)
    keys_single = head_keys.astype(jnp.float32).reshape(layout)
    values_single = head_values.astype(jnp.float32).reshape(layout)
    decay_rate = jnp.exp(-jnp.exp(-jax.nn.softplus(-decay_preact) - 0.5)).reshape(layout)
    learn_rate = jax.nn.sigmoid(learning_rate_preact).reshape(layout)
    unit_key = keys_single / jnp.maximum(jnp.linalg.norm(keys_single, axis=-1, keepdims=True), 1.0)
    remove_dir = -unit_key
    insert_dir = unit_key * learn_rate

    def advance(memory, inputs):
        decay_t, key_t, value_t, remove_t, insert_t, recept_t = inputs
        erased = jnp.einsum('hij,hj->hi', memory, remove_t, precision=EXACT)
        memory = memory * decay_t[:, None, :] + erased[:, :, None] * insert_t[:, None, :] + value_t[:, :, None] * key_t[:, None, :]
        return (memory, jnp.einsum('hij,hj->hi', memory, recept_t, precision=EXACT))
    start_state = jnp.zeros((head_count, HEAD_SIZE, HEAD_SIZE), jnp.float32)
    _, recurrence_output = lax.scan(advance, start_state, (decay_rate, keys_single, values_single, remove_dir, insert_dir, receptance_rows))
    mixer_output = final_output(recurrence_output, receptance_rows, keys_single, values_single, self_token_weight, head_norm_gain, output_gate_preact)
    group = WIDTH // N_TP

    def add_group(total, which):
        begin = (which * group).astype(jnp.int32)
        columns = lax.dynamic_slice_in_dim(mixer_output, begin, group, 1)
        rows_part = lax.dynamic_slice_in_dim(output_weight, begin, group, 0)
        product = jnp.dot(columns.astype(jnp.float32), rows_part.astype(jnp.float32), preferred_element_type=jnp.float32)
        return (total + lax.optimization_barrier(product.astype(jnp.bfloat16)).astype(jnp.float32), None)
    mix_sum, _ = lax.scan(add_group, jnp.zeros((sequence_length, D), jnp.float32), jnp.arange(N_TP, dtype=jnp.int32))
    mix = lax.optimization_barrier(mix_sum.astype(jnp.bfloat16)).astype(jnp.float32)
    after_mix = (residual.astype(jnp.float32) + mix).astype(jnp.bfloat16)
    widened = after_mix.astype(jnp.float32)
    normed = (widened * lax.rsqrt(lax.optimization_barrier(jnp.mean(widened * widened, axis=-1, keepdims=True)) + NORM_EPS) * premixer_norm_gain[None]).astype(jnp.bfloat16)
    hidden_group = FF // N_TP

    def add_hidden(total, which):
        begin = (which * hidden_group).astype(jnp.int32)
        gate_sum = jnp.dot(normed.astype(jnp.float32), lax.dynamic_slice_in_dim(mixer_gate_weight, begin, hidden_group, 1).astype(jnp.float32), preferred_element_type=jnp.float32)
        up_sum = jnp.dot(normed.astype(jnp.float32), lax.dynamic_slice_in_dim(mixer_up_weight, begin, hidden_group, 1).astype(jnp.float32), preferred_element_type=jnp.float32)
        hidden = (jax.nn.silu(gate_sum) * up_sum).astype(jnp.bfloat16)
        product = jnp.dot(hidden.astype(jnp.float32), lax.dynamic_slice_in_dim(mixer_down_weight, begin, hidden_group, 0).astype(jnp.float32), preferred_element_type=jnp.float32)
        return (total + lax.optimization_barrier(product.astype(jnp.bfloat16)).astype(jnp.float32), None)
    down_sum, _ = lax.scan(add_hidden, jnp.zeros((sequence_length, D), jnp.float32), jnp.arange(N_TP, dtype=jnp.int32))
    return (after_mix.astype(jnp.float32) + down_sum).astype(jnp.bfloat16)
```

```python
import functools

import jax
import jax.numpy as jnp
from jax import lax
from jax.experimental import pallas as pl
from jax.experimental.pallas import tpu as pltpu
from jax.sharding import Mesh
from jax.sharding import PartitionSpec as P

HS = 64
CHUNK = 64
W2 = 2 * HS
GROUP_EPS = 0.00064
NORM_EPS = 1e-06
F32 = jnp.float32
BF = jnp.bfloat16
NN = (((1,), (0,)), ((), ()))
NT = (((1,), (1,)), ((), ()))
SEMS = 160


def dg(a, b, dims=NN):
    return lax.dot_general(a, b, dims, preferred_element_type=F32)


def halves(x):
    hi = x.astype(BF)
    return hi, (x - hi.astype(F32)).astype(BF)


def dot_halves(a, b, dims=NN):
    return dg(a[0], b[0], dims) + (dg(a[0], b[1], dims) + dg(a[1], b[0], dims))


def dot3(a, b, dims=NN):
    return dot_halves(halves(a), halves(b), dims)


def dot2(a, b, dims=NN):
    hi, lo = halves(a)
    return dg(hi, b, dims) + dg(lo, b, dims)


def iota(shape, dim):
    return lax.broadcasted_iota(jnp.int32, shape, dim)


def head_masks():
    lane = iota((1, W2), 1)
    first = (lane < HS).astype(F32)
    return first, 1.0 - first


def stacked(x):
    first, second = head_masks()
    return jnp.concatenate([x * first, x * second], axis=0)


def folded(x):
    half = x.shape[0] // 2
    return x[:half] + x[half:]


def head_ones():
    i, j = iota((W2, W2), 0), iota((W2, W2), 1)
    return ((i < HS) == (j < HS)).astype(BF)


def compose(earlier, later):
    moved = dot3(earlier, stacked(later[:HS]))
    return jnp.concatenate([moved[:HS], moved[HS:] + later[HS:]], axis=0)


def identity_pair():
    i, j = iota((W2, W2), 0), iota((W2, W2), 1)
    return ((i == j) | (i + HS == j)).astype(F32) * (i < HS).astype(F32)


def local_chunk(r, k, v, pre, lr):
    logw = jax.nn.sigmoid(pre) * (-0.6065306597126334)
    i, j = iota((CHUNK, CHUNK), 0), iota((CHUNK, CHUNK), 1)
    tri = (i >= j).astype(BF)
    a1 = logw.astype(BF)
    rest = logw - a1.astype(F32)
    a2, a3 = halves(rest)
    cum = dg(tri, a1) + (dg(tri, a2) + dg(tri, a3))
    last = cum[CHUNK - 1 :, :]
    grown = jnp.exp(-cum)
    decayed = jnp.exp(cum)
    tail = jnp.exp(last - cum)
    norm = jnp.sqrt(dot2(k * k, head_ones()))
    unit = k / jnp.maximum(norm, 1.0)
    ins = unit * jax.nn.sigmoid(lr)
    us = stacked(-jnp.exp(cum - logw) * unit)
    rs = stacked(decayed * r)
    bs = stacked(ins * grown)
    ks = stacked(k * grown)
    bts = halves(stacked(ins * tail))
    kts = stacked(k * tail)
    vs = stacked(v).astype(BF)
    gram = dot3(jnp.concatenate([us, rs], axis=0), jnp.concatenate([bs, ks], axis=0), NT)
    i, j = iota((W2, W2), 0), iota((W2, W2), 1)
    same = (i < HS) == (j < HS)
    strict = same & (i > j)
    incl = same & (i >= j)
    lb = jnp.where(strict, gram[:W2, :W2], 0.0)
    lk = jnp.where(strict, gram[:W2, W2:], 0.0)
    mb = jnp.where(incl, gram[W2:, :W2], 0.0)
    mk = jnp.where(incl, gram[W2:, W2:], 0.0)
    inv = (i == j).astype(F32)
    size = 1
    while size < CHUNK:
        row, col = i // size, j // size
        part = jnp.where((row == col + 1) & (row % 2 == 1), lb, 0.0)
        if size == 1:
            inv = inv + part
        else:
            held = halves(inv)
            inv = inv + dot_halves(halves(dot_halves(held, halves(part))), held)
        size *= 2
    lkv = dot2(lk, vs)
    tuv = dot3(inv, jnp.concatenate([us, lkv], axis=1))
    tuv_halves = halves(tuv)
    turned = dot_halves(halves(tuv.T), bts)
    last_col = jnp.where(i == j, jnp.exp(last), 0.0)
    trans = folded(last_col + turned[:W2])
    kth, ktl = halves(kts)
    vt = stacked(v).T.astype(BF)
    state = folded(turned[W2:] + dg(vt, kth) + dg(vt, ktl))
    muv = dot_halves(halves(mb), tuv_halves)
    seen = folded(rs + muv[:, :W2])
    local = folded(muv[:, W2:] + dot2(mk, vs))
    return jnp.concatenate([trans, state], axis=0), seen, local


def kernel(
    nz,
    ny,
    ntp,
    r_ref,
    k_ref,
    v_ref,
    pre_ref,
    lr_ref,
    og_ref,
    stw_ref,
    hg_ref,
    ow_in,
    res_in,
    gain_ref,
    gate_in,
    up_in,
    down_in,
    out_ref,
    gu,
    dn,
    ow,
    res,
    py,
    pz,
    entry,
    seen_ref,
    local_ref,
    self_ref,
    mx,
    am,
    normed,
    hid,
    part,
    got,
    lsem,
    ssem,
    rsem,
    bar_unused,
):
    z, y, tp = lax.axis_index("z"), lax.axis_index("y"), lax.axis_index("tp")
    rows = r_ref.shape[0]
    chunks = rows // CHUNK
    own = rows // ntp
    width = res_in.shape[1]
    half_f = gate_in.shape[0]
    ff = gate_in.shape[1]
    half_ring = nz // 2
    nx = ntp // 2
    xx, core = tp // 2, tp % 2

    def zof(step):
        return lax.rem(z + step + nz, nz)

    def yof(step):
        return lax.rem(y + step + ny, ny)

    def tof(step):
        return lax.rem(tp + step + ntp, ntp)

    def sp(zz, yy):
        return zz * ny + yy

    def dev(zz=None, yy=None, tt=None):
        return {"z": z if zz is None else zz, "y": y if yy is None else yy, "tp": tp if tt is None else tt}

    loads = [
        pltpu.make_async_copy(gate_in, gu.at[sp(z, y), 0:half_f], lsem.at[0]),
        pltpu.make_async_copy(up_in, gu.at[sp(z, y), half_f : 2 * half_f], lsem.at[1]),
        pltpu.make_async_copy(down_in, dn.at[sp(z, y)], lsem.at[2]),
        pltpu.make_async_copy(ow_in, ow.at[tp], lsem.at[3]),
        pltpu.make_async_copy(res_in, res, lsem.at[4]),
    ]
    for load in loads:
        load.start()

    barrier = pltpu.get_barrier_semaphore()
    peers = [dev(zz=zof(1)), dev(zz=zof(-1))]
    peers += [dev(yy=yof(d)) for d in range(1, ny)]
    peers += [dev(tt=tof(d)) for d in range(1, ntp)]
    for peer in peers:
        pl.semaphore_signal(barrier, inc=1, device_id=peer, device_id_type=pl.DeviceIdType.MESH)
    pl.semaphore_wait(barrier, len(peers))
    for load in loads:
        load.wait()

    count = [0]
    sent = []

    def channel():
        count[0] += 1
        return count[0] - 1

    def copy(src, dst, ch, device):
        return pltpu.make_async_remote_copy(
            src_ref=src,
            dst_ref=dst,
            send_sem=ssem.at[ch],
            recv_sem=rsem.at[ch],
            device_id=device,
            device_id_type=pl.DeviceIdType.MESH,
        )

    def send(ref, ch, device):
        c = copy(ref, ref, ch, device)
        c.start()
        sent.append(c)

    def arrived(ref, ch, device):
        copy(ref, ref, ch, device).wait_recv()

    class Ring:
        def __init__(self, block):
            self.block = block
            self.ch = [(channel(), channel()) for _ in range(half_ring)]

        def piece(self, s, side):
            return side if s == half_ring else None

        def push(self, s):
            send(self.block(zof(1 - s), self.piece(s, 0)), self.ch[s - 1][0], dev(zz=zof(1)))
            send(self.block(zof(s - 1), self.piece(s, 1)), self.ch[s - 1][1], dev(zz=zof(-1)))

        def pull(self, s):
            arrived(self.block(zof(-s), self.piece(s, 0)), self.ch[s - 1][0], dev(zz=zof(-1)))
            arrived(self.block(zof(s), self.piece(s, 1)), self.ch[s - 1][1], dev(zz=zof(1)))

    class Across:
        def __init__(self, block):
            self.block = block
            self.ch = [channel() for _ in range(4)]

        def push(self):
            send(self.block(y, None), self.ch[0], dev(yy=yof(1)))
            send(self.block(y, None), self.ch[1], dev(yy=yof(-1)))

        def forward(self):
            arrived(self.block(yof(-1), None), self.ch[0], dev(yy=yof(-1)))
            send(self.block(yof(-1), 0), self.ch[2], dev(yy=yof(1)))
            arrived(self.block(yof(1), None), self.ch[1], dev(yy=yof(1)))
            send(self.block(yof(1), 1), self.ch[3], dev(yy=yof(-1)))

        def finish(self):
            arrived(self.block(yof(2), 0), self.ch[2], dev(yy=yof(-1)))
            arrived(self.block(yof(2), 1), self.ch[3], dev(yy=yof(1)))

    def gu_block(zz, yy, piece):
        slot = sp(zz, yy)
        if piece is None:
            return gu.at[slot]
        return gu.at[slot, piece * half_f : (piece + 1) * half_f]

    def dn_group(zz, piece):
        if piece is None:
            return dn.at[pl.ds(zz * ny, ny)]
        return dn.at[pl.ds(zz * ny + piece * (ny // 2), ny // 2)]

    def dn_block(yy, piece):
        slot = sp(z, yy)
        if piece is None:
            return dn.at[slot]
        return dn.at[slot, piece * (half_f // 2) : (piece + 1) * (half_f // 2)]

    def pz_block(zz, piece):
        if piece is None:
            return pz.at[zz]
        return pz.at[zz, piece * HS : (piece + 1) * HS]

    ring_gu = Ring(lambda zz, piece: gu_block(zz, y, piece))
    ring_dn = Ring(dn_group)
    ring_ps = Ring(pz_block)
    order = [0]
    for s in range(1, half_ring):
        order += [-s, s]
    order += [half_ring]
    across = [
        Across(functools.partial(lambda step, yy, piece: gu_block(zof(step), yy, piece), step))
        for step in order
    ]
    across_dn = Across(dn_block)
    done_across = [0]

    def pump_across(n=1):
        for _ in range(n):
            if done_across[0] < len(across):
                across[done_across[0]].forward()
                done_across[0] += 1

    def same_core(d):
        return lax.rem(xx + d + nx, nx) * 2 + core

    partner = xx * 2 + (1 - core)

    def with_core(d, c):
        return lax.rem(xx + d + nx, nx) * 2 + c

    ow_far = [channel() for _ in range(1, nx)]
    ow_near = [channel() for _ in range(nx)]

    ring_gu.push(1)
    across[0].push()
    across_dn.push()
    for d in range(1, nx):
        send(ow.at[tp], ow_far[d - 1], dev(tt=same_core(d)))
    send(ow.at[tp], ow_near[0], dev(tt=partner))

    ones = head_ones()
    pair = None
    for c in range(chunks):
        span = pl.ds(c * CHUNK, CHUNK)
        r, k, v = (ref[span, :].astype(F32) for ref in (r_ref, k_ref, v_ref))
        ps, seen, local = local_chunk(r, k, v, pre_ref[span, :], lr_ref[span, :])
        seen_ref[span, :] = seen
        local_ref[span, :] = local
        self_ref[span, :] = dot2(r * k * stw_ref[...], ones) * v
        pair = ps if pair is None else compose(pair, ps)
        if c < chunks - 1:
            entry[c] = pair
    py[y] = pair
    ch_y = [channel() for _ in range(1, ny)]
    for d in range(1, ny):
        send(py.at[y], ch_y[d - 1], dev(yy=yof(d)))
    across_dn.forward()
    for d in range(1, ny):
        arrived(py.at[yof(-d)], ch_y[d - 1], dev(yy=yof(-d)))
    inside = identity_pair()
    running = py[0]
    for yy in range(1, ny):
        inside = jnp.where(y == yy, running, inside)
        running = compose(running, py[yy])
    pz[z] = running
    ring_ps.push(1)

    trans_left = identity_pair()[:HS]
    state_left = jnp.zeros((HS, W2), F32)
    state_right = jnp.zeros((HS, W2), F32)
    for s in range(1, half_ring + 1):
        ring_gu.pull(s)
        if s < half_ring:
            ring_gu.push(s + 1)
            across[2 * s - 1].push()
            across[2 * s].push()
        else:
            across[2 * s - 1].push()
        ring_ps.pull(s)
        if s < half_ring:
            ring_ps.push(s + 1)
        pump_across()
        left = pz[zof(-s)]
        has_left = z >= s
        moved = dot3(left, stacked(trans_left))
        trans_left = jnp.where(has_left, moved[:HS], trans_left)
        state_left = jnp.where(has_left, state_left + moved[HS:], state_left)
        if s < half_ring:
            right = pz[zof(s)]
            has_right = z + s >= nz
            state_right = jnp.where(
                has_right, dot3(state_right, stacked(right[:HS])) + right[HS:], state_right
            )
    across_dn.finish()
    ring_dn.push(1)
    state = dot3(state_right, stacked(trans_left)) + state_left
    state = dot3(state, stacked(inside[:HS])) + inside[HS:]

    for c in range(chunks):
        span = pl.ds(c * CHUNK, CHUNK)
        at = state
        if c > 0:
            at = dot3(state, stacked(entry[c - 1][:HS])) + entry[c - 1][HS:]
        o = dot3(seen_ref[span, :], stacked(at), NT) + local_ref[span, :]
        centre = dot2(o, ones) * (1.0 / HS)
        shifted = o - centre
        spread = dot2(shifted * shifted, ones) * (1.0 / HS)
        merged = shifted * lax.rsqrt(spread + GROUP_EPS) * hg_ref[...] + self_ref[span, :]
        gated = merged * jax.nn.sigmoid(og_ref[span, :].astype(F32))
        mx[tp, span, :] = gated.astype(BF)
    ch_mx = [channel() for _ in range(1, ntp)]
    for d in range(1, ntp):
        send(mx.at[tp], ch_mx[d - 1], dev(tt=tof(d)))

    dn_step = [1]

    def pump_dn(n=1):
        for _ in range(n):
            if dn_step[0] <= half_ring:
                ring_dn.pull(dn_step[0])
                if dn_step[0] < half_ring:
                    ring_dn.push(dn_step[0] + 1)
                dn_step[0] += 1

    for d in range(1, nx):
        slot = ow.at[same_core(-d)]
        arrived(slot, ow_far[d - 1], dev(tt=same_core(-d)))
        send(slot, ow_near[d], dev(tt=partner))
    for d in range(1, ntp):
        arrived(mx.at[tof(-d)], ch_mx[d - 1], dev(tt=tof(-d)))
    arrived(ow.at[partner], ow_near[0], dev(tt=partner))
    for d in range(1, nx):
        arrived(ow.at[with_core(-d, 1 - core)], ow_near[d], dev(tt=partner))
    pump_across()
    pump_dn()

    tile = min(256, width)
    tiles = width // tile
    lhs = jnp.concatenate([mx[g] for g in range(ntp)], axis=1)

    def project(n, square):
        cols = pl.ds(pl.multiple_of(n * tile, tile), tile)
        mix = dg(lhs, ow[:, :, cols].reshape(ntp * W2, tile)).astype(BF).astype(F32)
        after = (res[:, cols].astype(F32) + mix).astype(BF).astype(F32)
        am[:, cols] = after
        sq = after * after
        for q in range(tile // W2):
            square = square + sq[:, q * W2 : (q + 1) * W2]
        return square

    square = jnp.zeros((rows, W2), F32)
    square = lax.fori_loop(0, tiles, project, square)
    pump_across()
    pump_dn()
    scale = lax.rsqrt(jnp.sum(square, axis=1, keepdims=True) * (1.0 / width) + NORM_EPS)

    def normalize(n, carry):
        cols = pl.ds(pl.multiple_of(n * tile, tile), tile)
        normed[:, cols] = (am[:, cols] * scale * gain_ref[:, cols]).astype(BF)
        return carry

    lax.fori_loop(0, tiles, normalize, 0)
    while done_across[0] < len(across):
        pump_across()
        pump_dn()
    for a in across:
        a.finish()

    at = 0
    while at < ff:
        wide = min(256, ff - at)
        x = normed[...]
        gate = dg(x, gu[:, 0:half_f, at : at + wide].reshape(width, wide))
        up = dg(x, gu[:, half_f : 2 * half_f, at : at + wide].reshape(width, wide))
        hid[:, at : at + wide] = (gate / (1.0 + jnp.exp(-gate)) * up).astype(BF)
        at += wide
        pump_dn()
    pump_dn(half_ring)

    slots = tile // half_f
    ch_part = [[channel() for _ in range(1, ntp)] for _ in range(2)]

    def down(n, carry):
        cols = pl.ds(pl.multiple_of(n * tile, tile), tile)
        w = dn[pl.ds(n * slots, slots)].reshape(tile, ff)
        prod = dg(hid[...], w, NT)
        part[:, :, cols] = prod.reshape(ntp, own, tile).astype(BF)
        return carry

    half_w = width // 2
    for piece in range(2):
        lax.fori_loop(piece * tiles // 2, (piece + 1) * tiles // 2, down, 0)
        cols = pl.ds(piece * half_w, half_w)
        for d in range(1, ntp):
            c = copy(
                part.at[tof(d), :, cols], got.at[tp, :, cols], ch_part[piece][d - 1], dev(tt=tof(d))
            )
            c.start()
            sent.append(c)
    total = part[tp].astype(F32)
    for d in range(1, ntp):
        for piece in range(2):
            cols = pl.ds(piece * half_w, half_w)
            arrived(got.at[tof(-d), :, cols], ch_part[piece][d - 1], dev(tt=tof(-d)))
        total = total + got[tof(-d)].astype(F32)
    mine = am[pl.ds(pl.multiple_of(tp * own, own), own), :]
    out_ref[...] = (mine + total).astype(BF)
    for c in sent:
        c.wait_send()
    assert count[0] <= SEMS, count[0]


def per_device(
    nz,
    ny,
    ntp,
    receptance,
    head_keys,
    head_values,
    decay_preact,
    learning_rate_preact,
    output_gate_preact,
    self_token_weight,
    head_norm_gain,
    output_weight,
    residual,
    premixer_norm_gain,
    mixer_gate_weight,
    mixer_up_weight,
    mixer_down_weight,
):
    rows = receptance.shape[0]
    width = residual.shape[1]
    half_f, ff = mixer_gate_weight.shape
    own = rows // ntp
    vmem = pl.BlockSpec(memory_space=pltpu.VMEM)
    hbm = pl.BlockSpec(memory_space=pl.ANY)
    return pl.pallas_call(
        functools.partial(kernel, nz, ny, ntp),
        out_shape=jax.ShapeDtypeStruct((own, width), BF),
        in_specs=[vmem] * 8 + [hbm, hbm, vmem, hbm, hbm, hbm],
        out_specs=vmem,
        scratch_shapes=[
            pltpu.VMEM((nz * ny, 2 * half_f, ff), BF),
            pltpu.VMEM((nz * ny, half_f, ff), BF),
            pltpu.VMEM((ntp, W2, width), BF),
            pltpu.VMEM((rows, width), BF),
            pltpu.VMEM((ny, W2, W2), F32),
            pltpu.VMEM((nz, W2, W2), F32),
            pltpu.VMEM((rows // CHUNK, W2, W2), F32),
            pltpu.VMEM((rows, W2), F32),
            pltpu.VMEM((rows, W2), F32),
            pltpu.VMEM((rows, W2), F32),
            pltpu.VMEM((ntp, rows, W2), BF),
            pltpu.VMEM((rows, width), F32),
            pltpu.VMEM((rows, width), BF),
            pltpu.VMEM((rows, ff), BF),
            pltpu.VMEM((ntp, own, width), BF),
            pltpu.VMEM((ntp, own, width), BF),
            pltpu.SemaphoreType.DMA((5,)),
            pltpu.SemaphoreType.DMA((SEMS,)),
            pltpu.SemaphoreType.DMA((SEMS,)),
            pltpu.SMEM((1,), jnp.int32),
        ],
        compiler_params=pltpu.CompilerParams(
            collective_id=0, has_side_effects=True, vmem_limit_bytes=60 * 1024 * 1024
        ),
        name="layer",
    )(
        receptance,
        head_keys,
        head_values,
        decay_preact,
        learning_rate_preact,
        output_gate_preact,
        self_token_weight.reshape(1, -1),
        head_norm_gain.reshape(1, -1),
        output_weight,
        residual,
        premixer_norm_gain.reshape(1, -1),
        mixer_gate_weight,
        mixer_up_weight,
        mixer_down_weight.T,
    )


def build(mesh, nz, ny):
    ntp = mesh.shape["tp"]
    torus = Mesh(mesh.devices.reshape(nz, ny, ntp), ("z", "y", "tp"))
    sp = ("z", "y")
    cut = P(sp, "tp")
    in_specs = (cut,) * 6 + (
        P("tp", None),
        P("tp"),
        P("tp", None),
        P(sp, None),
        P(),
        cut,
        cut,
        P("tp", sp),
    )
    return jax.shard_map(
        functools.partial(per_device, nz, ny, ntp),
        mesh=torus,
        in_specs=in_specs,
        out_specs=P(("z", "y", "tp"), None),
        check_vma=False,
    )


def solution(mesh):
    return build(mesh, 16, 4)
```

```python
import functools

import jax
import jax.numpy as jnp
from jax import lax
from jax.experimental import pallas as pl
from jax.experimental.pallas import tpu as pltpu
from jax.sharding import Mesh
from jax.sharding import PartitionSpec as P

HS = 64
CHUNK = 64
W2 = 2 * HS
GROUP_EPS = 0.00064
NORM_EPS = 1e-06
F32 = jnp.float32
BF = jnp.bfloat16
NN = (((1,), (0,)), ((), ()))
NT = (((1,), (1,)), ((), ()))
SEMS = 200


def dg(a, b, dims=NN):
    return lax.dot_general(a, b, dims, preferred_element_type=F32)


def halves(x):
    hi = x.astype(BF)
    return hi, (x - hi.astype(F32)).astype(BF)


def dot_halves(a, b, dims=NN):
    return dg(a[0], b[0], dims) + (dg(a[0], b[1], dims) + dg(a[1], b[0], dims))


def dot3(a, b, dims=NN):
    return dot_halves(halves(a), halves(b), dims)


def dot2(a, b, dims=NN):
    hi, lo = halves(a)
    return dg(hi, b, dims) + dg(lo, b, dims)


def iota(shape, dim):
    return lax.broadcasted_iota(jnp.int32, shape, dim)


def head_masks():
    lane = iota((1, W2), 1)
    first = (lane < HS).astype(F32)
    return first, 1.0 - first


def stacked(x):
    first, second = head_masks()
    return jnp.concatenate([x * first, x * second], axis=0)


def folded(x):
    half = x.shape[0] // 2
    return x[:half] + x[half:]


def head_ones():
    i, j = iota((W2, W2), 0), iota((W2, W2), 1)
    return ((i < HS) == (j < HS)).astype(BF)


def compose(earlier, later):
    moved = dot3(earlier, stacked(later[:HS]))
    return jnp.concatenate([moved[:HS], moved[HS:] + later[HS:]], axis=0)


def identity_pair():
    i, j = iota((W2, W2), 0), iota((W2, W2), 1)
    return ((i == j) | (i + HS == j)).astype(F32) * (i < HS).astype(F32)


def chunk_stages(chunks):
    i, j = iota((CHUNK, CHUNK), 0), iota((CHUNK, CHUNK), 1)
    tri = (i >= j).astype(BF)
    ones = head_ones()
    i, j = iota((W2, W2), 0), iota((W2, W2), 1)
    same = (i < HS) == (j < HS)
    strict = same & (i > j)
    incl = same & (i >= j)
    made = []
    for r, k, v, pre, lr in chunks:
        logw = jax.nn.sigmoid(pre) * (-0.6065306597126334)
        a1 = logw.astype(BF)
        a2, a3 = halves(logw - a1.astype(F32))
        cum = dg(tri, a1) + (dg(tri, a2) + dg(tri, a3))
        last = cum[CHUNK - 1 :, :]
        grown = jnp.exp(-cum)
        tail = jnp.exp(last - cum)
        unit = k / jnp.maximum(jnp.sqrt(dot2(k * k, ones)), 1.0)
        ins = unit * jax.nn.sigmoid(lr)
        us = stacked(-jnp.exp(cum - logw) * unit)
        rs = stacked(jnp.exp(cum) * r)
        made.append(
            dict(
                last=last,
                us=us,
                rs=rs,
                left=halves(jnp.concatenate([us, rs], axis=0)),
                right=halves(
                    jnp.concatenate([stacked(ins * grown), stacked(k * grown)], axis=0)
                ),
                bts=halves(stacked(ins * tail)),
                kts=halves(stacked(k * tail)),
                v=stacked(v),
            )
        )
    yield
    for m in made:
        gram = dot_halves(m["left"], m["right"], NT)
        m["lb"] = jnp.where(strict, gram[:W2, :W2], 0.0)
        m["lk"] = jnp.where(strict, gram[:W2, W2:], 0.0)
        m["mb"] = jnp.where(incl, gram[W2:, :W2], 0.0)
        m["mk"] = jnp.where(incl, gram[W2:, W2:], 0.0)
        m["vs"] = m["v"].astype(BF)
    for m in made:
        m["lkv"] = dot2(m["lk"], m["vs"])
        m["mkv"] = dot2(m["mk"], m["vs"])
    yield
    size = 1
    while size < CHUNK:
        row, col = i // size, j // size
        below = (row == col + 1) & (row % 2 == 1)
        if size == 1:
            for m in made:
                m["inv"] = (i == j).astype(F32) + jnp.where(below, m["lb"], 0.0)
        else:
            held = [halves(m["inv"]) for m in made]
            mid = [
                dot_halves(h, halves(jnp.where(below, m["lb"], 0.0))) for h, m in zip(held, made)
            ]
            for m, h, x in zip(made, held, mid):
                m["inv"] = m["inv"] + dot_halves(halves(x), h)
        size *= 2
        if size == 8 or size == 32:
            yield
    for m in made:
        m["tuv"] = dot3(m["inv"], jnp.concatenate([m["us"], m["lkv"]], axis=1))
    out = []
    for m in made:
        turned = dot_halves(halves(m["tuv"].T), m["bts"])
        trans = folded(jnp.where(i == j, jnp.exp(m["last"]), 0.0) + turned[:W2])
        vt = m["v"].T.astype(BF)
        state = folded(turned[W2:] + dg(vt, m["kts"][0]) + dg(vt, m["kts"][1]))
        m["pair"] = jnp.concatenate([trans, state], axis=0)
    for m in made:
        muv = dot_halves(halves(m["mb"]), halves(m["tuv"]))
        out.append(
            (m["pair"], folded(m["rs"] + muv[:, :W2]), folded(muv[:, W2:] + m["mkv"]))
        )
    return out


def kernel(
    nz,
    ny,
    ntp,
    r_ref,
    k_ref,
    v_ref,
    pre_ref,
    lr_ref,
    og_ref,
    stw_ref,
    hg_ref,
    ow_in,
    res_in,
    gain_ref,
    gate_in,
    up_in,
    down_in,
    out_ref,
    gu,
    dn,
    ow,
    res,
    py,
    pz,
    entry,
    seen_ref,
    local_ref,
    self_ref,
    mx,
    am,
    normed,
    hid,
    part,
    got,
    pgot,
    comb,
    lsem,
    ssem,
    rsem,
):
    z, y, tp = lax.axis_index("z"), lax.axis_index("y"), lax.axis_index("tp")
    rows = r_ref.shape[0]
    chunks = rows // CHUNK
    own = rows // ntp
    width = res_in.shape[1]
    half_f = gate_in.shape[0]
    ff = gate_in.shape[1]
    half_ring = nz // 2
    nx = ntp // 2
    xx, core = tp // 2, tp % 2

    def zof(step):
        return lax.rem(z + step + nz, nz)

    def yof(step):
        return lax.rem(y + step + ny, ny)

    def tof(step):
        return lax.rem(tp + step + ntp, ntp)

    def sp(zz, yy):
        return zz * ny + yy

    def dev(zz=None, yy=None, tt=None):
        return {"z": z if zz is None else zz, "y": y if yy is None else yy, "tp": tp if tt is None else tt}

    scope = [None]

    def mark(name):
        if scope[0] is not None:
            scope[0].__exit__(None, None, None)
        scope[0] = None
        if name:
            scope[0] = jax.named_scope(name)
            scope[0].__enter__()

    mark("enter")
    loads = [
        pltpu.make_async_copy(gate_in, gu.at[sp(z, y), 0:half_f], lsem.at[0]),
        pltpu.make_async_copy(up_in, gu.at[sp(z, y), half_f : 2 * half_f], lsem.at[1]),
        pltpu.make_async_copy(down_in, dn.at[sp(z, y)], lsem.at[2]),
        pltpu.make_async_copy(ow_in, ow.at[tp], lsem.at[3]),
        pltpu.make_async_copy(res_in, res, lsem.at[4]),
    ]
    for load in loads:
        load.start()

    barrier = pltpu.get_barrier_semaphore()
    peers = [dev(zz=zof(1)), dev(zz=zof(-1))]
    peers += [dev(yy=yof(d)) for d in range(1, ny)]
    peers += [dev(tt=tof(d)) for d in range(1, ntp)]
    for peer in peers:
        pl.semaphore_signal(barrier, inc=1, device_id=peer, device_id_type=pl.DeviceIdType.MESH)
    pl.semaphore_wait(barrier, len(peers))
    for load in loads:
        load.wait()

    count = [0]
    sent = []

    def channel():
        count[0] += 1
        return count[0] - 1

    def copy(src, dst, ch, device):
        return pltpu.make_async_remote_copy(
            src_ref=src,
            dst_ref=dst,
            send_sem=ssem.at[ch],
            recv_sem=rsem.at[ch],
            device_id=device,
            device_id_type=pl.DeviceIdType.MESH,
        )

    def send(ref, ch, device):
        c = copy(ref, ref, ch, device)
        c.start()
        sent.append(c)

    def arrived(ref, ch, device):
        copy(ref, ref, ch, device).wait_recv()

    class Ring:
        def __init__(self, block):
            self.block = block
            self.ch = [(channel(), channel()) for _ in range(half_ring)]
            self.step = 1

        def piece(self, s, side):
            return side if s == half_ring else None

        def push(self, s):
            send(self.block(zof(1 - s), self.piece(s, 0)), self.ch[s - 1][0], dev(zz=zof(1)))
            send(self.block(zof(s - 1), self.piece(s, 1)), self.ch[s - 1][1], dev(zz=zof(-1)))

        def turn(self):
            s = self.step
            if s > half_ring:
                return
            arrived(self.block(zof(-s), self.piece(s, 0)), self.ch[s - 1][0], dev(zz=zof(-1)))
            arrived(self.block(zof(s), self.piece(s, 1)), self.ch[s - 1][1], dev(zz=zof(1)))
            if s < half_ring:
                self.push(s + 1)
            self.step = s + 1

    class Across:
        def __init__(self, block, at, to):
            self.block, self.at, self.to = block, at, to
            self.ch = [channel() for _ in range(4)]

        def push(self):
            send(self.block(self.at(0), None), self.ch[0], self.to(1))
            send(self.block(self.at(0), None), self.ch[1], self.to(-1))

        def forward(self):
            arrived(self.block(self.at(-1), None), self.ch[0], self.to(-1))
            send(self.block(self.at(-1), 0), self.ch[2], self.to(1))
            arrived(self.block(self.at(1), None), self.ch[1], self.to(1))
            send(self.block(self.at(1), 1), self.ch[3], self.to(-1))

        def finish(self):
            arrived(self.block(self.at(2), 0), self.ch[2], self.to(-1))
            arrived(self.block(self.at(2), 1), self.ch[3], self.to(1))

    def cut(ref, piece, size):
        return ref if piece is None else ref.at[piece * size : (piece + 1) * size]

    def gu_block(zz, yy, piece):
        return cut(gu.at[sp(zz, yy)], piece, half_f)

    def dn_pair(which, zz, piece):
        if piece is None:
            return dn.at[pl.ds(zz * ny + which * (ny // 2), ny // 2)]
        return dn.at[pl.ds(zz * ny + which * (ny // 2) + piece * (ny // 4), ny // 4)]

    def y_dev(d):
        return dev(yy=yof(d))

    ring_gu = Ring(lambda zz, piece: gu_block(zz, y, piece))
    ring_d0 = Ring(functools.partial(dn_pair, 0))
    ring_d1 = Ring(functools.partial(dn_pair, 1))
    ring_ps = Ring(lambda zz, piece: cut(pz.at[zz], piece, HS))
    order = [0]
    for s in range(1, half_ring):
        order += [-s, s]
    order += [half_ring]
    across = [
        Across(
            functools.partial(lambda step, yy, piece: gu_block(zof(step), yy, piece), step),
            yof,
            y_dev,
        )
        for step in order
    ]
    across_dn = Across(lambda yy, piece: cut(dn.at[sp(z, yy)], piece, half_f // 2), yof, y_dev)

    bulk = [ring_gu] * 3 + [ring_d0]
    while len(bulk) < 3 * half_ring:
        bulk += [ring_d1, ring_gu, ring_d0]
    bulk += [ring_d1] * half_ring + [ring_d0] * half_ring
    progress = {"bulk": 0, "push": 1, "forward": 0}

    def turn(n=1):
        done = 0
        while done < n and progress["bulk"] < len(bulk):
            ring = bulk[progress["bulk"]]
            progress["bulk"] += 1
            if ring.step <= half_ring:
                ring.turn()
                done += 1

    def y_push(n=1):
        for _ in range(n):
            i = progress["push"]
            if i < len(across) and (i + 1) // 2 < ring_gu.step:
                across[i].push()
                progress["push"] += 1

    def y_forward(n=1):
        for _ in range(n):
            if progress["forward"] < progress["push"]:
                across[progress["forward"]].forward()
                progress["forward"] += 1

    def same_core(d):
        return lax.rem(xx + d + nx, nx) * 2 + core

    def other_core(d):
        return lax.rem(xx + d + nx, nx) * 2 + (1 - core)

    def x_dev(d):
        return dev(tt=same_core(d))

    partner = other_core(0)
    near = dev(tt=partner)
    across_ow = None
    if nx == 4:
        across_ow = Across(lambda t, piece: cut(ow.at[t], piece, W2 // 2), same_core, x_dev)
    ow_far = [channel() for _ in range(1, nx)]
    ow_near = [channel() for _ in range(nx)]

    def ow_start():
        if across_ow is not None:
            across_ow.push()
        else:
            for d in range(1, nx):
                send(ow.at[tp], ow_far[d - 1], x_dev(d))
        send(ow.at[tp], ow_near[0], near)

    def ow_share(d):
        send(ow.at[same_core(d)], ow_near[d % nx], near)

    def ow_middle():
        if across_ow is not None:
            across_ow.forward()
            ow_share(1)
            ow_share(-1)

    def ow_last():
        if across_ow is not None:
            across_ow.finish()
            ow_share(2)
        else:
            for d in range(1, nx):
                arrived(ow.at[same_core(-d)], ow_far[d - 1], x_dev(-d))
                ow_share(-d)

    def ow_finish():
        for d in range(nx):
            arrived(ow.at[other_core(d)], ow_near[d], near)

    mark("launch")
    ring_gu.push(1)
    across[0].push()
    across_dn.push()
    ow_start()

    mark("recur")
    ones = head_ones()
    spans = [pl.ds(c * CHUNK, CHUNK) for c in range(chunks)]
    given = []
    for span in spans:
        r, k, v = (ref[span, :].astype(F32) for ref in (r_ref, k_ref, v_ref))
        given.append((r, k, v, pre_ref[span, :], lr_ref[span, :]))
    stages = chunk_stages(given)
    stage = 0
    while True:
        try:
            next(stages)
        except StopIteration as end:
            made = end.value
            break
        mark(f"recur_pump{stage}")
        if stage == 1:
            turn()
            y_push()
        if stage == 2:
            across_dn.forward()
        if stage == 3:
            turn()
            y_forward()
        stage += 1
        mark(f"recur{stage}")
    pair = None
    for c, (ps, seen, local) in enumerate(made):
        seen_ref[spans[c], :] = seen
        local_ref[spans[c], :] = local
        pair = ps if pair is None else compose(pair, ps)
        if c < chunks - 1:
            entry[c] = pair
    mark("scan_y")
    py[y] = pair
    ch_y = [channel() for _ in range(1, ny)]
    for d in range(1, ny):
        send(py.at[y], ch_y[d - 1], dev(yy=yof(d)))
    y_push(2)
    across_dn.finish()
    ring_d0.push(1)
    for c, (r, k, v, _, _) in enumerate(given):
        self_ref[spans[c], :] = dot2(r * k * stw_ref[...], ones) * v
    turn()
    mark("scan_ywait")
    ring_d1.push(1)
    for d in range(1, ny):
        arrived(py.at[yof(-d)], ch_y[d - 1], dev(yy=yof(-d)))
    mark("scan_yfix")
    inside = identity_pair()
    running = py[0]
    for yy in range(1, ny):
        inside = jnp.where(y == yy, running, inside)
        running = compose(running, py[yy])
    pz[z] = running
    ring_ps.push(1)

    trans_left = identity_pair()[:HS]
    state_left = jnp.zeros((HS, W2), F32)
    state_right = jnp.zeros((HS, W2), F32)
    for s in range(1, half_ring + 1):
        mark(f"scan_z{s}")
        turn()
        ring_ps.turn()
        y_push()
        y_forward()
        if s == half_ring // 2:
            ow_middle()
        if s == half_ring - 1:
            ow_last()
        left = pz[zof(-s)]
        has_left = z >= s
        moved = dot3(left, stacked(trans_left))
        trans_left = jnp.where(has_left, moved[:HS], trans_left)
        state_left = jnp.where(has_left, state_left + moved[HS:], state_left)
        if s < half_ring:
            right = pz[zof(s)]
            has_right = z + s >= nz
            state_right = jnp.where(
                has_right, dot3(state_right, stacked(right[:HS])) + right[HS:], state_right
            )
    mark("state")
    state = dot3(state_right, stacked(trans_left)) + state_left
    state = dot3(state, stacked(inside[:HS])) + inside[HS:]

    mark("mech")
    for c in range(chunks):
        span = spans[c]
        at = state
        if c > 0:
            at = dot3(state, stacked(entry[c - 1][:HS])) + entry[c - 1][HS:]
        o = dot3(seen_ref[span, :], stacked(at), NT) + local_ref[span, :]
        centre = dot2(o, ones) * (1.0 / HS)
        shifted = o - centre
        spread = dot2(shifted * shifted, ones) * (1.0 / HS)
        merged = shifted * lax.rsqrt(spread + GROUP_EPS) * hg_ref[...] + self_ref[span, :]
        gated = merged * jax.nn.sigmoid(og_ref[span, :].astype(F32))
        mx[tp, span, :] = gated.astype(BF)
    mx_far = [channel() for _ in range(1, nx)]
    mx_near = [channel() for _ in range(nx)]
    for d in range(1, nx):
        send(mx.at[tp], mx_far[d - 1], x_dev(d))
    send(mx.at[tp], mx_near[0], near)
    mark("exch_pump")
    turn(2)
    y_push()
    y_forward()
    mark("exch_far")
    for d in range(1, nx):
        slot = mx.at[same_core(-d)]
        arrived(slot, mx_far[d - 1], x_dev(-d))
        send(slot, mx_near[d], near)
    mark("exch_near")
    for d in range(nx):
        arrived(mx.at[other_core(-d)], mx_near[d], near)
    mark("exch_ow")
    ow_finish()
    mark("exch_pump2")
    turn(2)
    y_push()
    y_forward()

    mark("project")
    tile = min(256, width)
    tiles = width // tile
    lhs = jnp.concatenate([mx[g] for g in range(ntp)], axis=1)

    def project(n, square):
        cols = pl.ds(pl.multiple_of(n * tile, tile), tile)
        mix = dg(lhs, ow[:, :, cols].reshape(ntp * W2, tile)).astype(BF).astype(F32)
        after = (res[:, cols].astype(F32) + mix).astype(BF).astype(F32)
        am[:, cols] = after
        sq = after * after
        for q in range(tile // W2):
            square = square + sq[:, q * W2 : (q + 1) * W2]
        return square

    square = jnp.zeros((rows, W2), F32)
    square = lax.fori_loop(0, tiles, project, square)
    mark("norm")
    scale = lax.rsqrt(jnp.sum(square, axis=1, keepdims=True) * (1.0 / width) + NORM_EPS)

    def normalize(n, carry):
        cols = pl.ds(pl.multiple_of(n * tile, tile), tile)
        normed[:, cols] = (am[:, cols] * scale * gain_ref[:, cols]).astype(BF)
        return carry

    lax.fori_loop(0, tiles, normalize, 0)
    mark("pumprest")
    while progress["forward"] < len(across):
        turn()
        y_push(2)
        y_forward()
    mark("finish")
    for a in across:
        a.finish()

    mark("gateup")
    at = 0
    while at < ff:
        wide = min(256, ff - at)
        x = normed[...]
        gate = dg(x, gu[:, 0:half_f, at : at + wide].reshape(width, wide))
        up = dg(x, gu[:, half_f : 2 * half_f, at : at + wide].reshape(width, wide))
        hid[:, at : at + wide] = (gate / (1.0 + jnp.exp(-gate)) * up).astype(BF)
        at += wide
        turn()
    mark("dnwait")
    turn(3 * half_ring)

    slots = tile // half_f
    half_w = width // 2

    def down(n, carry):
        cols = pl.ds(pl.multiple_of(n * tile, tile), tile)
        w = dn[pl.ds(n * slots, slots)].reshape(tile, ff)
        prod = dg(hid[...], w, NT).reshape(nx, 2, own, tile).astype(BF)
        part[0, :, :, cols] = prod[:, 0]
        part[1, :, :, cols] = prod[:, 1]
        return carry

    def pass_on(src, dst, ch, device):
        c = copy(src, dst, ch, device)
        c.start()
        sent.append(c)

    pieces = [pl.ds(piece * half_w, half_w) for piece in range(2)]
    ch_core = [channel() for _ in range(2)]
    ch_part = [[channel() for _ in range(1, nx)] for _ in range(2)]
    for piece, cols in enumerate(pieces):
        mark(f"down{piece}")
        lax.fori_loop(piece * tiles // 2, (piece + 1) * tiles // 2, down, 0)
        pass_on(part.at[1 - core, :, :, cols], pgot.at[:, :, cols], ch_core[piece], near)

    def x_at(d):
        return lax.rem(xx + d + nx, nx)

    for piece, cols in enumerate(pieces):
        mark(f"rs_core{piece}")
        arrived(pgot.at[:, :, cols], ch_core[piece], near)
        for d in [2, 1, 3] if nx == 4 else range(1, nx):
            both = part[core, x_at(d), :, cols].astype(F32) + pgot[x_at(d), :, cols].astype(F32)
            comb[d - 1, :, cols] = both.astype(BF)
            pass_on(comb.at[d - 1, :, cols], got.at[d - 1, :, cols], ch_part[piece][d - 1], x_dev(d))
    mark("rs_wait")
    for piece, cols in enumerate(pieces):
        total = am[pl.ds(pl.multiple_of(tp * own, own), own), cols]
        total = total + part[core, xx, :, cols].astype(F32) + pgot[xx, :, cols].astype(F32)
        for d in range(1, nx):
            arrived(got.at[d - 1, :, cols], ch_part[piece][d - 1], x_dev(-d))
            total = total + got[d - 1, :, cols].astype(F32)
        out_ref[:, cols] = total.astype(BF)
    mark("sendwait")
    for c in sent:
        c.wait_send()
    mark(None)
    assert count[0] <= SEMS, count[0]


def per_device(
    nz,
    ny,
    ntp,
    receptance,
    head_keys,
    head_values,
    decay_preact,
    learning_rate_preact,
    output_gate_preact,
    self_token_weight,
    head_norm_gain,
    output_weight,
    residual,
    premixer_norm_gain,
    mixer_gate_weight,
    mixer_up_weight,
    mixer_down_weight,
):
    rows = receptance.shape[0]
    width = residual.shape[1]
    half_f, ff = mixer_gate_weight.shape
    own = rows // ntp
    nx = ntp // 2
    vmem = pl.BlockSpec(memory_space=pltpu.VMEM)
    hbm = pl.BlockSpec(memory_space=pl.ANY)
    return pl.pallas_call(
        functools.partial(kernel, nz, ny, ntp),
        out_shape=jax.ShapeDtypeStruct((own, width), BF),
        in_specs=[vmem] * 8 + [hbm, hbm, vmem, hbm, hbm, hbm],
        out_specs=vmem,
        scratch_shapes=[
            pltpu.VMEM((nz * ny, 2 * half_f, ff), BF),
            pltpu.VMEM((nz * ny, half_f, ff), BF),
            pltpu.VMEM((ntp, W2, width), BF),
            pltpu.VMEM((rows, width), BF),
            pltpu.VMEM((ny, W2, W2), F32),
            pltpu.VMEM((nz, W2, W2), F32),
            pltpu.VMEM((rows // CHUNK, W2, W2), F32),
            pltpu.VMEM((rows, W2), F32),
            pltpu.VMEM((rows, W2), F32),
            pltpu.VMEM((rows, W2), F32),
            pltpu.VMEM((ntp, rows, W2), BF),
            pltpu.VMEM((rows, width), F32),
            pltpu.VMEM((rows, width), BF),
            pltpu.VMEM((rows, ff), BF),
            pltpu.VMEM((2, nx, own, width), BF),
            pltpu.VMEM((max(nx - 1, 1), own, width), BF),
            pltpu.VMEM((nx, own, width), BF),
            pltpu.VMEM((max(nx - 1, 1), own, width), BF),
            pltpu.SemaphoreType.DMA((5,)),
            pltpu.SemaphoreType.DMA((SEMS,)),
            pltpu.SemaphoreType.DMA((SEMS,)),
        ],
        compiler_params=pltpu.CompilerParams(
            collective_id=0, has_side_effects=True, vmem_limit_bytes=60 * 1024 * 1024
        ),
        name="layer",
    )(
        receptance,
        head_keys,
        head_values,
        decay_preact,
        learning_rate_preact,
        output_gate_preact,
        self_token_weight.reshape(1, -1),
        head_norm_gain.reshape(1, -1),
        output_weight,
        residual,
        premixer_norm_gain.reshape(1, -1),
        mixer_gate_weight,
        mixer_up_weight,
        mixer_down_weight.T,
    )


def build(mesh, nz, ny):
    ntp = mesh.shape["tp"]
    torus = Mesh(mesh.devices.reshape(nz, ny, ntp), ("z", "y", "tp"))
    sp = ("z", "y")
    cut = P(sp, "tp")
    in_specs = (cut,) * 6 + (
        P("tp", None),
        P("tp"),
        P("tp", None),
        P(sp, None),
        P(),
        cut,
        cut,
        P("tp", sp),
    )
    return jax.shard_map(
        functools.partial(per_device, nz, ny, ntp),
        mesh=torus,
        in_specs=in_specs,
        out_specs=P(("z", "y", "tp"), None),
        check_vma=False,
    )


def solution(mesh):
    return build(mesh, 16, 4)
```

```python
import functools

import jax
import jax.numpy as jnp
from jax import lax
from jax.experimental import pallas as pl
from jax.experimental.pallas import tpu as pltpu
from jax.sharding import Mesh
from jax.sharding import PartitionSpec as P

HS = 64
CHUNK = 64
W2 = 2 * HS
GROUP_EPS = 0.00064
NORM_EPS = 1e-06
F32 = jnp.float32
BF = jnp.bfloat16
NN = (((1,), (0,)), ((), ()))
NT = (((1,), (1,)), ((), ()))
SEMS = 96


def dg(a, b, dims=NN):
    return lax.dot_general(a, b, dims, preferred_element_type=F32)


def halves(x):
    hi = x.astype(BF)
    return hi, (x - hi.astype(F32)).astype(BF)


def dot_halves(a, b, dims=NN):
    return dg(a[0], b[0], dims) + (dg(a[0], b[1], dims) + dg(a[1], b[0], dims))


def dot3(a, b, dims=NN):
    return dot_halves(halves(a), halves(b), dims)


def dot2(a, b, dims=NN):
    hi, lo = halves(a)
    return dg(hi, b, dims) + dg(lo, b, dims)


def iota(shape, dim):
    return lax.broadcasted_iota(jnp.int32, shape, dim)


def head_masks():
    lane = iota((1, W2), 1)
    first = (lane < HS).astype(F32)
    return first, 1.0 - first


def stacked(x):
    first, second = head_masks()
    return jnp.concatenate([x * first, x * second], axis=0)


def folded(x):
    half = x.shape[0] // 2
    return x[:half] + x[half:]


def head_ones():
    i, j = iota((W2, W2), 0), iota((W2, W2), 1)
    return ((i < HS) == (j < HS)).astype(BF)


def compose(earlier, later):
    moved = dot3(earlier, stacked(later[:HS]))
    return jnp.concatenate([moved[:HS], moved[HS:] + later[HS:]], axis=0)


def identity_pair():
    i, j = iota((W2, W2), 0), iota((W2, W2), 1)
    return ((i == j) | (i + HS == j)).astype(F32) * (i < HS).astype(F32)


def chunk_stages(chunks):
    i, j = iota((CHUNK, CHUNK), 0), iota((CHUNK, CHUNK), 1)
    tri = (i >= j).astype(BF)
    ones = head_ones()
    i, j = iota((W2, W2), 0), iota((W2, W2), 1)
    same = (i < HS) == (j < HS)
    strict = same & (i > j)
    incl = same & (i >= j)
    made = []
    for r, k, v, pre, lr in chunks:
        logw = jax.nn.sigmoid(pre) * (-0.6065306597126334)
        a1 = logw.astype(BF)
        a2, a3 = halves(logw - a1.astype(F32))
        cum = dg(tri, a1) + (dg(tri, a2) + dg(tri, a3))
        last = cum[CHUNK - 1 :, :]
        grown = jnp.exp(-cum)
        tail = jnp.exp(last - cum)
        unit = k / jnp.maximum(jnp.sqrt(dot2(k * k, ones)), 1.0)
        ins = unit * jax.nn.sigmoid(lr)
        us = stacked(-jnp.exp(cum - logw) * unit)
        rs = stacked(jnp.exp(cum) * r)
        made.append(
            dict(
                last=last,
                us=us,
                rs=rs,
                left=halves(jnp.concatenate([us, rs], axis=0)),
                right=halves(
                    jnp.concatenate([stacked(ins * grown), stacked(k * grown)], axis=0)
                ),
                bts=halves(stacked(ins * tail)),
                kts=halves(stacked(k * tail)),
                v=stacked(v),
            )
        )
    for m in made:
        gram = dot_halves(m["left"], m["right"], NT)
        m["lb"] = jnp.where(strict, gram[:W2, :W2], 0.0)
        m["lk"] = jnp.where(strict, gram[:W2, W2:], 0.0)
        m["mb"] = jnp.where(incl, gram[W2:, :W2], 0.0)
        m["mk"] = jnp.where(incl, gram[W2:, W2:], 0.0)
        m["vs"] = m["v"].astype(BF)
    for m in made:
        m["lkv"] = dot2(m["lk"], m["vs"])
        m["mkv"] = dot2(m["mk"], m["vs"])
    size = 1
    while size < CHUNK:
        row, col = i // size, j // size
        below = (row == col + 1) & (row % 2 == 1)
        if size == 1:
            for m in made:
                m["inv"] = (i == j).astype(F32) + jnp.where(below, m["lb"], 0.0)
        else:
            held = [halves(m["inv"]) for m in made]
            mid = [
                dot_halves(h, halves(jnp.where(below, m["lb"], 0.0))) for h, m in zip(held, made)
            ]
            for m, h, x in zip(made, held, mid):
                m["inv"] = m["inv"] + dot_halves(halves(x), h)
        size *= 2
    for m in made:
        m["tuv"] = dot3(m["inv"], jnp.concatenate([m["us"], m["lkv"]], axis=1))
    out = []
    for m in made:
        turned = dot_halves(halves(m["tuv"].T), m["bts"])
        trans = folded(jnp.where(i == j, jnp.exp(m["last"]), 0.0) + turned[:W2])
        vt = m["v"].T.astype(BF)
        state = folded(turned[W2:] + dg(vt, m["kts"][0]) + dg(vt, m["kts"][1]))
        m["pair"] = jnp.concatenate([trans, state], axis=0)
    for m in made:
        muv = dot_halves(halves(m["mb"]), halves(m["tuv"]))
        out.append(
            (m["pair"], folded(m["rs"] + muv[:, :W2]), folded(muv[:, W2:] + m["mkv"]))
        )
    return out


def kernel(
    nz,
    ny,
    ntp,
    r_in,
    k_in,
    v_in,
    pre_in,
    lr_in,
    og_in,
    stw_in,
    hg_in,
    ow_in,
    res_in,
    gain_in,
    gate_in,
    up_in,
    down_in,
    out_ref,
    r_ref,
    k_ref,
    v_ref,
    pre_ref,
    lr_ref,
    og_ref,
    stw_ref,
    hg_ref,
    gain_ref,
    gu,
    dn,
    ow,
    res,
    py,
    pz,
    entry,
    seen_ref,
    local_ref,
    self_ref,
    mx,
    am,
    normed,
    hid,
    part,
    got,
    pgot,
    comb,
    lsem,
    ssem,
    rsem,
):
    z, y, tp = lax.axis_index("z"), lax.axis_index("y"), lax.axis_index("tp")
    rows = r_in.shape[0]
    chunks = rows // CHUNK
    own = rows // ntp
    width = res_in.shape[1]
    half_f = gate_in.shape[0]
    ff = gate_in.shape[1]
    half_ring = nz // 2
    extra = half_f // 4
    nx = ntp // 2
    xx, core = tp // 2, tp % 2

    def zof(step):
        return lax.rem(z + step + nz, nz)

    def yof(step):
        return lax.rem(y + step + ny, ny)

    def tof(step):
        return lax.rem(tp + step + ntp, ntp)

    def sp(zz, yy):
        return zz * ny + yy

    def dev(zz=None, yy=None, tt=None):
        return {"z": z if zz is None else zz, "y": y if yy is None else yy, "tp": tp if tt is None else tt}

    scope = [None]

    def mark(name):
        if scope[0] is not None:
            scope[0].__exit__(None, None, None)
        scope[0] = None
        if name:
            scope[0] = jax.named_scope(name)
            scope[0].__enter__()

    mark("enter")
    here = sp(z, y)
    weights = [
        (gate_in, gu.at[here, 0:half_f]),
        (up_in, gu.at[here, half_f : 2 * half_f]),
        (down_in.at[0:extra], gu.at[here, 2 * half_f : 2 * half_f + extra]),
        (down_in.at[extra:half_f], dn.at[here]),
        (ow_in, ow.at[tp]),
    ]
    streams = [
        (k_in, k_ref),
        (pre_in, pre_ref),
        (lr_in, lr_ref),
        (r_in, r_ref),
        (v_in, v_ref),
        (og_in, og_ref),
        (stw_in, stw_ref),
        (hg_in, hg_ref),
        (gain_in, gain_ref),
        (res_in, res),
    ]
    loads = [
        pltpu.make_async_copy(src, dst, lsem.at[i])
        for i, (src, dst) in enumerate(weights + streams)
    ]
    for load in loads:
        load.start()

    barrier = pltpu.get_barrier_semaphore()
    peers = [dev(zz=zof(1)), dev(zz=zof(-1))]
    peers += [dev(yy=yof(d)) for d in range(1, ny)]
    peers += [dev(tt=tof(d)) for d in range(1, ntp)]
    for peer in peers:
        pl.semaphore_signal(barrier, inc=1, device_id=peer, device_id_type=pl.DeviceIdType.MESH)
    pl.semaphore_wait(barrier, len(peers))
    for load in loads[: len(weights)]:
        load.wait()

    count = [0]

    def channel():
        count[0] += 1
        return count[0] - 1

    def copy(src, dst, out, ch, device):
        return pltpu.make_async_remote_copy(
            src_ref=src,
            dst_ref=dst,
            send_sem=ssem.at[out],
            recv_sem=rsem.at[ch],
            device_id=device,
            device_id_type=pl.DeviceIdType.MESH,
        )

    GU, DN, PS, PY, OW, MX, PART, COMB = range(8)

    def send(ref, out, ch, device):
        copy(ref, ref, out, ch, device).start()

    def arrived(ref, ch):
        copy(ref, ref, 0, ch, dev(zz=zof(1))).wait_recv()

    class Ring:
        def __init__(self, block, out, one, two):
            self.block, self.out, self.one, self.two = block, out, one, two
            self.ch = [channel() for _ in range(half_ring)]
            self.step = 1

        def piece(self, s, side):
            return side if s == half_ring else None

        def push(self, s):
            ch = self.ch[s - 1]
            send(self.block(zof(1 - s), self.piece(s, 0)), self.out, ch, dev(zz=zof(1)))
            send(self.block(zof(s - 1), self.piece(s, 1)), self.out, ch, dev(zz=zof(-1)))

        def turn(self):
            s = self.step
            if s > half_ring:
                return
            arrived(self.one if s == half_ring else self.two, self.ch[s - 1])
            if s < half_ring:
                self.push(s + 1)
            self.step = s + 1

    class PairRing:
        def __init__(self):
            self.ch = [(channel(), channel()) for _ in range(half_ring)]

        def part(self, zz, half):
            return pz.at[zz, half * HS : (half + 1) * HS]

        def push(self, s, half):
            ch = self.ch[s - 1][half]
            if s < half_ring or half == 0:
                send(self.part(zof(1 - s), half), PS, ch, dev(zz=zof(1)))
            if s < half_ring or half == 1:
                send(self.part(zof(s - 1), half), PS, ch, dev(zz=zof(-1)))

        def turn(self, s):
            for half in range(2):
                arrived(pz.at[0] if s < half_ring else self.part(0, half), self.ch[s - 1][half])
                if s < half_ring:
                    self.push(s + 1, half)

    class Across:
        def __init__(self, block, at, to, out, one, two, last=None):
            self.block, self.at, self.to, self.out = block, at, to, out
            self.one, self.two = one, two
            self.first = channel()
            self.last = channel() if last is None else last

        def push(self):
            send(self.block(self.at(0), None), self.out, self.first, self.to(1))
            send(self.block(self.at(0), None), self.out, self.first, self.to(-1))

        def forward(self):
            arrived(self.two, self.first)
            send(self.block(self.at(-1), 0), self.out, self.last, self.to(1))
            send(self.block(self.at(1), 1), self.out, self.last, self.to(-1))

        def finish(self):
            arrived(self.one, self.last)

    def cut(ref, piece, length):
        if piece is None:
            return ref
        middle = (length // 2 + 7) // 8 * 8
        return ref.at[0:middle] if piece == 0 else ref.at[middle:length]

    a_rows = 2 * half_f + extra
    b_rows = half_f - extra

    def gu_block(zz, yy, piece):
        return cut(gu.at[sp(zz, yy)], piece, a_rows)

    def dn_block(zz, yy, piece):
        return cut(dn.at[sp(zz, yy)], piece, b_rows)

    def y_dev(d):
        return dev(yy=yof(d))

    ring_gu = Ring(lambda zz, piece: gu_block(zz, y, piece), GU, gu.at[0], gu.at[0:2])
    ring_dn = [
        Ring(
            functools.partial(lambda k, zz, piece: dn_block(zz, yof(k), piece), k),
            DN,
            dn.at[0],
            dn.at[0:2],
        )
        for k in (0, 1, -1, 2)
    ]
    ring_ps = PairRing()
    order = [0]
    for s in range(1, half_ring):
        order += [-s, s]
    order += [half_ring]
    far_halves = channel()
    across = [
        Across(
            functools.partial(lambda step, yy, piece: gu_block(zof(step), yy, piece), step),
            yof,
            y_dev,
            GU,
            gu.at[0:nz],
            gu.at[0:2],
            far_halves,
        )
        for step in order
    ]
    across_dn = Across(
        lambda yy, piece: dn_block(z, yy, piece), yof, y_dev, DN, dn.at[0], dn.at[0:2]
    )

    progress = {"push": 1, "forward": 0, "dn": 0}

    def turn_gu():
        ring_gu.turn()

    def turn_dn(n=1):
        for _ in range(n):
            ring_dn[progress["dn"] % 4].turn()
            progress["dn"] += 1

    def y_push(n=1):
        for _ in range(n):
            i = progress["push"]
            if i < len(across) and (i + 1) // 2 < ring_gu.step:
                across[i].push()
                progress["push"] += 1

    def y_forward(n=1):
        for _ in range(n):
            if progress["forward"] < progress["push"]:
                across[progress["forward"]].forward()
                progress["forward"] += 1

    def same_core(d):
        return lax.rem(xx + d + nx, nx) * 2 + core

    def other_core(d):
        return lax.rem(xx + d + nx, nx) * 2 + (1 - core)

    def x_dev(d):
        return dev(tt=same_core(d))

    partner = other_core(0)
    near = dev(tt=partner)
    across_ow = None
    if nx == 4:
        across_ow = Across(
            lambda t, piece: cut(ow.at[t], piece, W2),
            same_core,
            x_dev,
            OW,
            ow.at[0],
            ow.at[0:2],
        )
    ow_far = [channel() for _ in range(1, nx)] if across_ow is None else []
    ow_near = channel()

    def ow_share(d):
        send(ow.at[same_core(d)], OW, ow_near, near)

    def ow_start():
        if across_ow is not None:
            across_ow.push()
        else:
            for d in range(1, nx):
                send(ow.at[tp], OW, ow_far[d - 1], x_dev(d))
        ow_share(0)

    def ow_middle():
        if across_ow is not None:
            across_ow.forward()
            ow_share(1)
            ow_share(-1)

    def ow_last():
        if across_ow is not None:
            across_ow.finish()
            ow_share(2)
        else:
            for d in range(1, nx):
                arrived(ow.at[0], ow_far[d - 1])
                ow_share(-d)

    def ow_finish():
        arrived(ow.at[0:nx], ow_near)

    mark("launch")
    ring_gu.push(1)
    ring_dn[0].push(1)
    across_dn.push()
    across[0].push()
    ow_start()
    for load in loads[len(weights) :]:
        load.wait()

    mark("recur")
    ones = head_ones()
    spans = [pl.ds(c * CHUNK, CHUNK) for c in range(chunks)]
    given = []
    for span in spans:
        r, k, v = (ref[span, :].astype(F32) for ref in (r_ref, k_ref, v_ref))
        given.append((r, k, v, pre_ref[span, :], lr_ref[span, :]))
    made = chunk_stages(given)
    pair = None
    for c, (ps, seen, local) in enumerate(made):
        seen_ref[spans[c], :] = seen
        local_ref[spans[c], :] = local
        pair = ps if pair is None else compose(pair, ps)
        if c < chunks - 1:
            entry[c] = pair
    mark("scan_y")
    py[y] = pair
    ch_y = channel()
    for d in (2, 1, 3) if ny == 4 else range(1, ny):
        send(py.at[y], PY, ch_y, dev(yy=yof(d)))
    mark("pre_gu")
    turn_gu()
    mark("pre_dn")
    ring_dn[0].turn()
    mark("pre_dny")
    across_dn.forward()
    ring_dn[1].push(1)
    ring_dn[2].push(1)
    stw = stw_ref[...]
    stw = jnp.concatenate([stw[0:1], stw[1:2]], axis=1)
    for c, (r, k, v, _, _) in enumerate(given):
        self_ref[spans[c], :] = dot2(r * k * stw, ones) * v
    mark("pre_y0")
    y_forward()
    y_push()
    mark("scan_ywait")
    arrived(py.at[0 : ny - 1], ch_y)
    mark("scan_yfix")
    inside = identity_pair()
    running = py[0]
    for yy in range(1, ny):
        inside = jnp.where(y == yy, running, inside)
        running = compose(running, py[yy])
    pz[z] = running
    ring_ps.push(1, 0)
    ring_ps.push(1, 1)
    mark("pre_dn2")
    across_dn.finish()
    ring_dn[3].push(1)
    y_push()
    progress["dn"] = 1

    trans_left = identity_pair()[:HS]
    state_left = jnp.zeros((HS, W2), F32)
    state_right = jnp.zeros((HS, W2), F32)
    for s in range(1, half_ring + 1):
        mark(f"scan_z{s}")
        ring_ps.turn(s)
        mark(f"bulk{s}")
        if s % 2 == 1:
            turn_gu()
            turn_dn()
        else:
            turn_dn(3)
        y_push()
        mark(f"yfwd{s}")
        y_forward()
        mark(f"calc{s}")
        if s == half_ring // 2:
            ow_middle()
        if s == half_ring - 1:
            ow_last()
        left = pz[zof(-s)]
        has_left = z >= s
        moved = dot3(left, stacked(trans_left))
        trans_left = jnp.where(has_left, moved[:HS], trans_left)
        state_left = jnp.where(has_left, state_left + moved[HS:], state_left)
        if s < half_ring:
            right = pz[zof(s)]
            has_right = z + s >= nz
            state_right = jnp.where(
                has_right, dot3(state_right, stacked(right[:HS])) + right[HS:], state_right
            )
    mark("state")
    state = dot3(state_right, stacked(trans_left)) + state_left
    state = dot3(state, stacked(inside[:HS])) + inside[HS:]

    turn_gu()
    y_push()
    mark("mech")
    for c in range(chunks):
        span = spans[c]
        at = state
        if c > 0:
            at = dot3(state, stacked(entry[c - 1][:HS])) + entry[c - 1][HS:]
        o = dot3(seen_ref[span, :], stacked(at), NT) + local_ref[span, :]
        centre = dot2(o, ones) * (1.0 / HS)
        shifted = o - centre
        spread = dot2(shifted * shifted, ones) * (1.0 / HS)
        merged = shifted * lax.rsqrt(spread + GROUP_EPS) * hg_ref[...] + self_ref[span, :]
        gated = merged * jax.nn.sigmoid(og_ref[span, :].astype(F32))
        mx[tp, span, :] = gated.astype(BF)
    mx_far = [channel() for _ in range(1, nx)]
    mx_near = channel()
    for d in range(1, nx):
        send(mx.at[tp], MX, mx_far[d - 1], x_dev(d))
    send(mx.at[tp], MX, mx_near, near)
    mark("exch_pump")
    turn_dn(3)
    y_push()
    y_forward()
    mark("exch_far")
    for d in range(1, nx):
        arrived(mx.at[0], mx_far[d - 1])
        send(mx.at[same_core(-d)], MX, mx_near, near)
    mark("exch_pump2")
    turn_gu()
    y_push()
    turn_dn()
    y_forward()
    mark("exch_near")
    arrived(mx.at[0:nx], mx_near)
    mark("exch_ow")
    ow_finish()
    mark("exch_pump3")
    turn_dn(3)
    y_push(2)
    y_forward()

    mark("project")
    tile = min(256, width)
    tiles = width // tile
    lhs = jnp.concatenate([mx[g] for g in range(ntp)], axis=1)

    def project(n, square):
        cols = pl.ds(pl.multiple_of(n * tile, tile), tile)
        mix = dg(lhs, ow[:, :, cols].reshape(ntp * W2, tile)).astype(BF).astype(F32)
        after = (res[:, cols].astype(F32) + mix).astype(BF).astype(F32)
        am[:, cols] = after
        sq = after * after
        for q in range(tile // W2):
            square = square + sq[:, q * W2 : (q + 1) * W2]
        return square

    square = jnp.zeros((rows, W2), F32)
    square = lax.fori_loop(0, tiles, project, square)
    mark("norm")
    turn_gu()
    y_push(2)
    turn_dn(2)
    y_forward()
    scale = lax.rsqrt(jnp.sum(square, axis=1, keepdims=True) * (1.0 / width) + NORM_EPS)

    def normalize(n, carry):
        cols = pl.ds(pl.multiple_of(n * tile, tile), tile)
        normed[:, cols] = (am[:, cols] * scale * gain_ref[:, cols]).astype(BF)
        return carry

    lax.fori_loop(0, tiles, normalize, 0)
    mark("pumprest")
    while progress["forward"] < len(across):
        turn_gu()
        y_push(2)
        turn_dn(2)
        y_forward()
    mark("finish")
    across[0].finish()

    mark("gateup")
    at = 0
    while at < ff:
        wide = min(256, ff - at)
        x = normed[...]
        gate = dg(x, gu[:, 0:half_f, at : at + wide].reshape(width, wide))
        up = dg(x, gu[:, half_f : 2 * half_f, at : at + wide].reshape(width, wide))
        hid[:, at : at + wide] = (gate / (1.0 + jnp.exp(-gate)) * up).astype(BF)
        at += wide
        turn_dn(2)
    mark("dnwait")
    turn_dn(4 * half_ring)

    slots = tile // half_f
    half_w = width // 2

    def down(n, carry):
        cols = pl.ds(pl.multiple_of(n * tile, tile), tile)
        these = pl.ds(n * slots, slots)
        first = gu[these, 2 * half_f : 2 * half_f + extra, :]
        w = jnp.concatenate([first, dn[these]], axis=1).reshape(tile, ff)
        prod = dg(hid[...], w, NT).reshape(nx, 2, own, tile).astype(BF)
        part[0, :, :, cols] = prod[:, 0]
        part[1, :, :, cols] = prod[:, 1]
        return carry

    pieces = [pl.ds(piece * half_w, half_w) for piece in range(2)]
    ch_core = [channel() for _ in range(2)]
    ch_part = [channel() for _ in range(2)]
    for piece, cols in enumerate(pieces):
        mark(f"down{piece}")
        lax.fori_loop(piece * tiles // 2, (piece + 1) * tiles // 2, down, 0)
        copy(
            part.at[1 - core, :, :, cols], pgot.at[:, :, cols], PART, ch_core[piece], near
        ).start()

    def x_at(d):
        return lax.rem(xx + d + nx, nx)

    for piece, cols in enumerate(pieces):
        mark(f"rs_core{piece}")
        arrived(pgot.at[:, :, cols], ch_core[piece])
        for d in [2, 1, 3] if nx == 4 else range(1, nx):
            both = part[core, x_at(d), :, cols].astype(F32) + pgot[x_at(d), :, cols].astype(F32)
            comb[d - 1, :, cols] = both.astype(BF)
            copy(
                comb.at[d - 1, :, cols], got.at[d - 1, :, cols], COMB, ch_part[piece], x_dev(d)
            ).start()
    mark("rs_wait")
    for piece, cols in enumerate(pieces):
        total = am[pl.ds(pl.multiple_of(tp * own, own), own), cols]
        total = total + part[core, xx, :, cols].astype(F32) + pgot[xx, :, cols].astype(F32)
        if nx > 1:
            arrived(got.at[:, :, cols], ch_part[piece])
        for d in range(1, nx):
            total = total + got[d - 1, :, cols].astype(F32)
        out_ref[:, cols] = total.astype(BF)
    mark("sendwait")
    gone = [
        (gu.at[0 : nz * ny - 1], GU),
        (dn.at[0 : nz * ny - 1], DN),
        (pz.at[0 : nz - 1], PS),
        (py.at[0 : ny - 1], PY),
        (ow.at[0 : ntp - 1], OW),
        (mx.at[0 : ntp - 1], MX),
        (part.at[0], PART),
    ]
    if nx > 1:
        gone.append((comb, COMB))
    for ref, out in gone:
        copy(ref, ref, out, 0, near).wait_send()
    mark(None)
    assert count[0] <= SEMS, count[0]


def per_device(
    nz,
    ny,
    ntp,
    receptance,
    head_keys,
    head_values,
    decay_preact,
    learning_rate_preact,
    output_gate_preact,
    self_token_weight,
    head_norm_gain,
    output_weight,
    residual,
    premixer_norm_gain,
    mixer_gate_weight,
    mixer_up_weight,
    mixer_down_weight,
):
    rows = receptance.shape[0]
    width = residual.shape[1]
    half_f, ff = mixer_gate_weight.shape
    own = rows // ntp
    nx = ntp // 2
    vmem = pl.BlockSpec(memory_space=pltpu.VMEM)
    hbm = pl.BlockSpec(memory_space=pl.ANY)
    return pl.pallas_call(
        functools.partial(kernel, nz, ny, ntp),
        out_shape=jax.ShapeDtypeStruct((own, width), BF),
        in_specs=[hbm] * 14,
        out_specs=vmem,
        scratch_shapes=[
            pltpu.VMEM((rows, W2), BF),
            pltpu.VMEM((rows, W2), BF),
            pltpu.VMEM((rows, W2), BF),
            pltpu.VMEM((rows, W2), F32),
            pltpu.VMEM((rows, W2), F32),
            pltpu.VMEM((rows, W2), BF),
            pltpu.VMEM((2, HS), F32),
            pltpu.VMEM((1, W2), F32),
            pltpu.VMEM((1, width), F32),
            pltpu.VMEM((nz * ny, 2 * half_f + half_f // 4, ff), BF),
            pltpu.VMEM((nz * ny, half_f - half_f // 4, ff), BF),
            pltpu.VMEM((ntp, W2, width), BF),
            pltpu.VMEM((rows, width), BF),
            pltpu.VMEM((ny, W2, W2), F32),
            pltpu.VMEM((nz, W2, W2), F32),
            pltpu.VMEM((rows // CHUNK, W2, W2), F32),
            pltpu.VMEM((rows, W2), F32),
            pltpu.VMEM((rows, W2), F32),
            pltpu.VMEM((rows, W2), F32),
            pltpu.VMEM((ntp, rows, W2), BF),
            pltpu.VMEM((rows, width), F32),
            pltpu.VMEM((rows, width), BF),
            pltpu.VMEM((rows, ff), BF),
            pltpu.VMEM((2, nx, own, width), BF),
            pltpu.VMEM((max(nx - 1, 1), own, width), BF),
            pltpu.VMEM((nx, own, width), BF),
            pltpu.VMEM((max(nx - 1, 1), own, width), BF),
            pltpu.SemaphoreType.DMA((15,)),
            pltpu.SemaphoreType.DMA((8,)),
            pltpu.SemaphoreType.DMA((SEMS,)),
        ],
        compiler_params=pltpu.CompilerParams(
            collective_id=0, has_side_effects=True, vmem_limit_bytes=60 * 1024 * 1024
        ),
        name="layer",
    )(
        receptance,
        head_keys,
        head_values,
        decay_preact,
        learning_rate_preact,
        output_gate_preact,
        self_token_weight,
        head_norm_gain.reshape(1, -1),
        output_weight,
        residual,
        premixer_norm_gain.reshape(1, -1),
        mixer_gate_weight,
        mixer_up_weight,
        mixer_down_weight.T,
    )


def build(mesh, nz, ny):
    ntp = mesh.shape["tp"]
    torus = Mesh(mesh.devices.reshape(nz, ny, ntp), ("z", "y", "tp"))
    sp = ("z", "y")
    cut = P(sp, "tp")
    in_specs = (cut,) * 6 + (
        P("tp", None),
        P("tp"),
        P("tp", None),
        P(sp, None),
        P(),
        cut,
        cut,
        P("tp", sp),
    )
    return jax.shard_map(
        functools.partial(per_device, nz, ny, ntp),
        mesh=torus,
        in_specs=in_specs,
        out_specs=P(("z", "y", "tp"), None),
        check_vma=False,
    )


def solution(mesh):
    return build(mesh, 16, 4)
```

```python
import functools

import jax
import jax.numpy as jnp
from jax import lax
from jax.experimental import pallas as pl
from jax.experimental.pallas import tpu as pltpu
from jax.sharding import Mesh
from jax.sharding import PartitionSpec as P

HS = 64
CHUNK = 64
W2 = 2 * HS
GROUP_EPS = 0.00064
NORM_EPS = 1e-06
F32 = jnp.float32
BF = jnp.bfloat16
NN = (((1,), (0,)), ((), ()))
NT = (((1,), (1,)), ((), ()))
SEMS = 96


def dg(a, b, dims=NN):
    return lax.dot_general(a, b, dims, preferred_element_type=F32)


def halves(x):
    hi = x.astype(BF)
    return hi, (x - hi.astype(F32)).astype(BF)


def dot_halves(a, b, dims=NN):
    return dg(a[0], b[0], dims) + (dg(a[0], b[1], dims) + dg(a[1], b[0], dims))


def dot3(a, b, dims=NN):
    return dot_halves(halves(a), halves(b), dims)


def dot2(a, b, dims=NN):
    hi, lo = halves(a)
    return dg(hi, b, dims) + dg(lo, b, dims)


def iota(shape, dim):
    return lax.broadcasted_iota(jnp.int32, shape, dim)


def head_masks():
    lane = iota((1, W2), 1)
    first = (lane < HS).astype(F32)
    return first, 1.0 - first


def stacked(x):
    first, second = head_masks()
    return jnp.concatenate([x * first, x * second], axis=0)


def folded(x):
    half = x.shape[0] // 2
    return x[:half] + x[half:]


def head_ones():
    i, j = iota((W2, W2), 0), iota((W2, W2), 1)
    return ((i < HS) == (j < HS)).astype(BF)


def compose(earlier, later):
    later_d = stacked(later[:HS])
    i, j = iota((W2, W2), 0), iota((W2, W2), 1)
    moved = dot3(earlier, later_d + (i == j).astype(F32))
    return jnp.concatenate([moved[:HS] + later[:HS], moved[HS:] + later[HS:]], axis=0)


def chunk_stages(chunks):
    i, j = iota((CHUNK, CHUNK), 0), iota((CHUNK, CHUNK), 1)
    tri = (i >= j).astype(BF)
    ones = head_ones()
    i, j = iota((W2, W2), 0), iota((W2, W2), 1)
    same = (i < HS) == (j < HS)
    strict = same & (i > j)
    incl = same & (i >= j)
    made = []
    for r, k, v, pre, lr in chunks:
        logw = jax.nn.sigmoid(pre) * (-0.6065306597126334)
        a1 = logw.astype(BF)
        a2, a3 = halves(logw - a1.astype(F32))
        cum = dg(tri, a1) + (dg(tri, a2) + dg(tri, a3))
        last = cum[CHUNK - 1 :, :]
        grown = jnp.exp(-cum)
        tail = jnp.exp(last - cum)
        unit = k / jnp.maximum(jnp.sqrt(dot2(k * k, ones)), 1.0)
        ins = unit * jax.nn.sigmoid(lr)
        us = stacked(-jnp.exp(cum - logw) * unit)
        rs = stacked(jnp.exp(cum) * r)
        made.append(
            dict(
                last=last,
                us=us,
                rs=rs,
                left=halves(jnp.concatenate([us, rs], axis=0)),
                right=halves(
                    jnp.concatenate([stacked(ins * grown), stacked(k * grown)], axis=0)
                ),
                bts=halves(stacked(ins * tail)),
                kts=halves(stacked(k * tail)),
                v=stacked(v),
            )
        )
    for m in made:
        gram = dot_halves(m["left"], m["right"], NT)
        m["lb"] = jnp.where(strict, gram[:W2, :W2], 0.0)
        m["lk"] = jnp.where(strict, gram[:W2, W2:], 0.0)
        m["mb"] = jnp.where(incl, gram[W2:, :W2], 0.0)
        m["mk"] = jnp.where(incl, gram[W2:, W2:], 0.0)
        m["vs"] = m["v"].astype(BF)
    yield
    for m in made:
        m["lkv"] = dot2(m["lk"], m["vs"])
        m["mkv"] = dot2(m["mk"], m["vs"])
    size = 1
    while size < CHUNK:
        row, col = i // size, j // size
        below = (row == col + 1) & (row % 2 == 1)
        if size == 1:
            for m in made:
                m["inv"] = (i == j).astype(F32) + jnp.where(below, m["lb"], 0.0)
        else:
            held = [halves(m["inv"]) for m in made]
            mid = [
                dot_halves(h, halves(jnp.where(below, m["lb"], 0.0))) for h, m in zip(held, made)
            ]
            for m, h, x in zip(made, held, mid):
                m["inv"] = m["inv"] + dot_halves(halves(x), h)
        size *= 2
    for m in made:
        m["tuv"] = dot3(m["inv"], jnp.concatenate([m["us"], m["lkv"]], axis=1))
    out = []
    for m in made:
        turned = dot_halves(halves(m["tuv"].T), m["bts"])
        trans = folded(jnp.where(i == j, jnp.exp(m["last"]) - 1.0, 0.0) + turned[:W2])
        vt = m["v"].T.astype(BF)
        state = folded(turned[W2:] + dg(vt, m["kts"][0]) + dg(vt, m["kts"][1]))
        m["pair"] = jnp.concatenate([trans, state], axis=0)
    for m in made:
        muv = dot_halves(halves(m["mb"]), halves(m["tuv"]))
        out.append(
            (m["pair"], folded(m["rs"] + muv[:, :W2]), folded(muv[:, W2:] + m["mkv"]))
        )
    return out


def kernel(
    nz,
    ny,
    ntp,
    r_in,
    k_in,
    v_in,
    pre_in,
    lr_in,
    og_in,
    stw_in,
    hg_in,
    ow_in,
    res_in,
    gain_in,
    gate_in,
    up_in,
    down_in,
    out_ref,
    r_ref,
    k_ref,
    v_ref,
    pre_ref,
    lr_ref,
    og_ref,
    stw_ref,
    hg_ref,
    gain_ref,
    gu,
    dn,
    ow,
    res,
    py,
    pz,
    entry,
    seen_ref,
    local_ref,
    self_ref,
    mx,
    am,
    normed,
    hid,
    part,
    got,
    pgot,
    comb,
    lsem,
    ssem,
    rsem,
):
    z, y, tp = lax.axis_index("z"), lax.axis_index("y"), lax.axis_index("tp")
    rows = r_in.shape[0]
    chunks = rows // CHUNK
    own = rows // ntp
    width = res_in.shape[1]
    half_f = gate_in.shape[0]
    ff = gate_in.shape[1]
    half_ring = nz // 2
    nx = ntp // 2
    xx, core = tp // 2, tp % 2

    def zof(step):
        return lax.rem(z + step + nz, nz)

    def yof(step):
        return lax.rem(y + step + ny, ny)

    def tof(step):
        return lax.rem(tp + step + ntp, ntp)

    def sp(zz, yy):
        return zz * ny + yy

    def dev(zz=None, yy=None, tt=None):
        return {"z": z if zz is None else zz, "y": y if yy is None else yy, "tp": tp if tt is None else tt}

    scope = [None]

    def mark(name):
        if scope[0] is not None:
            scope[0].__exit__(None, None, None)
        scope[0] = None
        if name:
            scope[0] = jax.named_scope(name)
            scope[0].__enter__()

    mark("enter")
    here = sp(z, y)
    weights = [
        (gate_in, gu.at[here, 0:half_f]),
        (up_in, gu.at[here, half_f : 2 * half_f]),
        (down_in, dn.at[here]),
        (ow_in, ow.at[tp]),
    ]
    streams = [
        (pre_in, pre_ref),
        (k_in, k_ref),
        (lr_in, lr_ref),
        (r_in, r_ref),
        (v_in, v_ref),
        (og_in, og_ref),
        (stw_in, stw_ref),
        (hg_in, hg_ref),
        (gain_in, gain_ref),
        (res_in, res),
    ]
    loads = [
        pltpu.make_async_copy(src, dst, lsem.at[i])
        for i, (src, dst) in enumerate(weights + streams)
    ]
    for load in loads[len(weights) :] + loads[: len(weights)]:
        load.start()

    barrier = pltpu.get_barrier_semaphore()
    peers = [dev(zz=zof(1)), dev(zz=zof(-1))]
    peers += [dev(yy=yof(d)) for d in range(1, ny)]
    peers += [dev(tt=tof(d)) for d in range(1, ntp)]
    for peer in peers:
        pl.semaphore_signal(barrier, inc=1, device_id=peer, device_id_type=pl.DeviceIdType.MESH)
    early = len(weights) + 5
    for load in loads[len(weights) : early]:
        load.wait()
    mark("recur_a")
    spans = [pl.ds(c * CHUNK, CHUNK) for c in range(chunks)]
    given = []
    for span in spans:
        r, k, v = (ref[span, :].astype(F32) for ref in (r_ref, k_ref, v_ref))
        given.append((r, k, v, pre_ref[span, :], lr_ref[span, :]))
    stages = chunk_stages(given)
    next(stages)
    mark("greet")
    pl.semaphore_wait(barrier, len(peers))
    for load in loads[: len(weights)]:
        load.wait()

    count = [0]

    def channel():
        count[0] += 1
        return count[0] - 1

    def copy(src, dst, out, ch, device):
        return pltpu.make_async_remote_copy(
            src_ref=src,
            dst_ref=dst,
            send_sem=ssem.at[out],
            recv_sem=rsem.at[ch],
            device_id=device,
            device_id_type=pl.DeviceIdType.MESH,
        )

    GU, DN, PS, PY, OW, MX, PART, COMB = range(8)

    def send(ref, out, ch, device):
        copy(ref, ref, out, ch, device).start()

    def arrived(ref, ch):
        copy(ref, ref, 0, ch, dev(zz=zof(1))).wait_recv()

    class Ring:
        def __init__(self, block, out, one, two):
            self.block, self.out, self.one, self.two = block, out, one, two
            self.ch = [channel() for _ in range(half_ring)]
            self.step = 1

        def piece(self, s, side):
            return side if s == half_ring else None

        def push(self, s):
            ch = self.ch[s - 1]
            send(self.block(zof(1 - s), self.piece(s, 0)), self.out, ch, dev(zz=zof(1)))
            send(self.block(zof(s - 1), self.piece(s, 1)), self.out, ch, dev(zz=zof(-1)))

        def turn(self):
            s = self.step
            if s > half_ring:
                return
            arrived(self.one if s == half_ring else self.two, self.ch[s - 1])
            if s < half_ring:
                self.push(s + 1)
            self.step = s + 1

    class PairRing:
        def __init__(self):
            self.ch = [(channel(), channel()) for _ in range(half_ring)]

        def part(self, zz, half):
            return pz.at[zz, half * HS : (half + 1) * HS]

        def push(self, s, half):
            ch = self.ch[s - 1][half]
            if s < half_ring or half == 0:
                send(self.part(zof(1 - s), half), PS, ch, dev(zz=zof(1)))
            if s < half_ring or half == 1:
                send(self.part(zof(s - 1), half), PS, ch, dev(zz=zof(-1)))

        def turn(self, s):
            for half in range(2):
                arrived(pz.at[0] if s < half_ring else self.part(0, half), self.ch[s - 1][half])
                if s < half_ring:
                    self.push(s + 1, half)

    class Across:
        def __init__(self, block, at, to, out, one, two, last=None):
            self.block, self.at, self.to, self.out = block, at, to, out
            self.one, self.two = one, two
            self.first = channel()
            self.last = channel() if last is None else last

        def push(self):
            send(self.block(self.at(0), None), self.out, self.first, self.to(1))
            send(self.block(self.at(0), None), self.out, self.first, self.to(-1))

        def forward(self):
            arrived(self.two, self.first)
            send(self.block(self.at(-1), 0), self.out, self.last, self.to(1))
            send(self.block(self.at(1), 1), self.out, self.last, self.to(-1))

        def finish(self):
            arrived(self.one, self.last)

    def cut(ref, piece, length):
        if piece is None:
            return ref
        middle = (length // 2 + 7) // 8 * 8
        return ref.at[0:middle] if piece == 0 else ref.at[middle:length]

    a_rows = 2 * half_f
    b_rows = half_f

    def gu_block(zz, yy, piece):
        return cut(gu.at[sp(zz, yy)], piece, a_rows)

    def dn_block(zz, yy, piece):
        return cut(dn.at[sp(zz, yy)], piece, b_rows)

    def y_dev(d):
        return dev(yy=yof(d))

    ring_gu = Ring(lambda zz, piece: gu_block(zz, y, piece), GU, gu.at[0], gu.at[0:2])
    ring_dn = [
        Ring(
            functools.partial(lambda k, zz, piece: dn_block(zz, yof(k), piece), k),
            DN,
            dn.at[0],
            dn.at[0:2],
        )
        for k in (0, 1, -1, 2)
    ]
    ring_ps = PairRing()
    order = [0]
    for s in range(1, half_ring):
        order += [-s, s]
    order += [half_ring]
    far_halves = channel()
    across = [
        Across(
            functools.partial(lambda step, yy, piece: gu_block(zof(step), yy, piece), step),
            yof,
            y_dev,
            GU,
            gu.at[0:nz],
            gu.at[0:2],
            far_halves,
        )
        for step in order
    ]
    across_dn = Across(
        lambda yy, piece: dn_block(z, yy, piece), yof, y_dev, DN, dn.at[0], dn.at[0:2]
    )

    progress = {"push": 1, "forward": 0, "dn": 0}

    def turn_gu():
        ring_gu.turn()

    def turn_dn(n=1):
        for _ in range(n):
            ring_dn[progress["dn"] % 4].turn()
            progress["dn"] += 1

    def y_push(n=1):
        for _ in range(n):
            i = progress["push"]
            if i < len(across) and (i + 1) // 2 < ring_gu.step:
                across[i].push()
                progress["push"] += 1

    def y_forward(n=1):
        for _ in range(n):
            if progress["forward"] < progress["push"]:
                across[progress["forward"]].forward()
                progress["forward"] += 1

    def same_core(d):
        return lax.rem(xx + d + nx, nx) * 2 + core

    def other_core(d):
        return lax.rem(xx + d + nx, nx) * 2 + (1 - core)

    def x_dev(d):
        return dev(tt=same_core(d))

    partner = other_core(0)
    near = dev(tt=partner)
    across_ow = None
    if nx == 4:
        across_ow = Across(
            lambda t, piece: cut(ow.at[t], piece, W2),
            same_core,
            x_dev,
            OW,
            ow.at[0],
            ow.at[0:2],
        )
    ow_far = [channel() for _ in range(1, nx)] if across_ow is None else []
    ow_near = channel()

    def ow_share(d):
        send(ow.at[same_core(d)], OW, ow_near, near)

    def ow_start():
        if across_ow is not None:
            across_ow.push()
        else:
            for d in range(1, nx):
                send(ow.at[tp], OW, ow_far[d - 1], x_dev(d))
        ow_share(0)

    def ow_middle():
        if across_ow is not None:
            across_ow.forward()
            ow_share(1)
            ow_share(-1)

    def ow_last():
        if across_ow is not None:
            across_ow.finish()
            ow_share(2)
        else:
            for d in range(1, nx):
                arrived(ow.at[0], ow_far[d - 1])
                ow_share(-d)

    def ow_finish():
        arrived(ow.at[0:nx], ow_near)

    mark("launch")
    ring_gu.push(1)
    ring_dn[0].push(1)
    across_dn.push()
    across[0].push()
    ow_start()
    for load in loads[early:]:
        load.wait()

    mark("recur")
    ones = head_ones()
    try:
        next(stages)
    except StopIteration as end:
        made = end.value
    pair = None
    for c, (ps, seen, local) in enumerate(made):
        seen_ref[spans[c], :] = seen
        local_ref[spans[c], :] = local
        pair = ps if pair is None else compose(pair, ps)
        if c < chunks - 1:
            entry[c] = pair
    mark("scan_y")
    py[y] = pair.astype(BF)
    ch_y = channel()
    for d in (2, 1, 3) if ny == 4 else range(1, ny):
        send(py.at[y], PY, ch_y, dev(yy=yof(d)))
    mark("pre_gu")
    turn_gu()
    mark("pre_dn")
    ring_dn[0].turn()
    mark("pre_dny")
    across_dn.forward()
    stw = stw_ref[...]
    stw = jnp.concatenate([stw[0:1], stw[1:2]], axis=1)
    for c, (r, k, v, _, _) in enumerate(given):
        self_ref[spans[c], :] = dot2(r * k * stw, ones) * v
    mark("pre_y0")
    y_forward()
    y_push()
    mark("scan_ywait")
    arrived(py.at[0 : ny - 1], ch_y)
    mark("scan_yfix")
    inside = jnp.zeros((W2, W2), F32)
    running = py[0].astype(F32)
    for yy in range(1, ny):
        inside = jnp.where(y == yy, running, inside)
        running = compose(running, py[yy].astype(F32))
    pz[z] = running.astype(BF)
    ring_ps.push(1, 0)
    ring_ps.push(1, 1)
    mark("pre_dn2")
    ring_dn[1].push(1)
    ring_dn[2].push(1)
    across_dn.finish()
    ring_dn[3].push(1)
    turn_gu()
    y_push(2)
    progress["dn"] = 1

    trans_left = jnp.zeros((HS, W2), F32)
    state_left = jnp.zeros((HS, W2), F32)
    state_right = jnp.zeros((HS, W2), F32)
    for s in range(1, half_ring + 1):
        mark(f"scan_z{s}")
        ring_ps.turn(s)
        mark(f"bulk{s}")
        if s in (1, 2, 4, 6, 7):
            turn_gu()
            turn_dn(2)
        else:
            turn_dn(4)
        y_push(2)
        mark(f"yfwd{s}")
        y_forward(2 if s % 2 == 0 else 1)
        mark(f"calc{s}")
        if s == half_ring // 2:
            ow_middle()
        if s == half_ring - 1:
            ow_last()
        left = pz[zof(-s)]
        has_left = z >= s
        hi, lo = halves(stacked(trans_left))
        moved = dg(left, hi) + dg(left, lo) + left.astype(F32)
        trans_left = jnp.where(has_left, trans_left + moved[:HS], trans_left)
        state_left = jnp.where(has_left, state_left + moved[HS:], state_left)
        if s < half_ring:
            right = pz[zof(s)].astype(F32)
            has_right = z + s >= nz
            moved = dot2(state_right, stacked(right[:HS]).astype(BF)) + right[HS:]
            state_right = jnp.where(has_right, state_right + moved, state_right)
    mark("state")
    state = state_right + dot3(state_right, stacked(trans_left)) + state_left
    state = state + dot3(state, stacked(inside[:HS])) + inside[HS:]

    turn_gu()
    y_push(2)
    turn_dn(1)
    mark("mech")
    seen = []
    for c in range(chunks):
        at = state
        if c > 0:
            at = state + dot3(state, stacked(entry[c - 1][:HS])) + entry[c - 1][HS:]
        seen.append(dot3(seen_ref[spans[c], :], stacked(at), NT))
    o = jnp.concatenate(seen, axis=0) + local_ref[...]
    shifted = o - dot2(o, ones) * (1.0 / HS)
    spread = dot2(shifted * shifted, ones) * (1.0 / HS)
    merged = shifted * lax.rsqrt(spread + GROUP_EPS) * hg_ref[...] + self_ref[...]
    mx[tp] = (merged * jax.nn.sigmoid(og_ref[...].astype(F32))).astype(BF)
    mx_far = [channel() for _ in range(1, nx)]
    mx_near = channel()
    x_order = [2, 1, 3] if nx == 4 else list(range(1, nx))
    for d in x_order:
        send(mx.at[tp], MX, mx_far[d - 1], x_dev(d))
    send(mx.at[tp], MX, mx_near, near)
    mark("exch_pump")
    y_forward()
    turn_dn(3)
    mark("exch_far")
    for d in reversed(x_order):
        arrived(mx.at[0], mx_far[d - 1])
        send(mx.at[same_core(-d)], MX, mx_near, near)
    mark("exch_pump2")
    y_forward()
    turn_dn(3)
    mark("exch_near")
    arrived(mx.at[0:nx], mx_near)
    mark("exch_ow")
    ow_finish()
    mark("exch_pump3")
    y_push(2)
    y_forward()

    mark("project")
    tile = min(256, width // 4)
    tiles = width // tile
    lhs = jnp.concatenate([mx[g] for g in range(ntp)], axis=1)

    def project(n, square):
        cols = pl.ds(pl.multiple_of(n * tile, tile), tile)
        mix = dg(lhs, ow[:, :, cols].reshape(ntp * W2, tile)).astype(BF).astype(F32)
        after = (res[:, cols].astype(F32) + mix).astype(BF).astype(F32)
        am[:, cols] = after
        sq = after * after
        for q in range(tile // W2):
            square = square + sq[:, q * W2 : (q + 1) * W2]
        return square

    square = jnp.zeros((rows, W2), F32)
    square = lax.fori_loop(0, tiles, project, square, unroll=2)
    mark("norm")
    y_push(2)
    y_forward()
    turn_dn(1)
    y_forward()
    turn_dn(1)
    scale = lax.rsqrt(jnp.sum(square, axis=1, keepdims=True) * (1.0 / width) + NORM_EPS)

    def normalize(n, carry):
        cols = pl.ds(pl.multiple_of(n * tile, tile), tile)
        normed[:, cols] = (am[:, cols] * scale * gain_ref[:, cols]).astype(BF)
        return carry

    lax.fori_loop(0, tiles, normalize, 0)
    mark("pumprest")
    while progress["forward"] < len(across):
        turn_gu()
        y_push(2)
        y_forward()
        turn_dn()
    mark("finish")
    across[0].finish()

    mark("gateup")
    at = 0
    while at < ff:
        wide = min(256, ff - at)
        x = normed[...]
        gate = dg(x, gu[:, 0:half_f, at : at + wide].reshape(width, wide))
        up = dg(x, gu[:, half_f : 2 * half_f, at : at + wide].reshape(width, wide))
        hid[:, at : at + wide] = (gate / (1.0 + jnp.exp(-gate)) * up).astype(BF)
        at += wide
        turn_dn(2)
    mark("dnwait")
    turn_dn(4 * half_ring)

    slots = tile // half_f

    def down(n, carry):
        cols = pl.ds(pl.multiple_of(n * tile, tile), tile)
        w = dn[pl.ds(n * slots, slots)].reshape(tile, ff)
        prod = dg(hid[...], w, NT).reshape(nx, 2, own, tile).astype(BF)
        part[0, :, :, cols] = prod[:, 0]
        part[1, :, :, cols] = prod[:, 1]
        return carry

    cuts = 4
    quarter = width // cuts
    pieces = [pl.ds(piece * quarter, quarter) for piece in range(cuts)]
    ch_core = [channel() for _ in range(cuts)]
    ch_part = [channel() for _ in range(cuts)]

    def x_at(d):
        return lax.rem(xx + d + nx, nx)

    def add_cores(piece):
        cols = pieces[piece]
        arrived(pgot.at[:, :, cols], ch_core[piece])
        for d in [2, 1, 3] if nx == 4 else range(1, nx):
            both = part[core, x_at(d), :, cols].astype(F32) + pgot[x_at(d), :, cols].astype(F32)
            comb[d - 1, :, cols] = both.astype(BF)
            copy(
                comb.at[d - 1, :, cols], got.at[d - 1, :, cols], COMB, ch_part[piece], x_dev(d)
            ).start()

    for piece, cols in enumerate(pieces):
        mark(f"down{piece}")
        lax.fori_loop(piece * tiles // cuts, (piece + 1) * tiles // cuts, down, 0, unroll=True)
        copy(
            part.at[1 - core, :, :, cols], pgot.at[:, :, cols], PART, ch_core[piece], near
        ).start()
        if piece >= 2:
            add_cores(piece - 2)
    mark("rs_core")
    add_cores(cuts - 2)
    add_cores(cuts - 1)
    mark("rs_wait")
    for piece, cols in enumerate(pieces):
        total = am[pl.ds(pl.multiple_of(tp * own, own), own), cols]
        total = total + part[core, xx, :, cols].astype(F32) + pgot[xx, :, cols].astype(F32)
        if nx > 1:
            arrived(got.at[:, :, cols], ch_part[piece])
        for d in range(1, nx):
            total = total + got[d - 1, :, cols].astype(F32)
        out_ref[:, cols] = total.astype(BF)
    mark("sendwait")
    gone = [
        (gu.at[0 : nz * ny - 1], GU),
        (dn.at[0 : nz * ny - 1], DN),
        (pz.at[0 : nz - 1], PS),
        (py.at[0 : ny - 1], PY),
        (ow.at[0 : ntp - 1], OW),
        (mx.at[0 : ntp - 1], MX),
        (part.at[0], PART),
    ]
    if nx > 1:
        gone.append((comb, COMB))
    for ref, out in gone:
        copy(ref, ref, out, 0, near).wait_send()
    mark(None)
    assert count[0] <= SEMS, count[0]


def per_device(
    nz,
    ny,
    ntp,
    receptance,
    head_keys,
    head_values,
    decay_preact,
    learning_rate_preact,
    output_gate_preact,
    self_token_weight,
    head_norm_gain,
    output_weight,
    residual,
    premixer_norm_gain,
    mixer_gate_weight,
    mixer_up_weight,
    mixer_down_weight,
):
    rows = receptance.shape[0]
    width = residual.shape[1]
    half_f, ff = mixer_gate_weight.shape
    own = rows // ntp
    nx = ntp // 2
    vmem = pl.BlockSpec(memory_space=pltpu.VMEM)
    hbm = pl.BlockSpec(memory_space=pltpu.HBM)
    return pl.pallas_call(
        functools.partial(kernel, nz, ny, ntp),
        out_shape=jax.ShapeDtypeStruct((own, width), BF),
        in_specs=[hbm] * 14,
        out_specs=vmem,
        scratch_shapes=[
            pltpu.VMEM((rows, W2), BF),
            pltpu.VMEM((rows, W2), BF),
            pltpu.VMEM((rows, W2), BF),
            pltpu.VMEM((rows, W2), F32),
            pltpu.VMEM((rows, W2), F32),
            pltpu.VMEM((rows, W2), BF),
            pltpu.VMEM((2, HS), F32),
            pltpu.VMEM((1, W2), F32),
            pltpu.VMEM((1, width), F32),
            pltpu.VMEM((nz * ny, 2 * half_f, ff), BF),
            pltpu.VMEM((nz * ny, half_f, ff), BF),
            pltpu.VMEM((ntp, W2, width), BF),
            pltpu.VMEM((rows, width), BF),
            pltpu.VMEM((ny, W2, W2), BF),
            pltpu.VMEM((nz, W2, W2), BF),
            pltpu.VMEM((rows // CHUNK, W2, W2), F32),
            pltpu.VMEM((rows, W2), F32),
            pltpu.VMEM((rows, W2), F32),
            pltpu.VMEM((rows, W2), F32),
            pltpu.VMEM((ntp, rows, W2), BF),
            pltpu.VMEM((rows, width), F32),
            pltpu.VMEM((rows, width), BF),
            pltpu.VMEM((rows, ff), BF),
            pltpu.VMEM((2, nx, own, width), BF),
            pltpu.VMEM((max(nx - 1, 1), own, width), BF),
            pltpu.VMEM((nx, own, width), BF),
            pltpu.VMEM((max(nx - 1, 1), own, width), BF),
            pltpu.SemaphoreType.DMA((14,)),
            pltpu.SemaphoreType.DMA((8,)),
            pltpu.SemaphoreType.DMA((SEMS,)),
        ],
        compiler_params=pltpu.CompilerParams(
            collective_id=0, has_side_effects=True, vmem_limit_bytes=60 * 1024 * 1024
        ),
        name="layer",
    )(
        receptance,
        head_keys,
        head_values,
        decay_preact,
        learning_rate_preact,
        output_gate_preact,
        self_token_weight,
        head_norm_gain.reshape(1, -1),
        output_weight,
        residual,
        premixer_norm_gain.reshape(1, -1),
        mixer_gate_weight,
        mixer_up_weight,
        mixer_down_weight.T,
    )


def build(mesh, nz, ny):
    ntp = mesh.shape["tp"]
    torus = Mesh(mesh.devices.reshape(nz, ny, ntp), ("z", "y", "tp"))
    sp = ("z", "y")
    cut = P(sp, "tp")
    in_specs = (cut,) * 6 + (
        P("tp", None),
        P("tp"),
        P("tp", None),
        P(sp, None),
        P(),
        cut,
        cut,
        P("tp", sp),
    )
    return jax.shard_map(
        functools.partial(per_device, nz, ny, ntp),
        mesh=torus,
        in_specs=in_specs,
        out_specs=P(("z", "y", "tp"), None),
        check_vma=False,
    )


def solution(mesh):
    return build(mesh, 16, 4)
```

```python
import functools

import jax
import jax.numpy as jnp
from jax import lax
from jax.experimental import pallas as pl
from jax.experimental.pallas import tpu as pltpu
from jax.sharding import Mesh
from jax.sharding import PartitionSpec as P

HS = 64
CHUNK = 64
W2 = 2 * HS
GROUP_EPS = 0.00064
NORM_EPS = 1e-06
F32 = jnp.float32
BF = jnp.bfloat16
NN = (((1,), (0,)), ((), ()))
NT = (((1,), (1,)), ((), ()))
SEMS = 96


def dg(a, b, dims=NN):
    return lax.dot_general(a, b, dims, preferred_element_type=F32)


def halves(x):
    hi = x.astype(BF)
    return hi, (x - hi.astype(F32)).astype(BF)


def dot_halves(a, b, dims=NN):
    return dg(a[0], b[0], dims) + (dg(a[0], b[1], dims) + dg(a[1], b[0], dims))


def dot3(a, b, dims=NN):
    return dot_halves(halves(a), halves(b), dims)


def dot2(a, b, dims=NN):
    hi, lo = halves(a)
    return dg(hi, b, dims) + dg(lo, b, dims)


def iota(shape, dim):
    return lax.broadcasted_iota(jnp.int32, shape, dim)


def head_masks():
    lane = iota((1, W2), 1)
    first = (lane < HS).astype(F32)
    return first, 1.0 - first


def stacked(x):
    first, second = head_masks()
    return jnp.concatenate([x * first, x * second], axis=0)


def folded(x):
    half = x.shape[0] // 2
    return x[:half] + x[half:]


def head_ones():
    i, j = iota((W2, W2), 0), iota((W2, W2), 1)
    return ((i < HS) == (j < HS)).astype(BF)


def compose(earlier, later):
    later_d = stacked(later[:HS])
    i, j = iota((W2, W2), 0), iota((W2, W2), 1)
    moved = dot3(earlier, later_d + (i == j).astype(F32))
    return jnp.concatenate([moved[:HS] + later[:HS], moved[HS:] + later[HS:]], axis=0)


def chunk_stages(chunks):
    i, j = iota((CHUNK, CHUNK), 0), iota((CHUNK, CHUNK), 1)
    tri = (i >= j).astype(BF)
    ones = head_ones()
    i, j = iota((W2, W2), 0), iota((W2, W2), 1)
    same = (i < HS) == (j < HS)
    strict = same & (i > j)
    incl = same & (i >= j)
    made = []
    for r, k, v, pre, lr in chunks:
        logw = jax.nn.sigmoid(pre) * (-0.6065306597126334)
        a1 = logw.astype(BF)
        a2, a3 = halves(logw - a1.astype(F32))
        cum = dg(tri, a1) + (dg(tri, a2) + dg(tri, a3))
        last = cum[CHUNK - 1 :, :]
        grown = jnp.exp(-cum)
        tail = jnp.exp(last - cum)
        unit = k / jnp.maximum(jnp.sqrt(dot2(k * k, ones)), 1.0)
        ins = unit * jax.nn.sigmoid(lr)
        us = stacked(-jnp.exp(cum - logw) * unit)
        rs = stacked(jnp.exp(cum) * r)
        made.append(
            dict(
                last=last,
                us=us,
                rs=rs,
                left=halves(jnp.concatenate([us, rs], axis=0)),
                right=halves(
                    jnp.concatenate([stacked(ins * grown), stacked(k * grown)], axis=0)
                ),
                bts=halves(stacked(ins * tail)),
                kts=halves(stacked(k * tail)),
                v=stacked(v),
            )
        )
    for m in made:
        gram = dot_halves(m["left"], m["right"], NT)
        m["lb"] = jnp.where(strict, gram[:W2, :W2], 0.0)
        m["lk"] = jnp.where(strict, gram[:W2, W2:], 0.0)
        m["mb"] = jnp.where(incl, gram[W2:, :W2], 0.0)
        m["mk"] = jnp.where(incl, gram[W2:, W2:], 0.0)
        m["vs"] = m["v"].astype(BF)
    for m in made:
        m["lkv"] = dot2(m["lk"], m["vs"])
        m["mkv"] = dot2(m["mk"], m["vs"])
    size = 1
    while size < CHUNK:
        row, col = i // size, j // size
        below = (row == col + 1) & (row % 2 == 1)
        if size == 1:
            for m in made:
                m["inv"] = (i == j).astype(F32) + jnp.where(below, m["lb"], 0.0)
        else:
            held = [halves(m["inv"]) for m in made]
            mid = [
                dot_halves(h, halves(jnp.where(below, m["lb"], 0.0))) for h, m in zip(held, made)
            ]
            for m, h, x in zip(made, held, mid):
                m["inv"] = m["inv"] + dot_halves(halves(x), h)
        size *= 2
        if size == 8:
            yield
    for m in made:
        m["tuv"] = dot3(m["inv"], jnp.concatenate([m["us"], m["lkv"]], axis=1))
    out = []
    for m in made:
        turned = dot_halves(halves(m["tuv"].T), m["bts"])
        trans = folded(jnp.where(i == j, jnp.exp(m["last"]) - 1.0, 0.0) + turned[:W2])
        vt = m["v"].T.astype(BF)
        state = folded(turned[W2:] + dg(vt, m["kts"][0]) + dg(vt, m["kts"][1]))
        m["pair"] = jnp.concatenate([trans, state], axis=0)
    for m in made:
        muv = dot_halves(halves(m["mb"]), halves(m["tuv"]))
        out.append(
            (m["pair"], folded(m["rs"] + muv[:, :W2]), folded(muv[:, W2:] + m["mkv"]))
        )
    return out


def kernel(
    nz,
    ny,
    ntp,
    r_in,
    k_in,
    v_in,
    pre_in,
    lr_in,
    og_in,
    stw_in,
    hg_in,
    ow_in,
    res_in,
    gain_in,
    gate_in,
    up_in,
    down_in,
    out_ref,
    r_ref,
    k_ref,
    v_ref,
    pre_ref,
    lr_ref,
    og_ref,
    stw_ref,
    hg_ref,
    gain_ref,
    gu,
    dn,
    ow,
    res,
    py,
    pz,
    entry,
    seen_ref,
    local_ref,
    self_ref,
    mx,
    am,
    normed,
    hid,
    part,
    got,
    pgot,
    comb,
    early_sum,
    lsem,
    ssem,
    rsem,
):
    z, y, tp = lax.axis_index("z"), lax.axis_index("y"), lax.axis_index("tp")
    rows = r_in.shape[0]
    chunks = rows // CHUNK
    own = rows // ntp
    width = res_in.shape[1]
    half_f = gate_in.shape[0]
    ff = gate_in.shape[1]
    half_ring = nz // 2
    nx = ntp // 2
    xx, core = tp // 2, tp % 2

    def zof(step):
        return lax.rem(z + step + nz, nz)

    def yof(step):
        return lax.rem(y + step + ny, ny)

    def tof(step):
        return lax.rem(tp + step + ntp, ntp)

    def sp(zz, yy):
        return zz * ny + yy

    def dev(zz=None, yy=None, tt=None):
        return {"z": z if zz is None else zz, "y": y if yy is None else yy, "tp": tp if tt is None else tt}

    scope = [None]

    def mark(name):
        if scope[0] is not None:
            scope[0].__exit__(None, None, None)
        scope[0] = None
        if name:
            scope[0] = jax.named_scope(name)
            scope[0].__enter__()

    mark("enter")
    here = sp(z, y)
    weights = [
        (gate_in, gu.at[here, 0:half_f]),
        (up_in, gu.at[here, half_f : 2 * half_f]),
        (down_in, dn.at[here]),
        (ow_in, ow.at[tp]),
    ]
    streams = [
        (pre_in, pre_ref),
        (k_in, k_ref),
        (lr_in, lr_ref),
        (r_in, r_ref),
        (v_in, v_ref),
        (og_in, og_ref),
        (stw_in, stw_ref),
        (hg_in, hg_ref),
        (gain_in, gain_ref),
        (res_in, res),
    ]
    loads = [
        pltpu.make_async_copy(src, dst, lsem.at[i])
        for i, (src, dst) in enumerate(weights + streams)
    ]
    for load in loads[len(weights) :] + loads[: len(weights)]:
        load.start()

    barrier = pltpu.get_barrier_semaphore()
    peers = [dev(zz=zof(1)), dev(zz=zof(-1))]
    peers += [dev(yy=yof(d)) for d in range(1, ny)]
    peers += [dev(tt=tof(d)) for d in range(1, ntp)]
    for peer in peers:
        pl.semaphore_signal(barrier, inc=1, device_id=peer, device_id_type=pl.DeviceIdType.MESH)
    early = len(weights) + 5
    for load in loads[len(weights) : early]:
        load.wait()
    mark("recur_a")
    spans = [pl.ds(c * CHUNK, CHUNK) for c in range(chunks)]
    given = []
    for span in spans:
        r, k, v = (ref[span, :].astype(F32) for ref in (r_ref, k_ref, v_ref))
        given.append((r, k, v, pre_ref[span, :], lr_ref[span, :]))
    stages = chunk_stages(given)
    next(stages)
    mark("greet")
    pl.semaphore_wait(barrier, len(peers))
    for load in loads[: len(weights)]:
        load.wait()

    count = [0]

    def channel():
        count[0] += 1
        return count[0] - 1

    def copy(src, dst, out, ch, device):
        return pltpu.make_async_remote_copy(
            src_ref=src,
            dst_ref=dst,
            send_sem=ssem.at[out],
            recv_sem=rsem.at[ch],
            device_id=device,
            device_id_type=pl.DeviceIdType.MESH,
        )

    GU, DN, PS, PY, OW, MX, PART, COMB = range(8)

    def send(ref, out, ch, device):
        copy(ref, ref, out, ch, device).start()

    def arrived(ref, ch):
        copy(ref, ref, 0, ch, dev(zz=zof(1))).wait_recv()

    class Ring:
        def __init__(self, block, out, one, two):
            self.block, self.out, self.one, self.two = block, out, one, two
            self.ch = [channel() for _ in range(half_ring)]
            self.step = 1

        def piece(self, s, side):
            return side if s == half_ring else None

        def push(self, s):
            ch = self.ch[s - 1]
            send(self.block(zof(1 - s), self.piece(s, 0)), self.out, ch, dev(zz=zof(1)))
            send(self.block(zof(s - 1), self.piece(s, 1)), self.out, ch, dev(zz=zof(-1)))

        def turn(self):
            s = self.step
            if s > half_ring:
                return
            arrived(self.one if s == half_ring else self.two, self.ch[s - 1])
            if s < half_ring:
                self.push(s + 1)
            self.step = s + 1

    class PairRing:
        def __init__(self):
            self.ch = [(channel(), channel()) for _ in range(half_ring)]

        def part(self, zz, half):
            return pz.at[zz, half * HS : (half + 1) * HS]

        def push(self, s, half):
            ch = self.ch[s - 1][half]
            if s < half_ring or half == 0:
                send(self.part(zof(1 - s), half), PS, ch, dev(zz=zof(1)))
            if s < half_ring or half == 1:
                send(self.part(zof(s - 1), half), PS, ch, dev(zz=zof(-1)))

        def turn(self, s):
            for half in range(2):
                arrived(pz.at[0] if s < half_ring else self.part(0, half), self.ch[s - 1][half])
                if s < half_ring:
                    self.push(s + 1, half)

    class Across:
        def __init__(self, block, at, to, out, one, two, last=None):
            self.block, self.at, self.to, self.out = block, at, to, out
            self.one, self.two = one, two
            self.first = channel()
            self.last = channel() if last is None else last

        def push(self):
            send(self.block(self.at(0), None), self.out, self.first, self.to(1))
            send(self.block(self.at(0), None), self.out, self.first, self.to(-1))

        def forward(self):
            arrived(self.two, self.first)
            send(self.block(self.at(-1), 0), self.out, self.last, self.to(1))
            send(self.block(self.at(1), 1), self.out, self.last, self.to(-1))

        def finish(self):
            arrived(self.one, self.last)

    def cut(ref, piece, length):
        if piece is None:
            return ref
        middle = (length // 2 + 7) // 8 * 8
        return ref.at[0:middle] if piece == 0 else ref.at[middle:length]

    a_rows = 2 * half_f
    b_rows = half_f

    def gu_block(zz, yy, piece):
        return cut(gu.at[sp(zz, yy)], piece, a_rows)

    def dn_block(zz, yy, piece):
        return cut(dn.at[sp(zz, yy)], piece, b_rows)

    def y_dev(d):
        return dev(yy=yof(d))

    ring_gu = Ring(lambda zz, piece: gu_block(zz, y, piece), GU, gu.at[0], gu.at[0:2])
    ring_dn = [
        Ring(
            functools.partial(lambda k, zz, piece: dn_block(zz, yof(k), piece), k),
            DN,
            dn.at[0],
            dn.at[0:2],
        )
        for k in (0, 1, -1, 2)
    ]
    ring_ps = PairRing()
    order = [0]
    for s in range(1, half_ring):
        order += [-s, s]
    order += [half_ring]
    late = max(1, nz // 4)
    far_early, far_late = channel(), channel()
    across = [
        Across(
            functools.partial(lambda step, yy, piece: gu_block(zof(step), yy, piece), step),
            yof,
            y_dev,
            GU,
            gu.at[0:late] if i >= nz - late else gu.at[0 : nz - late],
            gu.at[0:2],
            far_late if i >= nz - late else far_early,
        )
        for i, step in enumerate(order)
    ]
    across_dn = Across(
        lambda yy, piece: dn_block(z, yy, piece), yof, y_dev, DN, dn.at[0], dn.at[0:2]
    )

    progress = {"push": 1, "forward": 0, "dn": 0}

    def turn_gu():
        ring_gu.turn()

    def turn_dn(n=1):
        for _ in range(n):
            ring_dn[progress["dn"] % 4].turn()
            progress["dn"] += 1

    def y_push(n=1):
        for _ in range(n):
            i = progress["push"]
            if i < len(across) and (i + 1) // 2 < ring_gu.step:
                across[i].push()
                progress["push"] += 1

    def y_forward(n=1):
        for _ in range(n):
            if progress["forward"] < progress["push"]:
                across[progress["forward"]].forward()
                progress["forward"] += 1

    def same_core(d):
        return lax.rem(xx + d + nx, nx) * 2 + core

    def other_core(d):
        return lax.rem(xx + d + nx, nx) * 2 + (1 - core)

    def x_dev(d):
        return dev(tt=same_core(d))

    partner = other_core(0)
    near = dev(tt=partner)
    across_ow = None
    if nx == 4:
        across_ow = Across(
            lambda t, piece: cut(ow.at[t], piece, W2),
            same_core,
            x_dev,
            OW,
            ow.at[0],
            ow.at[0:2],
        )
    ow_far = [channel() for _ in range(1, nx)] if across_ow is None else []
    ow_near = channel()

    def ow_share(d):
        send(ow.at[same_core(d)], OW, ow_near, near)

    def ow_start():
        if across_ow is not None:
            across_ow.push()
        else:
            for d in range(1, nx):
                send(ow.at[tp], OW, ow_far[d - 1], x_dev(d))
        ow_share(0)

    def ow_middle():
        if across_ow is not None:
            across_ow.forward()
            ow_share(1)
            ow_share(-1)

    def ow_last():
        if across_ow is not None:
            across_ow.finish()
            ow_share(2)
        else:
            for d in range(1, nx):
                arrived(ow.at[0], ow_far[d - 1])
                ow_share(-d)

    def ow_finish():
        arrived(ow.at[0:nx], ow_near)

    mark("launch")
    ring_gu.push(1)
    ring_dn[0].push(1)
    across_dn.push()
    across[0].push()
    ow_start()
    for load in loads[early:]:
        load.wait()

    mark("recur")
    ones = head_ones()
    try:
        next(stages)
    except StopIteration as end:
        made = end.value
    pair = None
    for c, (ps, seen, local) in enumerate(made):
        seen_ref[spans[c], :] = seen
        local_ref[spans[c], :] = local
        pair = ps if pair is None else compose(pair, ps)
        if c < chunks - 1:
            entry[c] = pair
    mark("scan_y")
    py[y] = pair.astype(BF)
    ch_y = channel()
    for d in (2, 1, 3) if ny == 4 else range(1, ny):
        send(py.at[y], PY, ch_y, dev(yy=yof(d)))
    mark("pre_gu")
    turn_gu()
    mark("pre_dn")
    ring_dn[0].turn()
    mark("pre_dny")
    across_dn.forward()
    stw = stw_ref[...]
    stw = jnp.concatenate([stw[0:1], stw[1:2]], axis=1)
    for c, (r, k, v, _, _) in enumerate(given):
        self_ref[spans[c], :] = dot2(r * k * stw, ones) * v
    mark("pre_y0")
    y_forward()
    y_push()
    mark("scan_ywait")
    arrived(py.at[0 : ny - 1], ch_y)
    mark("scan_yfix")
    inside = jnp.zeros((W2, W2), F32)
    running = py[0].astype(F32)
    for yy in range(1, ny):
        inside = jnp.where(y == yy, running, inside)
        running = compose(running, py[yy].astype(F32))
    pz[z] = running.astype(BF)
    ring_ps.push(1, 0)
    ring_ps.push(1, 1)
    mark("pre_dn2")
    ring_dn[1].push(1)
    ring_dn[2].push(1)
    across_dn.finish()
    ring_dn[3].push(1)
    turn_gu()
    y_push(2)
    progress["dn"] = 1

    trans_left = jnp.zeros((HS, W2), F32)
    state_left = jnp.zeros((HS, W2), F32)
    state_right = jnp.zeros((HS, W2), F32)
    for s in range(1, half_ring + 1):
        mark(f"scan_z{s}")
        ring_ps.turn(s)
        mark(f"bulk{s}")
        if s < half_ring:
            if s in (1, 2, 4, 6, 7):
                turn_gu()
                turn_dn(2)
            else:
                turn_dn(4)
            y_push(2)
            mark(f"yfwd{s}")
            y_forward(2 if s % 2 == 0 else 1)
        mark(f"calc{s}")
        if s == half_ring // 2:
            ow_middle()
        if s == half_ring - 1:
            ow_last()
        left = pz[zof(-s)]
        has_left = z >= s
        hi, lo = halves(stacked(trans_left))
        moved = dg(left, hi) + dg(left, lo) + left.astype(F32)
        trans_left = jnp.where(has_left, trans_left + moved[:HS], trans_left)
        state_left = jnp.where(has_left, state_left + moved[HS:], state_left)
        if s < half_ring:
            right = pz[zof(s)].astype(F32)
            has_right = z + s >= nz
            moved = dot2(state_right, stacked(right[:HS]).astype(BF)) + right[HS:]
            state_right = jnp.where(has_right, state_right + moved, state_right)
    mark("state")
    state = state_right + dot3(state_right, stacked(trans_left)) + state_left
    state = state + dot3(state, stacked(inside[:HS])) + inside[HS:]

    mark("mech")
    seen = []
    for c in range(chunks):
        at = state
        if c > 0:
            at = state + dot3(state, stacked(entry[c - 1][:HS])) + entry[c - 1][HS:]
        seen.append(dot3(seen_ref[spans[c], :], stacked(at), NT))
    o = jnp.concatenate(seen, axis=0) + local_ref[...]
    shifted = o - dot2(o, ones) * (1.0 / HS)
    spread = dot2(shifted * shifted, ones) * (1.0 / HS)
    merged = shifted * lax.rsqrt(spread + GROUP_EPS) * hg_ref[...] + self_ref[...]
    mx[tp] = (merged * jax.nn.sigmoid(og_ref[...].astype(F32))).astype(BF)
    mx_far = [channel() for _ in range(1, nx)]
    mx_near = channel()
    x_order = [2, 1, 3] if nx == 4 else list(range(1, nx))
    for d in x_order:
        send(mx.at[tp], MX, mx_far[d - 1], x_dev(d))
    send(mx.at[tp], MX, mx_near, near)
    mark("exch_pump")
    turn_dn(2)
    y_forward()
    turn_gu()
    y_push(2)
    turn_dn(2)
    y_forward()
    mark("exch_far")
    for d in reversed(x_order):
        arrived(mx.at[0], mx_far[d - 1])
        send(mx.at[same_core(-d)], MX, mx_near, near)
    mark("exch_pump2")
    turn_dn(2)
    y_forward()
    mark("exch_near")
    arrived(mx.at[0:nx], mx_near)
    mark("exch_ow")
    ow_finish()
    mark("exch_pump3")
    turn_dn(1)
    y_push(2)
    y_forward()

    mark("project")
    tile = min(256, width // 4)
    tiles = width // tile
    lhs = jnp.concatenate([mx[g] for g in range(ntp)], axis=1)

    def project(n, square):
        cols = pl.ds(pl.multiple_of(n * tile, tile), tile)
        mix = dg(lhs, ow[:, :, cols].reshape(ntp * W2, tile)).astype(BF).astype(F32)
        after = (res[:, cols].astype(F32) + mix).astype(BF).astype(F32)
        am[:, cols] = after
        sq = after * after
        for q in range(tile // W2):
            square = square + sq[:, q * W2 : (q + 1) * W2]
        return square

    square = jnp.zeros((rows, W2), F32)
    square = lax.fori_loop(0, tiles, project, square, unroll=2)
    mark("norm")
    y_push(2)
    y_forward()
    turn_dn(1)
    y_forward()
    turn_dn(1)
    scale = lax.rsqrt(jnp.sum(square, axis=1, keepdims=True) * (1.0 / width) + NORM_EPS)

    def normalize(n, carry):
        cols = pl.ds(pl.multiple_of(n * tile, tile), tile)
        normed[:, cols] = (am[:, cols] * scale * gain_ref[:, cols]).astype(BF)
        return carry

    lax.fori_loop(0, tiles, normalize, 0)
    mark("pumprest")
    while progress["forward"] < len(across):
        turn_gu()
        y_push(2)
        y_forward()
        turn_dn()
    z_rows = ny * half_f

    def gate_up(steps, at, wide):
        x = jnp.concatenate(
            [normed[:, pl.ds(pl.multiple_of(zof(t) * z_rows, z_rows), z_rows)] for t in steps],
            axis=1,
        )
        sums = []
        for first in (0, half_f):
            w = [
                gu[pl.ds(zof(t) * ny, ny), first : first + half_f, at : at + wide].reshape(
                    z_rows, wide
                )
                for t in steps
            ]
            sums.append(dg(x, jnp.concatenate(w, axis=0)))
        return sums

    bands = [(at, min(256, ff - at)) for at in range(0, ff, 256)]
    mark("finish_a")
    across[0].finish()
    mark("gateup_a")
    for at, wide in bands:
        gate, up = gate_up(order[: nz - late], at, wide)
        early_sum[0, :, at : at + wide] = gate
        early_sum[1, :, at : at + wide] = up
        turn_dn()
    mark("finish_b")
    turn_dn(2)
    across[-1].finish()
    mark("gateup_b")
    for at, wide in bands:
        gate, up = gate_up(order[nz - late :], at, wide)
        gate = gate + early_sum[0, :, at : at + wide]
        up = up + early_sum[1, :, at : at + wide]
        hid[:, at : at + wide] = (gate / (1.0 + jnp.exp(-gate)) * up).astype(BF)
    mark("dnwait")
    turn_dn(4 * half_ring)

    slots = tile // half_f

    def down(n, carry):
        cols = pl.ds(pl.multiple_of(n * tile, tile), tile)
        w = dn[pl.ds(n * slots, slots)].reshape(tile, ff)
        prod = dg(hid[...], w, NT).reshape(nx, 2, own, tile).astype(BF)
        part[0, :, :, cols] = prod[:, 0]
        part[1, :, :, cols] = prod[:, 1]
        return carry

    cuts = 4
    quarter = width // cuts
    pieces = [pl.ds(piece * quarter, quarter) for piece in range(cuts)]
    ch_core = [channel() for _ in range(cuts)]
    ch_part = [channel() for _ in range(cuts)]

    def x_at(d):
        return lax.rem(xx + d + nx, nx)

    def add_cores(piece):
        cols = pieces[piece]
        arrived(pgot.at[:, :, cols], ch_core[piece])
        for d in [2, 1, 3] if nx == 4 else range(1, nx):
            both = part[core, x_at(d), :, cols].astype(F32) + pgot[x_at(d), :, cols].astype(F32)
            comb[d - 1, :, cols] = both.astype(BF)
            copy(
                comb.at[d - 1, :, cols], got.at[d - 1, :, cols], COMB, ch_part[piece], x_dev(d)
            ).start()

    for piece, cols in enumerate(pieces):
        mark(f"down{piece}")
        lax.fori_loop(piece * tiles // cuts, (piece + 1) * tiles // cuts, down, 0, unroll=True)
        copy(
            part.at[1 - core, :, :, cols], pgot.at[:, :, cols], PART, ch_core[piece], near
        ).start()
        if piece >= 2:
            add_cores(piece - 2)
    mark("rs_core")
    add_cores(cuts - 2)
    add_cores(cuts - 1)
    mark("rs_wait")
    for piece, cols in enumerate(pieces):
        total = am[pl.ds(pl.multiple_of(tp * own, own), own), cols]
        total = total + part[core, xx, :, cols].astype(F32) + pgot[xx, :, cols].astype(F32)
        if nx > 1:
            arrived(got.at[:, :, cols], ch_part[piece])
        for d in range(1, nx):
            total = total + got[d - 1, :, cols].astype(F32)
        out_ref[:, cols] = total.astype(BF)
    mark("sendwait")
    gone = [
        (gu.at[0 : nz * ny - 1], GU),
        (dn.at[0 : nz * ny - 1], DN),
        (pz.at[0 : nz - 1], PS),
        (py.at[0 : ny - 1], PY),
        (ow.at[0 : ntp - 1], OW),
        (mx.at[0 : ntp - 1], MX),
        (part.at[0], PART),
    ]
    if nx > 1:
        gone.append((comb, COMB))
    for ref, out in gone:
        copy(ref, ref, out, 0, near).wait_send()
    mark(None)
    assert count[0] <= SEMS, count[0]


def per_device(
    nz,
    ny,
    ntp,
    receptance,
    head_keys,
    head_values,
    decay_preact,
    learning_rate_preact,
    output_gate_preact,
    self_token_weight,
    head_norm_gain,
    output_weight,
    residual,
    premixer_norm_gain,
    mixer_gate_weight,
    mixer_up_weight,
    mixer_down_weight,
):
    rows = receptance.shape[0]
    width = residual.shape[1]
    half_f, ff = mixer_gate_weight.shape
    own = rows // ntp
    nx = ntp // 2
    vmem = pl.BlockSpec(memory_space=pltpu.VMEM)
    hbm = pl.BlockSpec(memory_space=pltpu.HBM)
    return pl.pallas_call(
        functools.partial(kernel, nz, ny, ntp),
        out_shape=jax.ShapeDtypeStruct((own, width), BF),
        in_specs=[hbm] * 14,
        out_specs=vmem,
        scratch_shapes=[
            pltpu.VMEM((rows, W2), BF),
            pltpu.VMEM((rows, W2), BF),
            pltpu.VMEM((rows, W2), BF),
            pltpu.VMEM((rows, W2), F32),
            pltpu.VMEM((rows, W2), F32),
            pltpu.VMEM((rows, W2), BF),
            pltpu.VMEM((2, HS), F32),
            pltpu.VMEM((1, W2), F32),
            pltpu.VMEM((1, width), F32),
            pltpu.VMEM((nz * ny, 2 * half_f, ff), BF),
            pltpu.VMEM((nz * ny, half_f, ff), BF),
            pltpu.VMEM((ntp, W2, width), BF),
            pltpu.VMEM((rows, width), BF),
            pltpu.VMEM((ny, W2, W2), BF),
            pltpu.VMEM((nz, W2, W2), BF),
            pltpu.VMEM((rows // CHUNK, W2, W2), F32),
            pltpu.VMEM((rows, W2), F32),
            pltpu.VMEM((rows, W2), F32),
            pltpu.VMEM((rows, W2), F32),
            pltpu.VMEM((ntp, rows, W2), BF),
            pltpu.VMEM((rows, width), F32),
            pltpu.VMEM((rows, width), BF),
            pltpu.VMEM((rows, ff), BF),
            pltpu.VMEM((2, nx, own, width), BF),
            pltpu.VMEM((max(nx - 1, 1), own, width), BF),
            pltpu.VMEM((nx, own, width), BF),
            pltpu.VMEM((max(nx - 1, 1), own, width), BF),
            pltpu.VMEM((2, rows, ff), F32),
            pltpu.SemaphoreType.DMA((14,)),
            pltpu.SemaphoreType.DMA((8,)),
            pltpu.SemaphoreType.DMA((SEMS,)),
        ],
        compiler_params=pltpu.CompilerParams(
            collective_id=0, has_side_effects=True, vmem_limit_bytes=60 * 1024 * 1024
        ),
        name="layer",
    )(
        receptance,
        head_keys,
        head_values,
        decay_preact,
        learning_rate_preact,
        output_gate_preact,
        self_token_weight,
        head_norm_gain.reshape(1, -1),
        output_weight,
        residual,
        premixer_norm_gain.reshape(1, -1),
        mixer_gate_weight,
        mixer_up_weight,
        mixer_down_weight.T,
    )


def build(mesh, nz, ny):
    ntp = mesh.shape["tp"]
    torus = Mesh(mesh.devices.reshape(nz, ny, ntp), ("z", "y", "tp"))
    sp = ("z", "y")
    cut = P(sp, "tp")
    in_specs = (cut,) * 6 + (
        P("tp", None),
        P("tp"),
        P("tp", None),
        P(sp, None),
        P(),
        cut,
        cut,
        P("tp", sp),
    )
    return jax.shard_map(
        functools.partial(per_device, nz, ny, ntp),
        mesh=torus,
        in_specs=in_specs,
        out_specs=P(("z", "y", "tp"), None),
        check_vma=False,
    )


def solution(mesh):
    return build(mesh, 16, 4)
```

```python
import functools

import jax
import jax.numpy as jnp
from jax import lax
from jax.experimental import pallas as pl
from jax.experimental.pallas import tpu as pltpu
from jax.sharding import Mesh
from jax.sharding import PartitionSpec as P

HS = 64
CHUNK = 64
W2 = 2 * HS
GROUP_EPS = 0.00064
NORM_EPS = 1e-06
F32 = jnp.float32
BF = jnp.bfloat16
NN = (((1,), (0,)), ((), ()))
NT = (((1,), (1,)), ((), ()))
SEMS = 96


def dg(a, b, dims=NN):
    return lax.dot_general(a, b, dims, preferred_element_type=F32)


def halves(x):
    hi = x.astype(BF)
    return hi, (x - hi.astype(F32)).astype(BF)


def dot_halves(a, b, dims=NN):
    return dg(a[0], b[0], dims) + (dg(a[0], b[1], dims) + dg(a[1], b[0], dims))


def dot3(a, b, dims=NN):
    return dot_halves(halves(a), halves(b), dims)


def dot2(a, b, dims=NN):
    hi, lo = halves(a)
    return dg(hi, b, dims) + dg(lo, b, dims)


def iota(shape, dim):
    return lax.broadcasted_iota(jnp.int32, shape, dim)


def head_masks():
    lane = iota((1, W2), 1)
    first = (lane < HS).astype(F32)
    return first, 1.0 - first


def stacked(x):
    first, second = head_masks()
    return jnp.concatenate([x * first, x * second], axis=0)


def folded(x):
    half = x.shape[0] // 2
    return x[:half] + x[half:]


def head_ones():
    i, j = iota((W2, W2), 0), iota((W2, W2), 1)
    return ((i < HS) == (j < HS)).astype(BF)


def compose(earlier, later):
    later_d = stacked(later[:HS])
    i, j = iota((W2, W2), 0), iota((W2, W2), 1)
    moved = dot3(earlier, later_d + (i == j).astype(F32))
    return jnp.concatenate([moved[:HS] + later[:HS], moved[HS:] + later[HS:]], axis=0)


def chunk_stages(chunks):
    i, j = iota((CHUNK, CHUNK), 0), iota((CHUNK, CHUNK), 1)
    tri = (i >= j).astype(BF)
    ones = head_ones()
    i, j = iota((W2, W2), 0), iota((W2, W2), 1)
    same = (i < HS) == (j < HS)
    strict = same & (i > j)
    incl = same & (i >= j)
    made = []
    for r, k, v, pre, lr in chunks:
        logw = jax.nn.sigmoid(pre) * (-0.6065306597126334)
        a1 = logw.astype(BF)
        a2, a3 = halves(logw - a1.astype(F32))
        cum = dg(tri, a1) + (dg(tri, a2) + dg(tri, a3))
        last = cum[CHUNK - 1 :, :]
        grown = jnp.exp(-cum)
        tail = jnp.exp(last - cum)
        unit = k / jnp.maximum(jnp.sqrt(dot2(k * k, ones)), 1.0)
        ins = unit * jax.nn.sigmoid(lr)
        us = stacked(-jnp.exp(cum - logw) * unit)
        rs = stacked(jnp.exp(cum) * r)
        made.append(
            dict(
                last=last,
                us=us,
                rs=rs,
                left=halves(jnp.concatenate([us, rs], axis=0)),
                right=halves(
                    jnp.concatenate([stacked(ins * grown), stacked(k * grown)], axis=0)
                ),
                bts=halves(stacked(ins * tail)),
                kts=halves(stacked(k * tail)),
                v=stacked(v),
            )
        )
    for m in made:
        gram = dot_halves(m["left"], m["right"], NT)
        m["lb"] = jnp.where(strict, gram[:W2, :W2], 0.0)
        m["lk"] = jnp.where(strict, gram[:W2, W2:], 0.0)
        m["mb"] = jnp.where(incl, gram[W2:, :W2], 0.0)
        m["mk"] = jnp.where(incl, gram[W2:, W2:], 0.0)
        m["vs"] = m["v"].astype(BF)
    for m in made:
        m["lkv"] = dot2(m["lk"], m["vs"])
        m["mkv"] = dot2(m["mk"], m["vs"])
    size = 1
    while size < CHUNK:
        row, col = i // size, j // size
        below = (row == col + 1) & (row % 2 == 1)
        if size == 1:
            for m in made:
                m["inv"] = (i == j).astype(F32) + jnp.where(below, m["lb"], 0.0)
        else:
            held = [halves(m["inv"]) for m in made]
            mid = [
                dot_halves(h, halves(jnp.where(below, m["lb"], 0.0))) for h, m in zip(held, made)
            ]
            for m, h, x in zip(made, held, mid):
                m["inv"] = m["inv"] + dot_halves(halves(x), h)
        size *= 2
        if size == 8:
            yield
    for m in made:
        m["tuv"] = dot3(m["inv"], jnp.concatenate([m["us"], m["lkv"]], axis=1))
    out = []
    for m in made:
        turned = dot_halves(halves(m["tuv"].T), m["bts"])
        trans = folded(jnp.where(i == j, jnp.exp(m["last"]) - 1.0, 0.0) + turned[:W2])
        vt = m["v"].T.astype(BF)
        state = folded(turned[W2:] + dg(vt, m["kts"][0]) + dg(vt, m["kts"][1]))
        m["pair"] = jnp.concatenate([trans, state], axis=0)
    for m in made:
        muv = dot_halves(halves(m["mb"]), halves(m["tuv"]))
        out.append(
            (m["pair"], folded(m["rs"] + muv[:, :W2]), folded(muv[:, W2:] + m["mkv"]))
        )
    return out


def kernel(
    nz,
    ny,
    ntp,
    r_in,
    k_in,
    v_in,
    pre_in,
    lr_in,
    og_in,
    stw_in,
    hg_in,
    ow_in,
    res_in,
    gain_in,
    gate_in,
    up_in,
    down_in,
    out_ref,
    r_ref,
    k_ref,
    v_ref,
    pre_ref,
    lr_ref,
    og_ref,
    stw_ref,
    hg_ref,
    gain_ref,
    gu,
    dn,
    ow,
    res,
    py,
    pz,
    entry,
    seen_ref,
    local_ref,
    self_ref,
    mx,
    am,
    normed,
    hid,
    part,
    got,
    pgot,
    comb,
    early_sum,
    lsem,
    ssem,
    rsem,
):
    z, y, tp = lax.axis_index("z"), lax.axis_index("y"), lax.axis_index("tp")
    rows = r_in.shape[0]
    chunks = rows // CHUNK
    own = rows // ntp
    width = res_in.shape[1]
    half_f = gate_in.shape[0]
    ff = gate_in.shape[1]
    half_ring = nz // 2
    nx = ntp // 2
    xx, core = tp // 2, tp % 2

    def zof(step):
        return lax.rem(z + step + nz, nz)

    def yof(step):
        return lax.rem(y + step + ny, ny)

    def tof(step):
        return lax.rem(tp + step + ntp, ntp)

    def sp(zz, yy):
        return zz * ny + yy

    def dev(zz=None, yy=None, tt=None):
        return {"z": z if zz is None else zz, "y": y if yy is None else yy, "tp": tp if tt is None else tt}

    scope = [None]

    def mark(name):
        if scope[0] is not None:
            scope[0].__exit__(None, None, None)
        scope[0] = None
        if name:
            scope[0] = jax.named_scope(name)
            scope[0].__enter__()

    mark("enter")
    here = sp(z, y)
    weights = [
        (gate_in, gu.at[here, 0:half_f]),
        (up_in, gu.at[here, half_f : 2 * half_f]),
        (down_in, dn.at[here]),
        (ow_in, ow.at[tp]),
    ]
    streams = [
        (pre_in, pre_ref),
        (k_in, k_ref),
        (lr_in, lr_ref),
        (r_in, r_ref),
        (v_in, v_ref),
        (og_in, og_ref),
        (stw_in, stw_ref),
        (hg_in, hg_ref),
        (gain_in, gain_ref),
        (res_in, res),
    ]
    loads = [
        pltpu.make_async_copy(src, dst, lsem.at[i])
        for i, (src, dst) in enumerate(weights + streams)
    ]
    for load in loads[len(weights) :] + loads[: len(weights)]:
        load.start()

    barrier = pltpu.get_barrier_semaphore()
    peers = [dev(zz=zof(1)), dev(zz=zof(-1))]
    peers += [dev(yy=yof(d)) for d in range(1, ny)]
    peers += [dev(tt=tof(d)) for d in range(1, ntp)]
    for peer in peers:
        pl.semaphore_signal(barrier, inc=1, device_id=peer, device_id_type=pl.DeviceIdType.MESH)
    early = len(weights) + 5
    for load in loads[len(weights) : early]:
        load.wait()
    mark("recur_a")
    spans = [pl.ds(c * CHUNK, CHUNK) for c in range(chunks)]
    given = []
    for span in spans:
        r, k, v = (ref[span, :].astype(F32) for ref in (r_ref, k_ref, v_ref))
        given.append((r, k, v, pre_ref[span, :], lr_ref[span, :]))
    stages = chunk_stages(given)
    next(stages)
    mark("greet")
    pl.semaphore_wait(barrier, len(peers))
    for load in loads[: len(weights)]:
        load.wait()

    count = [0]

    def channel():
        count[0] += 1
        return count[0] - 1

    def copy(src, dst, out, ch, device):
        return pltpu.make_async_remote_copy(
            src_ref=src,
            dst_ref=dst,
            send_sem=ssem.at[out],
            recv_sem=rsem.at[ch],
            device_id=device,
            device_id_type=pl.DeviceIdType.MESH,
        )

    GU, DN, PS, PY, OW, MX, PART, COMB = range(8)

    def send(ref, out, ch, device):
        copy(ref, ref, out, ch, device).start()

    def arrived(ref, ch):
        copy(ref, ref, 0, ch, dev(zz=zof(1))).wait_recv()

    class Ring:
        def __init__(self, block, out, one, two):
            self.block, self.out, self.one, self.two = block, out, one, two
            self.ch = [channel() for _ in range(half_ring)]
            self.step = 1

        def piece(self, s, side):
            return side if s == half_ring else None

        def push(self, s):
            ch = self.ch[s - 1]
            send(self.block(zof(1 - s), self.piece(s, 0)), self.out, ch, dev(zz=zof(1)))
            send(self.block(zof(s - 1), self.piece(s, 1)), self.out, ch, dev(zz=zof(-1)))

        def turn(self):
            s = self.step
            if s > half_ring:
                return
            arrived(self.one if s == half_ring else self.two, self.ch[s - 1])
            if s < half_ring:
                self.push(s + 1)
            self.step = s + 1

    class PairRing:
        def __init__(self):
            self.ch = [(channel(), channel()) for _ in range(half_ring)]

        def part(self, zz, half):
            return pz.at[zz, half * HS : (half + 1) * HS]

        def push(self, s, half):
            ch = self.ch[s - 1][half]
            if s < half_ring or half == 0:
                send(self.part(zof(1 - s), half), PS, ch, dev(zz=zof(1)))
            if s < half_ring or half == 1:
                send(self.part(zof(s - 1), half), PS, ch, dev(zz=zof(-1)))

        def turn(self, s):
            for half in range(2):
                arrived(pz.at[0] if s < half_ring else self.part(0, half), self.ch[s - 1][half])
                if s < half_ring:
                    self.push(s + 1, half)

    class Across:
        def __init__(self, block, at, to, out, one, two, last=None):
            self.block, self.at, self.to, self.out = block, at, to, out
            self.one, self.two = one, two
            self.first = channel()
            self.last = channel() if last is None else last

        def push(self):
            send(self.block(self.at(0), None), self.out, self.first, self.to(1))
            send(self.block(self.at(0), None), self.out, self.first, self.to(-1))

        def forward(self):
            arrived(self.two, self.first)
            send(self.block(self.at(-1), 0), self.out, self.last, self.to(1))
            send(self.block(self.at(1), 1), self.out, self.last, self.to(-1))

        def finish(self):
            arrived(self.one, self.last)

    def cut(ref, piece, length):
        if piece is None:
            return ref
        middle = (length // 2 + 7) // 8 * 8
        return ref.at[0:middle] if piece == 0 else ref.at[middle:length]

    a_rows = 2 * half_f
    b_rows = half_f

    def gu_block(zz, yy, piece):
        return cut(gu.at[sp(zz, yy)], piece, a_rows)

    def dn_block(zz, yy, piece):
        return cut(dn.at[sp(zz, yy)], piece, b_rows)

    def y_dev(d):
        return dev(yy=yof(d))

    ring_gu = Ring(lambda zz, piece: gu_block(zz, y, piece), GU, gu.at[0], gu.at[0:2])
    ring_dn = [
        Ring(
            functools.partial(lambda k, zz, piece: dn_block(zz, yof(k), piece), k),
            DN,
            dn.at[0],
            dn.at[0:2],
        )
        for k in (0, 1, -1, 2)
    ]
    ring_ps = PairRing()
    order = [0]
    for s in range(1, half_ring):
        order += [-s, s]
    order += [half_ring]
    late = max(1, nz // 4)
    far_early, far_late = channel(), channel()
    across = [
        Across(
            functools.partial(lambda step, yy, piece: gu_block(zof(step), yy, piece), step),
            yof,
            y_dev,
            GU,
            gu.at[0:late] if i >= nz - late else gu.at[0 : nz - late],
            gu.at[0:2],
            far_late if i >= nz - late else far_early,
        )
        for i, step in enumerate(order)
    ]
    across_dn = Across(
        lambda yy, piece: dn_block(z, yy, piece), yof, y_dev, DN, dn.at[0], dn.at[0:2]
    )

    progress = {"push": 1, "forward": 0, "dn": 0}

    def turn_gu():
        ring_gu.turn()

    def turn_dn(n=1):
        for _ in range(n):
            ring_dn[progress["dn"] % 4].turn()
            progress["dn"] += 1

    def y_push(n=1):
        for _ in range(n):
            i = progress["push"]
            if i < len(across) and (i + 1) // 2 < ring_gu.step:
                across[i].push()
                progress["push"] += 1

    def y_forward(n=1):
        for _ in range(n):
            if progress["forward"] < progress["push"]:
                across[progress["forward"]].forward()
                progress["forward"] += 1

    def same_core(d):
        return lax.rem(xx + d + nx, nx) * 2 + core

    def other_core(d):
        return lax.rem(xx + d + nx, nx) * 2 + (1 - core)

    def x_dev(d):
        return dev(tt=same_core(d))

    partner = other_core(0)
    near = dev(tt=partner)
    across_ow = None
    if nx == 4:
        across_ow = Across(
            lambda t, piece: cut(ow.at[t], piece, W2),
            same_core,
            x_dev,
            OW,
            ow.at[0],
            ow.at[0:2],
        )
    ow_far = [channel() for _ in range(1, nx)] if across_ow is None else []
    ow_near = channel()

    def ow_share(d):
        send(ow.at[same_core(d)], OW, ow_near, near)

    def ow_start():
        if across_ow is not None:
            across_ow.push()
        else:
            for d in range(1, nx):
                send(ow.at[tp], OW, ow_far[d - 1], x_dev(d))
        ow_share(0)

    def ow_middle():
        if across_ow is not None:
            across_ow.forward()
            ow_share(1)
            ow_share(-1)

    def ow_last():
        if across_ow is not None:
            across_ow.finish()
            ow_share(2)
        else:
            for d in range(1, nx):
                arrived(ow.at[0], ow_far[d - 1])
                ow_share(-d)

    def ow_finish():
        arrived(ow.at[0:nx], ow_near)

    mark("launch")
    ring_gu.push(1)
    ring_dn[0].push(1)
    across_dn.push()
    across[0].push()
    ow_start()
    for load in loads[early:]:
        load.wait()

    mark("recur")
    ones = head_ones()
    try:
        next(stages)
    except StopIteration as end:
        made = end.value
    pair = None
    for c, (ps, seen, local) in enumerate(made):
        seen_ref[spans[c], :] = seen
        local_ref[spans[c], :] = local
        pair = ps if pair is None else compose(pair, ps)
        if c < chunks - 1:
            entry[c] = pair
    mark("scan_y")
    py[y] = pair.astype(BF)
    ch_y = channel()
    for d in (2, 1, 3) if ny == 4 else range(1, ny):
        send(py.at[y], PY, ch_y, dev(yy=yof(d)))
    mark("pre_gu")
    turn_gu()
    mark("pre_dn")
    ring_dn[0].turn()
    mark("pre_dny")
    across_dn.forward()
    stw = stw_ref[...]
    stw = jnp.concatenate([stw[0:1], stw[1:2]], axis=1)
    for c, (r, k, v, _, _) in enumerate(given):
        self_ref[spans[c], :] = dot2(r * k * stw, ones) * v
    mark("pre_y0")
    y_forward()
    y_push()
    mark("scan_ywait")
    arrived(py.at[0 : ny - 1], ch_y)
    mark("scan_yfix")
    inside = jnp.zeros((W2, W2), F32)
    running = py[0].astype(F32)
    for yy in range(1, ny):
        inside = jnp.where(y == yy, running, inside)
        running = compose(running, py[yy].astype(F32))
    pz[z] = running.astype(BF)
    ring_ps.push(1, 0)
    ring_ps.push(1, 1)
    mark("pre_dn2")
    ring_dn[1].push(1)
    ring_dn[2].push(1)
    across_dn.finish()
    ring_dn[3].push(1)
    turn_gu()
    y_push(2)
    progress["dn"] = 1

    trans_left = jnp.zeros((HS, W2), F32)
    state_left = jnp.zeros((HS, W2), F32)
    state_right = jnp.zeros((HS, W2), F32)
    for s in range(1, half_ring + 1):
        mark(f"scan_z{s}")
        ring_ps.turn(s)
        mark(f"bulk{s}")
        if s < half_ring:
            if s in (1, 2, 4, 5, 7):
                turn_gu()
                turn_dn(2)
            else:
                turn_dn(3)
            y_push(2)
            mark(f"yfwd{s}")
            y_forward(2 if s % 2 == 0 else 1)
        mark(f"calc{s}")
        if s == half_ring // 2:
            ow_middle()
        if s == half_ring - 1:
            ow_last()
        left = pz[zof(-s)]
        has_left = z >= s
        hi, lo = halves(stacked(trans_left))
        moved = dg(left, hi) + dg(left, lo) + left.astype(F32)
        trans_left = jnp.where(has_left, trans_left + moved[:HS], trans_left)
        state_left = jnp.where(has_left, state_left + moved[HS:], state_left)
        if s < half_ring:
            right = pz[zof(s)].astype(F32)
            has_right = z + s >= nz
            moved = dot2(state_right, stacked(right[:HS]).astype(BF)) + right[HS:]
            state_right = jnp.where(has_right, state_right + moved, state_right)
    mark("state")
    state = state_right + dot3(state_right, stacked(trans_left)) + state_left
    state = state + dot3(state, stacked(inside[:HS])) + inside[HS:]

    mark("mech")
    seen = []
    for c in range(chunks):
        at = state
        if c > 0:
            at = state + dot3(state, stacked(entry[c - 1][:HS])) + entry[c - 1][HS:]
        seen.append(dot3(seen_ref[spans[c], :], stacked(at), NT))
    o = jnp.concatenate(seen, axis=0) + local_ref[...]
    shifted = o - dot2(o, ones) * (1.0 / HS)
    spread = dot2(shifted * shifted, ones) * (1.0 / HS)
    merged = shifted * lax.rsqrt(spread + GROUP_EPS) * hg_ref[...] + self_ref[...]
    mx[tp] = (merged * jax.nn.sigmoid(og_ref[...].astype(F32))).astype(BF)
    mx_far = [channel() for _ in range(1, nx)]
    mx_near = channel()
    x_order = [2, 1, 3] if nx == 4 else list(range(1, nx))
    for d in x_order:
        send(mx.at[tp], MX, mx_far[d - 1], x_dev(d))
    send(mx.at[tp], MX, mx_near, near)
    mark("exch_pump")
    turn_dn(2)
    y_forward()
    turn_gu()
    y_push(2)
    turn_dn(2)
    y_forward()
    mark("exch_far")
    for d in reversed(x_order):
        arrived(mx.at[0], mx_far[d - 1])
        send(mx.at[same_core(-d)], MX, mx_near, near)
    mark("exch_pump2")
    turn_dn(2)
    y_forward()
    mark("exch_near")
    arrived(mx.at[0:nx], mx_near)
    mark("exch_ow")
    ow_finish()
    mark("exch_pump3")
    turn_dn(1)
    y_push(2)
    y_forward()

    mark("project")
    tile = min(256, width // 4)
    tiles = width // tile
    lhs = jnp.concatenate([mx[g] for g in range(ntp)], axis=1)

    def project(n, square):
        cols = pl.ds(pl.multiple_of(n * tile, tile), tile)
        mix = dg(lhs, ow[:, :, cols].reshape(ntp * W2, tile)).astype(BF).astype(F32)
        after = (res[:, cols].astype(F32) + mix).astype(BF).astype(F32)
        am[:, cols] = after
        sq = after * after
        for q in range(tile // W2):
            square = square + sq[:, q * W2 : (q + 1) * W2]
        return square

    square = jnp.zeros((rows, W2), F32)
    square = lax.fori_loop(0, tiles, project, square, unroll=2)
    mark("norm")
    y_push(2)
    y_forward()
    turn_dn(1)
    y_forward()
    turn_dn(1)
    scale = lax.rsqrt(jnp.sum(square, axis=1, keepdims=True) * (1.0 / width) + NORM_EPS)

    def normalize(n, carry):
        cols = pl.ds(pl.multiple_of(n * tile, tile), tile)
        normed[:, cols] = (am[:, cols] * scale * gain_ref[:, cols]).astype(BF)
        return carry

    lax.fori_loop(0, tiles, normalize, 0)
    mark("pumprest")
    while progress["forward"] < len(across):
        turn_gu()
        y_push(2)
        y_forward()
        turn_dn()
    z_rows = ny * half_f

    def gate_up(steps, at, wide):
        x = jnp.concatenate(
            [normed[:, pl.ds(pl.multiple_of(zof(t) * z_rows, z_rows), z_rows)] for t in steps],
            axis=1,
        )
        sums = []
        for first in (0, half_f):
            w = [
                gu[pl.ds(zof(t) * ny, ny), first : first + half_f, at : at + wide].reshape(
                    z_rows, wide
                )
                for t in steps
            ]
            sums.append(dg(x, jnp.concatenate(w, axis=0)))
        return sums

    bands = [(at, min(256, ff - at)) for at in range(0, ff, 256)]
    mark("finish_a")
    across[0].finish()
    mark("gateup_a")
    for at, wide in bands:
        gate, up = gate_up(order[: nz - late], at, wide)
        early_sum[0, :, at : at + wide] = gate
        early_sum[1, :, at : at + wide] = up
        turn_dn()
    mark("finish_b")
    turn_dn(2)
    across[-1].finish()
    mark("gateup_b")
    for at, wide in bands:
        gate, up = gate_up(order[nz - late :], at, wide)
        gate = gate + early_sum[0, :, at : at + wide]
        up = up + early_sum[1, :, at : at + wide]
        hid[:, at : at + wide] = (gate / (1.0 + jnp.exp(-gate)) * up).astype(BF)
    mark("dnwait")
    turn_dn(4 * half_ring)

    slots = tile // half_f

    def down(n, carry):
        cols = pl.ds(pl.multiple_of(n * tile, tile), tile)
        w = dn[pl.ds(n * slots, slots)].reshape(tile, ff)
        prod = dg(hid[...], w, NT).reshape(nx, 2, own, tile).astype(BF)
        part[0, :, :, cols] = prod[:, 0]
        part[1, :, :, cols] = prod[:, 1]
        return carry

    cuts = 4
    quarter = width // cuts
    pieces = [pl.ds(piece * quarter, quarter) for piece in range(cuts)]
    ch_core = [channel() for _ in range(cuts)]
    ch_part = [channel() for _ in range(cuts)]

    def x_at(d):
        return lax.rem(xx + d + nx, nx)

    def add_cores(piece):
        cols = pieces[piece]
        arrived(pgot.at[:, :, cols], ch_core[piece])
        for d in [2, 1, 3] if nx == 4 else range(1, nx):
            both = part[core, x_at(d), :, cols].astype(F32) + pgot[x_at(d), :, cols].astype(F32)
            comb[d - 1, :, cols] = both.astype(BF)
            copy(
                comb.at[d - 1, :, cols], got.at[d - 1, :, cols], COMB, ch_part[piece], x_dev(d)
            ).start()

    for piece, cols in enumerate(pieces):
        mark(f"down{piece}")
        lax.fori_loop(piece * tiles // cuts, (piece + 1) * tiles // cuts, down, 0, unroll=True)
        copy(
            part.at[1 - core, :, :, cols], pgot.at[:, :, cols], PART, ch_core[piece], near
        ).start()
        if piece >= 2:
            add_cores(piece - 2)
    mark("rs_core")
    add_cores(cuts - 2)
    add_cores(cuts - 1)
    mark("rs_wait")
    for piece, cols in enumerate(pieces):
        total = am[pl.ds(pl.multiple_of(tp * own, own), own), cols]
        total = total + part[core, xx, :, cols].astype(F32) + pgot[xx, :, cols].astype(F32)
        if nx > 1:
            arrived(got.at[:, :, cols], ch_part[piece])
        for d in range(1, nx):
            total = total + got[d - 1, :, cols].astype(F32)
        out_ref[:, cols] = total.astype(BF)
    mark("sendwait")
    gone = [
        (gu.at[0 : nz * ny - 1], GU),
        (dn.at[0 : nz * ny - 1], DN),
        (pz.at[0 : nz - 1], PS),
        (py.at[0 : ny - 1], PY),
        (ow.at[0 : ntp - 1], OW),
        (mx.at[0 : ntp - 1], MX),
        (part.at[0], PART),
    ]
    if nx > 1:
        gone.append((comb, COMB))
    for ref, out in gone:
        copy(ref, ref, out, 0, near).wait_send()
    mark(None)
    assert count[0] <= SEMS, count[0]


def per_device(
    nz,
    ny,
    ntp,
    receptance,
    head_keys,
    head_values,
    decay_preact,
    learning_rate_preact,
    output_gate_preact,
    self_token_weight,
    head_norm_gain,
    output_weight,
    residual,
    premixer_norm_gain,
    mixer_gate_weight,
    mixer_up_weight,
    mixer_down_weight,
):
    rows = receptance.shape[0]
    width = residual.shape[1]
    half_f, ff = mixer_gate_weight.shape
    own = rows // ntp
    nx = ntp // 2
    vmem = pl.BlockSpec(memory_space=pltpu.VMEM)
    hbm = pl.BlockSpec(memory_space=pltpu.HBM)
    return pl.pallas_call(
        functools.partial(kernel, nz, ny, ntp),
        out_shape=jax.ShapeDtypeStruct((own, width), BF),
        in_specs=[hbm] * 14,
        out_specs=vmem,
        scratch_shapes=[
            pltpu.VMEM((rows, W2), BF),
            pltpu.VMEM((rows, W2), BF),
            pltpu.VMEM((rows, W2), BF),
            pltpu.VMEM((rows, W2), F32),
            pltpu.VMEM((rows, W2), F32),
            pltpu.VMEM((rows, W2), BF),
            pltpu.VMEM((2, HS), F32),
            pltpu.VMEM((1, W2), F32),
            pltpu.VMEM((1, width), F32),
            pltpu.VMEM((nz * ny, 2 * half_f, ff), BF),
            pltpu.VMEM((nz * ny, half_f, ff), BF),
            pltpu.VMEM((ntp, W2, width), BF),
            pltpu.VMEM((rows, width), BF),
            pltpu.VMEM((ny, W2, W2), BF),
            pltpu.VMEM((nz, W2, W2), BF),
            pltpu.VMEM((rows // CHUNK, W2, W2), F32),
            pltpu.VMEM((rows, W2), F32),
            pltpu.VMEM((rows, W2), F32),
            pltpu.VMEM((rows, W2), F32),
            pltpu.VMEM((ntp, rows, W2), BF),
            pltpu.VMEM((rows, width), F32),
            pltpu.VMEM((rows, width), BF),
            pltpu.VMEM((rows, ff), BF),
            pltpu.VMEM((2, nx, own, width), BF),
            pltpu.VMEM((max(nx - 1, 1), own, width), BF),
            pltpu.VMEM((nx, own, width), BF),
            pltpu.VMEM((max(nx - 1, 1), own, width), BF),
            pltpu.VMEM((2, rows, ff), F32),
            pltpu.SemaphoreType.DMA((14,)),
            pltpu.SemaphoreType.DMA((8,)),
            pltpu.SemaphoreType.DMA((SEMS,)),
        ],
        compiler_params=pltpu.CompilerParams(
            collective_id=0, has_side_effects=True, vmem_limit_bytes=60 * 1024 * 1024
        ),
        name="layer",
    )(
        receptance,
        head_keys,
        head_values,
        decay_preact,
        learning_rate_preact,
        output_gate_preact,
        self_token_weight,
        head_norm_gain.reshape(1, -1),
        output_weight,
        residual,
        premixer_norm_gain.reshape(1, -1),
        mixer_gate_weight,
        mixer_up_weight,
        mixer_down_weight.T,
    )


def build(mesh, nz, ny):
    ntp = mesh.shape["tp"]
    torus = Mesh(mesh.devices.reshape(nz, ny, ntp), ("z", "y", "tp"))
    sp = ("z", "y")
    cut = P(sp, "tp")
    in_specs = (cut,) * 6 + (
        P("tp", None),
        P("tp"),
        P("tp", None),
        P(sp, None),
        P(),
        cut,
        cut,
        P("tp", sp),
    )
    return jax.shard_map(
        functools.partial(per_device, nz, ny, ntp),
        mesh=torus,
        in_specs=in_specs,
        out_specs=P(("z", "y", "tp"), None),
        check_vma=False,
    )


def solution(mesh):
    return build(mesh, 16, 4)
```

```python
import functools

import jax
import jax.numpy as jnp
from jax import lax
from jax.experimental import pallas as pl
from jax.experimental.pallas import tpu as pltpu
from jax.sharding import Mesh
from jax.sharding import PartitionSpec as P

HS = 64
CHUNK = 64
W2 = 2 * HS
GROUP_EPS = 0.00064
NORM_EPS = 1e-06
F32 = jnp.float32
BF = jnp.bfloat16
NN = (((1,), (0,)), ((), ()))
NT = (((1,), (1,)), ((), ()))
SEMS = 92


def dg(a, b, dims=NN):
    return lax.dot_general(a, b, dims, preferred_element_type=F32)


def halves(x):
    hi = x.astype(BF)
    return hi, (x - hi.astype(F32)).astype(BF)


def dot_halves(a, b, dims=NN):
    return dg(a[0], b[0], dims) + (dg(a[0], b[1], dims) + dg(a[1], b[0], dims))


def dot3(a, b, dims=NN):
    return dot_halves(halves(a), halves(b), dims)


def dot2(a, b, dims=NN):
    hi, lo = halves(a)
    return dg(hi, b, dims) + dg(lo, b, dims)


def iota(shape, dim):
    return lax.broadcasted_iota(jnp.int32, shape, dim)


def head_masks():
    lane = iota((1, W2), 1)
    first = (lane < HS).astype(F32)
    return first, 1.0 - first


def stacked(x):
    first, second = head_masks()
    return jnp.concatenate([x * first, x * second], axis=0)


def folded(x):
    half = x.shape[0] // 2
    return x[:half] + x[half:]


def head_ones():
    i, j = iota((W2, W2), 0), iota((W2, W2), 1)
    return ((i < HS) == (j < HS)).astype(BF)


def compose(earlier, later):
    later_d = stacked(later[:HS])
    i, j = iota((W2, W2), 0), iota((W2, W2), 1)
    moved = dot3(earlier, later_d + (i == j).astype(F32))
    return jnp.concatenate([moved[:HS] + later[:HS], moved[HS:] + later[HS:]], axis=0)


def chunk_stages(chunks):
    i, j = iota((CHUNK, CHUNK), 0), iota((CHUNK, CHUNK), 1)
    tri = (i >= j).astype(BF)
    ones = head_ones()
    i, j = iota((W2, W2), 0), iota((W2, W2), 1)
    same = (i < HS) == (j < HS)
    strict = same & (i > j)
    incl = same & (i >= j)
    made = []
    for r, k, v, pre, lr in chunks:
        logw = jax.nn.sigmoid(pre) * (-0.6065306597126334)
        a1 = logw.astype(BF)
        a2, a3 = halves(logw - a1.astype(F32))
        cum = dg(tri, a1) + (dg(tri, a2) + dg(tri, a3))
        last = cum[CHUNK - 1 :, :]
        grown = jnp.exp(-cum)
        tail = jnp.exp(last - cum)
        unit = k / jnp.maximum(jnp.sqrt(dot2(k * k, ones)), 1.0)
        ins = unit * jax.nn.sigmoid(lr)
        us = stacked(-jnp.exp(cum - logw) * unit)
        rs = stacked(jnp.exp(cum) * r)
        made.append(
            dict(
                last=last,
                us=us,
                rs=rs,
                left=halves(jnp.concatenate([us, rs], axis=0)),
                right=halves(
                    jnp.concatenate([stacked(ins * grown), stacked(k * grown)], axis=0)
                ),
                bts=halves(stacked(ins * tail)),
                kts=halves(stacked(k * tail)),
                v=stacked(v),
            )
        )
    for m in made:
        gram = dot_halves(m["left"], m["right"], NT)
        m["lb"] = jnp.where(strict, gram[:W2, :W2], 0.0)
        m["lk"] = jnp.where(strict, gram[:W2, W2:], 0.0)
        m["mb"] = jnp.where(incl, gram[W2:, :W2], 0.0)
        m["mk"] = jnp.where(incl, gram[W2:, W2:], 0.0)
        m["vs"] = m["v"].astype(BF)
    for m in made:
        m["lkv"] = dot2(m["lk"], m["vs"])
        m["mkv"] = dot2(m["mk"], m["vs"])
    size = 1
    while size < CHUNK:
        row, col = i // size, j // size
        below = (row == col + 1) & (row % 2 == 1)
        if size == 1:
            for m in made:
                m["inv"] = (i == j).astype(F32) + jnp.where(below, m["lb"], 0.0)
        else:
            held = [halves(m["inv"]) for m in made]
            mid = [
                dot_halves(h, halves(jnp.where(below, m["lb"], 0.0))) for h, m in zip(held, made)
            ]
            for m, h, x in zip(made, held, mid):
                m["inv"] = m["inv"] + dot_halves(halves(x), h)
        size *= 2
        if size == 8:
            yield
    for m in made:
        m["tuv"] = dot3(m["inv"], jnp.concatenate([m["us"], m["lkv"]], axis=1))
    out = []
    for m in made:
        turned = dot_halves(halves(m["tuv"].T), m["bts"])
        trans = folded(jnp.where(i == j, jnp.exp(m["last"]) - 1.0, 0.0) + turned[:W2])
        vt = m["v"].T.astype(BF)
        state = folded(turned[W2:] + dg(vt, m["kts"][0]) + dg(vt, m["kts"][1]))
        m["pair"] = jnp.concatenate([trans, state], axis=0)
    for m in made:
        muv = dot_halves(halves(m["mb"]), halves(m["tuv"]))
        out.append(
            (m["pair"], folded(m["rs"] + muv[:, :W2]), folded(muv[:, W2:] + m["mkv"]))
        )
    return out


def kernel(
    nz,
    ny,
    ntp,
    r_in,
    k_in,
    v_in,
    pre_in,
    lr_in,
    og_in,
    stw_in,
    hg_in,
    ow_in,
    res_in,
    gain_in,
    gate_in,
    up_in,
    down_in,
    out_ref,
    r_ref,
    k_ref,
    v_ref,
    pre_ref,
    lr_ref,
    og_ref,
    stw_ref,
    hg_ref,
    gain_ref,
    gu,
    dn,
    ow,
    res,
    py,
    pz,
    entry,
    seen_ref,
    local_ref,
    self_ref,
    mx,
    am,
    normed,
    hid,
    part,
    got,
    pgot,
    comb,
    early_sum,
    lsem,
    ssem,
    rsem,
):
    z, y, tp = lax.axis_index("z"), lax.axis_index("y"), lax.axis_index("tp")
    rows = r_in.shape[0]
    chunks = rows // CHUNK
    own = rows // ntp
    width = res_in.shape[1]
    half_f = gate_in.shape[0]
    ff = gate_in.shape[1]
    half_ring = nz // 2
    nx = ntp // 2
    xx, core = tp // 2, tp % 2

    def zof(step):
        return lax.rem(z + step + nz, nz)

    def yof(step):
        return lax.rem(y + step + ny, ny)

    def tof(step):
        return lax.rem(tp + step + ntp, ntp)

    def sp(zz, yy):
        return zz * ny + yy

    def dev(zz=None, yy=None, tt=None):
        return {"z": z if zz is None else zz, "y": y if yy is None else yy, "tp": tp if tt is None else tt}

    scope = [None]

    def mark(name):
        if scope[0] is not None:
            scope[0].__exit__(None, None, None)
        scope[0] = None
        if name:
            scope[0] = jax.named_scope(name)
            scope[0].__enter__()

    mark("enter")
    here = sp(z, y)
    weights = [
        (gate_in, gu.at[here, 0:half_f]),
        (up_in, gu.at[here, half_f : 2 * half_f]),
        (down_in, dn.at[here]),
        (ow_in, ow.at[tp]),
    ]
    streams = [
        (pre_in, pre_ref),
        (k_in, k_ref),
        (lr_in, lr_ref),
        (r_in, r_ref),
        (v_in, v_ref),
        (og_in, og_ref),
        (stw_in, stw_ref),
        (hg_in, hg_ref),
        (gain_in, gain_ref),
        (res_in, res),
    ]
    loads = [
        pltpu.make_async_copy(src, dst, lsem.at[i])
        for i, (src, dst) in enumerate(weights + streams)
    ]
    for load in loads[len(weights) :] + loads[: len(weights)]:
        load.start()

    barrier = pltpu.get_barrier_semaphore()
    peers = [dev(zz=zof(1)), dev(zz=zof(-1))]
    peers += [dev(yy=yof(d)) for d in range(1, ny)]
    peers += [dev(tt=tof(d)) for d in range(1, ntp)]
    for peer in peers:
        pl.semaphore_signal(barrier, inc=1, device_id=peer, device_id_type=pl.DeviceIdType.MESH)
    early = len(weights) + 5
    for load in loads[len(weights) : early]:
        load.wait()
    mark("recur_a")
    spans = [pl.ds(c * CHUNK, CHUNK) for c in range(chunks)]
    given = []
    for span in spans:
        r, k, v = (ref[span, :].astype(F32) for ref in (r_ref, k_ref, v_ref))
        given.append((r, k, v, pre_ref[span, :], lr_ref[span, :]))
    stages = chunk_stages(given)
    next(stages)
    mark("greet")
    pl.semaphore_wait(barrier, len(peers))
    for load in loads[: len(weights)]:
        load.wait()

    count = [0]

    def channel():
        count[0] += 1
        return count[0] - 1

    def copy(src, dst, out, ch, device):
        return pltpu.make_async_remote_copy(
            src_ref=src,
            dst_ref=dst,
            send_sem=ssem.at[out],
            recv_sem=rsem.at[ch],
            device_id=device,
            device_id_type=pl.DeviceIdType.MESH,
        )

    GU, DN, PS, PY, OW, MX, PART, COMB = range(8)

    def send(ref, out, ch, device):
        copy(ref, ref, out, ch, device).start()

    def arrived(ref, ch):
        copy(ref, ref, 0, ch, dev(zz=zof(1))).wait_recv()

    class Ring:
        def __init__(self, block, out, one, two):
            self.block, self.out, self.one, self.two = block, out, one, two
            self.ch = [channel() for _ in range(half_ring)]
            self.step = 1

        def piece(self, s, side):
            return side if s == half_ring else None

        def push(self, s):
            ch = self.ch[s - 1]
            send(self.block(zof(1 - s), self.piece(s, 0)), self.out, ch, dev(zz=zof(1)))
            send(self.block(zof(s - 1), self.piece(s, 1)), self.out, ch, dev(zz=zof(-1)))

        def turn(self):
            s = self.step
            if s > half_ring:
                return
            arrived(self.one if s == half_ring else self.two, self.ch[s - 1])
            if s < half_ring:
                self.push(s + 1)
            self.step = s + 1

    class PairRing:
        def __init__(self):
            self.ch = [(channel(), channel()) for _ in range(half_ring)]

        def part(self, zz, half):
            return pz.at[zz, half * HS : (half + 1) * HS]

        def push(self, s, half):
            ch = self.ch[s - 1][half]
            if s < half_ring or half == 0:
                send(self.part(zof(1 - s), half), PS, ch, dev(zz=zof(1)))
            if s < half_ring or half == 1:
                send(self.part(zof(s - 1), half), PS, ch, dev(zz=zof(-1)))

        def turn(self, s):
            for half in range(2):
                arrived(pz.at[0] if s < half_ring else self.part(0, half), self.ch[s - 1][half])
                if s < half_ring:
                    self.push(s + 1, half)

    class Across:
        def __init__(self, block, at, to, out, one, two, last=None):
            self.block, self.at, self.to, self.out = block, at, to, out
            self.one, self.two = one, two
            self.first = channel()
            self.last = channel() if last is None else last

        def push(self):
            send(self.block(self.at(0), None), self.out, self.first, self.to(1))
            send(self.block(self.at(0), None), self.out, self.first, self.to(-1))

        def forward(self):
            arrived(self.two, self.first)
            send(self.block(self.at(-1), 0), self.out, self.last, self.to(1))
            send(self.block(self.at(1), 1), self.out, self.last, self.to(-1))

        def finish(self):
            arrived(self.one, self.last)

    def cut(ref, piece, length):
        if piece is None:
            return ref
        middle = (length // 2 + 7) // 8 * 8
        return ref.at[0:middle] if piece == 0 else ref.at[middle:length]

    a_rows = 2 * half_f
    b_rows = half_f

    def gu_block(zz, yy, piece):
        return cut(gu.at[sp(zz, yy)], piece, a_rows)

    def dn_block(zz, yy, piece):
        return cut(dn.at[sp(zz, yy)], piece, b_rows)

    def y_dev(d):
        return dev(yy=yof(d))

    ring_gu = Ring(lambda zz, piece: gu_block(zz, y, piece), GU, gu.at[0], gu.at[0:2])
    ring_dn = [
        Ring(
            functools.partial(lambda k, zz, piece: dn_block(zz, yof(k), piece), k),
            DN,
            dn.at[0],
            dn.at[0:2],
        )
        for k in (0, 1, -1, 2)
    ]
    ring_ps = PairRing()
    order = [0]
    for s in range(1, half_ring):
        order += [-s, s]
    order += [half_ring]
    late = max(1, nz // 4)
    far_early, far_late = channel(), channel()
    across = [
        Across(
            functools.partial(lambda step, yy, piece: gu_block(zof(step), yy, piece), step),
            yof,
            y_dev,
            GU,
            gu.at[0:late] if i >= nz - late else gu.at[0 : nz - late],
            gu.at[0:2],
            far_late if i >= nz - late else far_early,
        )
        for i, step in enumerate(order)
    ]
    across_dn = Across(
        lambda yy, piece: dn_block(z, yy, piece), yof, y_dev, DN, dn.at[0], dn.at[0:2]
    )

    progress = {"push": 1, "forward": 0, "dn": 0}

    def turn_gu():
        ring_gu.turn()

    def turn_dn(n=1):
        for _ in range(n):
            ring_dn[progress["dn"] % 4].turn()
            progress["dn"] += 1

    def y_push(n=1):
        for _ in range(n):
            i = progress["push"]
            if i < len(across) and (i + 1) // 2 < ring_gu.step:
                across[i].push()
                progress["push"] += 1

    def y_forward(n=1):
        for _ in range(n):
            if progress["forward"] < progress["push"]:
                across[progress["forward"]].forward()
                progress["forward"] += 1

    def same_core(d):
        return lax.rem(xx + d + nx, nx) * 2 + core

    def other_core(d):
        return lax.rem(xx + d + nx, nx) * 2 + (1 - core)

    def x_dev(d):
        return dev(tt=same_core(d))

    partner = other_core(0)
    near = dev(tt=partner)
    across_ow = None
    if nx == 4:
        across_ow = Across(
            lambda t, piece: cut(ow.at[t], piece, W2),
            same_core,
            x_dev,
            OW,
            ow.at[0],
            ow.at[0:2],
        )
    ow_far = [channel() for _ in range(1, nx)] if across_ow is None else []
    ow_near = channel()

    def ow_share(d):
        send(ow.at[same_core(d)], OW, ow_near, near)

    def ow_start():
        if across_ow is not None:
            across_ow.push()
        else:
            for d in range(1, nx):
                send(ow.at[tp], OW, ow_far[d - 1], x_dev(d))
        ow_share(0)

    def ow_middle():
        if across_ow is not None:
            across_ow.forward()
            ow_share(1)
            ow_share(-1)

    def ow_last():
        if across_ow is not None:
            across_ow.finish()
            ow_share(2)
        else:
            for d in range(1, nx):
                arrived(ow.at[0], ow_far[d - 1])
                ow_share(-d)

    def ow_finish():
        arrived(ow.at[0:nx], ow_near)

    mark("launch")
    ring_gu.push(1)
    ring_dn[0].push(1)
    across_dn.push()
    across[0].push()
    ow_start()
    for load in loads[early:]:
        load.wait()

    mark("recur")
    ones = head_ones()
    try:
        next(stages)
    except StopIteration as end:
        made = end.value
    pair = None
    for c, (ps, seen, local) in enumerate(made):
        seen_ref[spans[c], :] = seen
        local_ref[spans[c], :] = local
        pair = ps if pair is None else compose(pair, ps)
        if c < chunks - 1:
            entry[c] = pair
    mark("scan_y")
    py[y] = pair.astype(BF)
    ch_y = channel()
    for d in (2, 1, 3) if ny == 4 else range(1, ny):
        send(py.at[y], PY, ch_y, dev(yy=yof(d)))
    mark("pre_gu")
    turn_gu()
    mark("pre_dn")
    ring_dn[0].turn()
    mark("pre_dny")
    across_dn.forward()
    stw = stw_ref[...]
    stw = jnp.concatenate([stw[0:1], stw[1:2]], axis=1)
    for c, (r, k, v, _, _) in enumerate(given):
        self_ref[spans[c], :] = dot2(r * k * stw, ones) * v
    mark("pre_y0")
    y_forward()
    y_push()
    mark("scan_ywait")
    arrived(py.at[0 : ny - 1], ch_y)
    mark("scan_yfix")
    inside = jnp.zeros((W2, W2), F32)
    running = py[0].astype(F32)
    for yy in range(1, ny):
        inside = jnp.where(y == yy, running, inside)
        running = compose(running, py[yy].astype(F32))
    pz[z] = running.astype(BF)
    ring_ps.push(1, 0)
    ring_ps.push(1, 1)
    mark("pre_dn2")
    ring_dn[1].push(1)
    ring_dn[2].push(1)
    across_dn.finish()
    ring_dn[3].push(1)
    turn_gu()
    y_push(2)
    progress["dn"] = 1

    trans_left = jnp.zeros((HS, W2), F32)
    state_left = jnp.zeros((HS, W2), F32)
    state_right = jnp.zeros((HS, W2), F32)
    for s in range(1, half_ring + 1):
        mark(f"scan_z{s}")
        ring_ps.turn(s)
        mark(f"bulk{s}")
        if s < half_ring:
            if s in (1, 2, 4, 5, 7):
                turn_gu()
                turn_dn(2)
            else:
                turn_dn(3)
            y_push(2)
            mark(f"yfwd{s}")
            y_forward(2 if s % 2 == 0 else 1)
        mark(f"calc{s}")
        if s == half_ring // 2:
            ow_middle()
        if s == half_ring - 1:
            ow_last()
        left = pz[zof(-s)]
        has_left = z >= s
        hi, lo = halves(stacked(trans_left))
        moved = dg(left, hi) + dg(left, lo) + left.astype(F32)
        trans_left = jnp.where(has_left, trans_left + moved[:HS], trans_left)
        state_left = jnp.where(has_left, state_left + moved[HS:], state_left)
        if s < half_ring:
            right = pz[zof(s)].astype(F32)
            has_right = z + s >= nz
            moved = dot2(state_right, stacked(right[:HS]).astype(BF)) + right[HS:]
            state_right = jnp.where(has_right, state_right + moved, state_right)
    mark("state")
    state = state_right + dot3(state_right, stacked(trans_left)) + state_left
    state = state + dot3(state, stacked(inside[:HS])) + inside[HS:]

    mark("mech")
    seen = []
    for c in range(chunks):
        at = state
        if c > 0:
            at = state + dot3(state, stacked(entry[c - 1][:HS])) + entry[c - 1][HS:]
        seen.append(dot3(seen_ref[spans[c], :], stacked(at), NT))
    o = jnp.concatenate(seen, axis=0) + local_ref[...]
    shifted = o - dot2(o, ones) * (1.0 / HS)
    spread = dot2(shifted * shifted, ones) * (1.0 / HS)
    merged = shifted * lax.rsqrt(spread + GROUP_EPS) * hg_ref[...] + self_ref[...]
    mx[tp] = (merged * jax.nn.sigmoid(og_ref[...].astype(F32))).astype(BF)
    mx_far = [channel() for _ in range(1, nx)]
    mx_near = channel()
    x_order = [2, 1, 3] if nx == 4 else list(range(1, nx))
    for d in x_order:
        send(mx.at[tp], MX, mx_far[d - 1], x_dev(d))
    send(mx.at[tp], MX, mx_near, near)
    mark("exch_pump")
    turn_gu()
    y_push(2)
    y_forward()
    turn_dn(4)
    y_forward()
    mark("exch_far")
    for d in reversed(x_order):
        arrived(mx.at[0], mx_far[d - 1])
        send(mx.at[same_core(-d)], MX, mx_near, near)
    mark("exch_pump2")
    turn_dn(2)
    y_forward()
    mark("exch_near")
    arrived(mx.at[0:nx], mx_near)
    mark("exch_ow")
    ow_finish()
    mark("exch_pump3")
    turn_dn(1)
    y_push(2)
    y_forward()

    mark("project")
    tile = min(256, width // 4)
    tiles = width // tile
    lhs = jnp.concatenate([mx[g] for g in range(ntp)], axis=1)

    def project(n, square):
        cols = pl.ds(pl.multiple_of(n * tile, tile), tile)
        mix = dg(lhs, ow[:, :, cols].reshape(ntp * W2, tile)).astype(BF).astype(F32)
        after = (res[:, cols].astype(F32) + mix).astype(BF).astype(F32)
        am[:, cols] = after
        sq = after * after
        for q in range(tile // W2):
            square = square + sq[:, q * W2 : (q + 1) * W2]
        return square

    square = jnp.zeros((rows, W2), F32)
    square = lax.fori_loop(0, tiles, project, square, unroll=2)
    mark("norm")
    y_push(2)
    y_forward()
    turn_dn(1)
    y_forward()
    turn_dn(1)
    scale = lax.rsqrt(jnp.sum(square, axis=1, keepdims=True) * (1.0 / width) + NORM_EPS)

    def normalize(n, carry):
        cols = pl.ds(pl.multiple_of(n * tile, tile), tile)
        normed[:, cols] = (am[:, cols] * scale * gain_ref[:, cols]).astype(BF)
        return carry

    lax.fori_loop(0, tiles, normalize, 0)
    mark("pumprest")
    while progress["forward"] < len(across):
        turn_gu()
        y_push(2)
        y_forward()
        turn_dn()
    z_rows = ny * half_f

    def gate_up(steps, at, wide):
        x = jnp.concatenate(
            [normed[:, pl.ds(pl.multiple_of(zof(t) * z_rows, z_rows), z_rows)] for t in steps],
            axis=1,
        )
        sums = []
        for first in (0, half_f):
            w = [
                gu[pl.ds(zof(t) * ny, ny), first : first + half_f, at : at + wide].reshape(
                    z_rows, wide
                )
                for t in steps
            ]
            sums.append(dg(x, jnp.concatenate(w, axis=0)))
        return sums

    bands = [(at, min(256, ff - at)) for at in range(0, ff, 256)]
    mark("finish_a")
    across[0].finish()
    mark("gateup_a")
    for at, wide in bands:
        gate, up = gate_up(order[: nz - late], at, wide)
        early_sum[0, :, at : at + wide] = gate
        early_sum[1, :, at : at + wide] = up
        turn_dn()
    mark("finish_b")
    turn_dn(2)
    across[-1].finish()
    mark("gateup_b")
    for at, wide in bands:
        gate, up = gate_up(order[nz - late :], at, wide)
        gate = gate + early_sum[0, :, at : at + wide]
        up = up + early_sum[1, :, at : at + wide]
        hid[:, at : at + wide] = (gate / (1.0 + jnp.exp(-gate)) * up).astype(BF)
    mark("dnwait")
    turn_dn(4 * half_ring)

    slots = tile // half_f

    def down(n, carry):
        cols = pl.ds(pl.multiple_of(n * tile, tile), tile)
        w = dn[pl.ds(n * slots, slots)].reshape(tile, ff)
        prod = dg(hid[...], w, NT).reshape(nx, 2, own, tile).astype(BF)
        part[0, :, :, cols] = prod[:, 0]
        part[1, :, :, cols] = prod[:, 1]
        return carry

    cuts = 4
    quarter = width // cuts
    pieces = [pl.ds(piece * quarter, quarter) for piece in range(cuts)]
    ch_core = [channel() for _ in range(cuts)]
    ch_part = [channel() for _ in range(cuts)]

    def x_at(d):
        return lax.rem(xx + d + nx, nx)

    def add_cores(piece):
        cols = pieces[piece]
        arrived(pgot.at[:, :, cols], ch_core[piece])
        for d in [2, 1, 3] if nx == 4 else range(1, nx):
            both = part[core, x_at(d), :, cols].astype(F32) + pgot[x_at(d), :, cols].astype(F32)
            comb[d - 1, :, cols] = both.astype(BF)
            copy(
                comb.at[d - 1, :, cols], got.at[d - 1, :, cols], COMB, ch_part[piece], x_dev(d)
            ).start()

    for piece, cols in enumerate(pieces):
        mark(f"down{piece}")
        lax.fori_loop(piece * tiles // cuts, (piece + 1) * tiles // cuts, down, 0, unroll=True)
        copy(
            part.at[1 - core, :, :, cols], pgot.at[:, :, cols], PART, ch_core[piece], near
        ).start()
        if piece >= 2:
            add_cores(piece - 2)
    mark("rs_core")
    add_cores(cuts - 2)
    add_cores(cuts - 1)
    mark("rs_wait")
    for piece, cols in enumerate(pieces):
        total = am[pl.ds(pl.multiple_of(tp * own, own), own), cols]
        total = total + part[core, xx, :, cols].astype(F32) + pgot[xx, :, cols].astype(F32)
        if nx > 1:
            arrived(got.at[:, :, cols], ch_part[piece])
        for d in range(1, nx):
            total = total + got[d - 1, :, cols].astype(F32)
        out_ref[:, cols] = total.astype(BF)
    mark("sendwait")
    gone = [
        (gu.at[0 : nz * ny - 1], GU),
        (dn.at[0 : nz * ny - 1], DN),
        (pz.at[0 : nz - 1], PS),
        (py.at[0 : ny - 1], PY),
        (ow.at[0 : ntp - 1], OW),
        (mx.at[0 : ntp - 1], MX),
        (part.at[0], PART),
    ]
    if nx > 1:
        gone.append((comb, COMB))
    for ref, out in gone:
        copy(ref, ref, out, 0, near).wait_send()
    mark(None)
    assert count[0] <= SEMS, count[0]


def per_device(
    nz,
    ny,
    ntp,
    receptance,
    head_keys,
    head_values,
    decay_preact,
    learning_rate_preact,
    output_gate_preact,
    self_token_weight,
    head_norm_gain,
    output_weight,
    residual,
    premixer_norm_gain,
    mixer_gate_weight,
    mixer_up_weight,
    mixer_down_weight,
):
    rows = receptance.shape[0]
    width = residual.shape[1]
    half_f, ff = mixer_gate_weight.shape
    own = rows // ntp
    nx = ntp // 2
    vmem = pl.BlockSpec(memory_space=pltpu.VMEM)
    hbm = pl.BlockSpec(memory_space=pltpu.HBM)
    return pl.pallas_call(
        functools.partial(kernel, nz, ny, ntp),
        out_shape=jax.ShapeDtypeStruct((own, width), BF),
        in_specs=[hbm] * 14,
        out_specs=vmem,
        scratch_shapes=[
            pltpu.VMEM((rows, W2), BF),
            pltpu.VMEM((rows, W2), BF),
            pltpu.VMEM((rows, W2), BF),
            pltpu.VMEM((rows, W2), F32),
            pltpu.VMEM((rows, W2), F32),
            pltpu.VMEM((rows, W2), BF),
            pltpu.VMEM((2, HS), F32),
            pltpu.VMEM((1, W2), F32),
            pltpu.VMEM((1, width), F32),
            pltpu.VMEM((nz * ny, 2 * half_f, ff), BF),
            pltpu.VMEM((nz * ny, half_f, ff), BF),
            pltpu.VMEM((ntp, W2, width), BF),
            pltpu.VMEM((rows, width), BF),
            pltpu.VMEM((ny, W2, W2), BF),
            pltpu.VMEM((nz, W2, W2), BF),
            pltpu.VMEM((rows // CHUNK, W2, W2), F32),
            pltpu.VMEM((rows, W2), F32),
            pltpu.VMEM((rows, W2), F32),
            pltpu.VMEM((rows, W2), F32),
            pltpu.VMEM((ntp, rows, W2), BF),
            pltpu.VMEM((rows, width), F32),
            pltpu.VMEM((rows, width), BF),
            pltpu.VMEM((rows, ff), BF),
            pltpu.VMEM((2, nx, own, width), BF),
            pltpu.VMEM((max(nx - 1, 1), own, width), BF),
            pltpu.VMEM((nx, own, width), BF),
            pltpu.VMEM((max(nx - 1, 1), own, width), BF),
            pltpu.VMEM((2, rows, ff), F32),
            pltpu.SemaphoreType.DMA((14,)),
            pltpu.SemaphoreType.DMA((8,)),
            pltpu.SemaphoreType.DMA((SEMS,)),
        ],
        compiler_params=pltpu.CompilerParams(
            collective_id=0, has_side_effects=True, vmem_limit_bytes=60 * 1024 * 1024
        ),
        name="layer",
    )(
        receptance,
        head_keys,
        head_values,
        decay_preact,
        learning_rate_preact,
        output_gate_preact,
        self_token_weight,
        head_norm_gain.reshape(1, -1),
        output_weight,
        residual,
        premixer_norm_gain.reshape(1, -1),
        mixer_gate_weight,
        mixer_up_weight,
        mixer_down_weight.T,
    )


def build(mesh, nz, ny):
    ntp = mesh.shape["tp"]
    torus = Mesh(mesh.devices.reshape(nz, ny, ntp), ("z", "y", "tp"))
    sp = ("z", "y")
    cut = P(sp, "tp")
    in_specs = (cut,) * 6 + (
        P("tp", None),
        P("tp"),
        P("tp", None),
        P(sp, None),
        P(),
        cut,
        cut,
        P("tp", sp),
    )
    return jax.shard_map(
        functools.partial(per_device, nz, ny, ntp),
        mesh=torus,
        in_specs=in_specs,
        out_specs=P(("z", "y", "tp"), None),
        check_vma=False,
    )


def solution(mesh):
    return build(mesh, 16, 4)
```
